512 devices in a mesh: rep: 2 (over z_hi), fs: 32 (over z_lo, y), tp: 8 (over x, core).
Axes of the slice: x: 4, y: 4, z: 16 (z_hi: 2, z_lo: 8; z = z_hi * 8 + z_lo), core: 2. Of those that a mesh axis runs over, the one named last changes fastest.
Arguments:
- tokens: bfloat16 [64, 1024, 1024], P(('rep', 'fs'), 'tp'), may hold values from -6 to 6
- mixer_in_gain: float32 [1024], replicated, may hold values from 0.5 to 1.5
- query_weight: bfloat16 [1024, 1024], P('fs', 'tp'), may hold values from -0.1875 to 0.1875
- key_weight: bfloat16 [1024, 1024], P('fs', 'tp'), may hold values from -0.1875 to 0.1875
- value_weight: bfloat16 [1024, 2048], P('fs', 'tp'), may hold values from -0.1875 to 0.1875
- gate_weight: bfloat16 [1024, 2048], P('fs', 'tp'), may hold values from -0.1875 to 0.1875
- decay_logits: float32 [2, 8], P(None, 'tp'), may hold values from 3.4 to 6.2
- mixer_output: bfloat16 [2048, 1024], P('tp', 'fs'), may hold values from -0.125 to 0.125
- mixer_out_gain: float32 [1024], replicated, may hold values from 0.5 to 1.5
- channel_in_gain: float32 [1024], replicated, may hold values from 0.5 to 1.5
- gelu_weight: bfloat16 [1024, 2816], P('fs', 'tp'), may hold values from -0.1875 to 0.1875
- linear_weight: bfloat16 [1024, 2816], P('fs', 'tp'), may hold values from -0.1875 to 0.1875
- gelu_kernel: float32 [3, 2816], P(None, 'tp'), may hold values from -3.5 to 3.5
- linear_kernel: float32 [3, 2816], P(None, 'tp'), may hold values from -3.5 to 3.5
- gelu_bias: float32 [2816], P('tp'), may hold values from -1.2 to 1.2
- linear_bias: float32 [2816], P('tp'), may hold values from -1.2 to 1.2
- down_weight: bfloat16 [2816, 1024], P('tp', 'fs'), may hold values from -0.109375 to 0.109375
- channel_out_gain: float32 [1024], replicated, may hold values from 0.5 to 1.5
Outputs:
- layer_output: bfloat16 [64, 1024, 1024], P(('rep', 'fs'), 'tp')
The draws below stay inside these ranges and needn't reach their ends.
All inputs are finite; a program needn't handle non-finite values.
Results may differ from the reference program's by a relative error of at most 0.02.
Values may be sent and summed in bfloat16 or wider, within the bound.
A program may use at most 64 MiB of HBM per device.

```python
import jax
import jax.numpy as jnp
from jax import lax

D = 1024
HEADS = 8
DK = 128
DV = 256
FF = 2816
TAPS = 3
SPAN = 128
SEQ = 1024
SEQS = 64


def block_levels(own_key, shape, pieces, low, largest):
    level = 1.0
    for position, blocks in pieces:
        heights = jax.random.uniform(jax.random.fold_in(jax.random.fold_in(own_key, 6), position), (blocks,), jnp.float32, low / len(pieces), largest / len(pieces))
        level = level * jnp.repeat(jnp.exp(heights), shape[position] // blocks).reshape((-1,) + (1,) * (len(shape) - 1 - position))
    return level


def noise(own_key, dims, deviation, reach, pieces=(), kind=jnp.bfloat16):
    result = deviation * jax.random.normal(own_key, dims, jnp.float32)
    if pieces:
        result = result * block_levels(own_key, dims, pieces, -0.22, 0.18)
    return jnp.clip(result, -reach, reach).astype(kind)


def setup_inputs(seed: int = 0) -> dict:
    splits = jax.random.split(jax.random.key(seed), 19)
    return {
        "tokens": noise(splits[0], (SEQS, SEQ, D), 1.0, 6.0, ((0, 64), (1, 8))),
        "mixer_in_gain": jnp.clip(1.0 + 0.1 * jax.random.normal(splits[1], (D,), jnp.float32), 0.5, 1.5),
        "query_weight": noise(splits[2], (D, HEADS * DK), D ** -0.5, 0.1875, ((0, 32), (1, 8))),
        "key_weight": noise(splits[3], (D, HEADS * DK), D ** -0.5, 0.1875, ((0, 32), (1, 8))),
        "value_weight": noise(splits[4], (D, HEADS * DV), D ** -0.5, 0.1875, ((0, 32), (1, 8))),
        "gate_weight": noise(splits[5], (D, HEADS * DV), D ** -0.5, 0.1875, ((0, 32), (1, 8))),
        "decay_logits": jnp.clip(3.4 + 2.7999997 * jax.random.uniform(splits[6], (2, HEADS), jnp.float32) ** block_levels(splits[6], (2, HEADS), ((1, 8),), -0.2, 0.2), 3.4, 6.2),
        "mixer_output": noise(splits[7], (HEADS * DV, D), (HEADS * DV) ** -0.5, 0.125, ((0, 8), (1, 32))),
        "mixer_out_gain": jnp.clip(1.0 + 0.1 * jax.random.normal(splits[8], (D,), jnp.float32), 0.5, 1.5),
        "channel_in_gain": jnp.clip(1.0 + 0.1 * jax.random.normal(splits[9], (D,), jnp.float32), 0.5, 1.5),
        "gelu_weight": noise(splits[10], (D, FF), D ** -0.5, 0.1875, ((0, 32), (1, 8))),
        "linear_weight": noise(splits[11], (D, FF), D ** -0.5, 0.1875, ((0, 32), (1, 8))),
        "gelu_kernel": noise(splits[12], (TAPS, FF), TAPS ** -0.5, 3.5, ((1, 8),), jnp.float32),
        "linear_kernel": noise(splits[13], (TAPS, FF), TAPS ** -0.5, 3.5, ((1, 8),), jnp.float32),
        "gelu_bias": noise(splits[14], (FF,), 0.3, 1.2, ((0, 8),), jnp.float32),
        "linear_bias": noise(splits[15], (FF,), 0.3, 1.2, ((0, 8),), jnp.float32),
        "down_weight": noise(splits[16], (FF, D), FF ** -0.5, 0.109375, ((0, 8), (1, 32))),
        "channel_out_gain": jnp.clip(1.0 + 0.1 * jax.random.normal(splits[17], (D,), jnp.float32), 0.5, 1.5),
    }


epsilon = 1e-06
rope_base = 10000.0

def rms_scaled(row_values, norm_gain):
    values = row_values.astype(jnp.float32)
    return values * lax.rsqrt(lax.optimization_barrier(jnp.mean(values * values, axis=-1, keepdims=True)) + epsilon) * norm_gain

def rotate(values, positions):
    half_width = values.shape[-1] // 2
    frequency = 1.0 / rope_base ** (jnp.arange(half_width, dtype=jnp.float32) / half_width)
    angles = positions.astype(jnp.float32)[:, None] * frequency[None, :]
    cosine = jnp.cos(angles)[:, None, :]
    sine_part = jnp.sin(angles)[:, None, :]
    first_half = values[..., :half_width]
    second = values[..., half_width:]
    return jnp.concatenate([first_half * cosine - second * sine_part, first_half * sine_part + second * cosine], axis=-1)

def one_direction(queries, key_rows, value_rows, log_decay, strict):
    highest = lax.Precision.HIGHEST
    length = queries.shape[0]
    head_count = queries.shape[1]
    block_count = length // SPAN
    inside_index = jnp.arange(SPAN, dtype=jnp.float32)
    offset = inside_index[:, None] - inside_index[None, :]
    allowed = offset >= (1.0 if strict else 0.0)
    within = jnp.where(allowed[None], jnp.exp(jnp.where(allowed, offset, 0.0)[None] * log_decay[:, None, None]), 0.0)
    query_blocks = queries.reshape(block_count, SPAN, head_count, -1).astype(jnp.float32)
    key_blocks = key_rows.reshape(block_count, SPAN, head_count, -1).astype(jnp.float32)
    value_blocks = value_rows.reshape(block_count, SPAN, head_count, -1).astype(jnp.float32)
    scores = jnp.einsum('nchd,nmhd->nhcm', query_blocks, key_blocks, precision=highest) * within[None]
    inside = jnp.einsum('nhcm,nmhe->nche', scores, value_blocks, precision=highest)
    tail_decay = jnp.exp((SPAN - 1.0 - inside_index)[:, None] * log_decay[None, :])
    lead_decay = jnp.exp((inside_index + 1.0)[:, None] * log_decay[None, :])
    step_decay = jnp.exp(SPAN * log_decay)
    updates = jnp.einsum('nmhd,nmhe->nhde', key_blocks, value_blocks * tail_decay[None, :, :, None], precision=highest)

    def advance(carried, update):
        return (step_decay[:, None, None] * carried + update, carried)
    _, before = lax.scan(advance, jnp.zeros(updates.shape[1:], jnp.float32), updates)
    across = jnp.einsum('nchd,nhde->nche', query_blocks * lead_decay[None, :, :, None], before, precision=highest)
    return (inside + across).reshape(length, head_count, -1)

def retention(queries, key_rows, value_rows, logits):
    log_forward = jax.nn.log_sigmoid(logits[0])
    log_backward = jax.nn.log_sigmoid(logits[1])
    forward = one_direction(queries, key_rows, value_rows, log_forward, False)
    behind = one_direction(queries[::-1], key_rows[::-1], value_rows[::-1], log_backward, True)[::-1]
    return forward + behind

def head_norm(values):
    centred = values - lax.optimization_barrier(jnp.mean(values, axis=-1, keepdims=True))
    return centred * lax.rsqrt(lax.optimization_barrier(jnp.mean(centred * centred, axis=-1, keepdims=True)) + epsilon)

def conv_positions(values, kernel, biases):
    padded = jnp.pad(values.astype(jnp.float32), ((1, 1), (0, 0)))
    return kernel[0] * padded[:-2] + kernel[1] * padded[1:-1] + kernel[2] * padded[2:] + biases

def reference(tokens, mixer_in_gain, query_weight, key_weight, value_weight, gate_weight, decay_logits, mixer_output, mixer_out_gain, channel_in_gain, gelu_weight, linear_weight, gelu_kernel, linear_kernel, gelu_bias, linear_bias, down_weight, channel_out_gain):

    def one_sequence(token_rows):
        positions = jnp.arange(SEQ, dtype=jnp.int32)
        normed = rms_scaled(token_rows, mixer_in_gain).astype(jnp.bfloat16)
        query_raw = jnp.dot(normed, query_weight, preferred_element_type=jnp.float32).reshape(SEQ, HEADS, DK)
        queries = rotate(query_raw, positions).astype(jnp.bfloat16)
        key_raw = jnp.dot(normed, key_weight, preferred_element_type=jnp.float32).reshape(SEQ, HEADS, DK)
        key_rows = (rotate(key_raw, positions) * DK ** (-0.5)).astype(jnp.bfloat16)
        value_rows = jnp.dot(normed, value_weight, preferred_element_type=jnp.float32).astype(jnp.bfloat16).reshape(SEQ, HEADS, DV)
        gate_rows = jnp.dot(normed, gate_weight, preferred_element_type=jnp.float32).astype(jnp.bfloat16)
        retained = retention(queries, key_rows, value_rows, decay_logits)
        gated = (head_norm(retained).reshape(SEQ, HEADS * DV) * jax.nn.silu(gate_rows.astype(jnp.float32))).astype(jnp.bfloat16)
        mix_sum = jnp.dot(gated, mixer_output, preferred_element_type=jnp.float32)
        after_mix = (token_rows.astype(jnp.float32) + rms_scaled(mix_sum, mixer_out_gain)).astype(jnp.bfloat16)
        channel_in = rms_scaled(after_mix, channel_in_gain).astype(jnp.bfloat16)
        gelu_in = jnp.dot(channel_in, gelu_weight, preferred_element_type=jnp.float32).astype(jnp.bfloat16)
        linear_in = jnp.dot(channel_in, linear_weight, preferred_element_type=jnp.float32).astype(jnp.bfloat16)
        hidden = (jax.nn.gelu(conv_positions(gelu_in, gelu_kernel, gelu_bias)) * conv_positions(linear_in, linear_kernel, linear_bias)).astype(jnp.bfloat16)
        channel_sum = jnp.dot(hidden, down_weight, preferred_element_type=jnp.float32)
        return (after_mix.astype(jnp.float32) + rms_scaled(channel_sum, channel_out_gain)).astype(jnp.bfloat16)
    return lax.map(one_sequence, tokens)
```

```python
import functools

import jax
import jax.numpy as jnp
import numpy as np
from jax import lax
from jax.experimental import pallas as pl
from jax.experimental.pallas import tpu as pltpu
from jax.sharding import PartitionSpec as P

MESH = pl.DeviceIdType.MESH
F32 = jnp.float32
BF16 = jnp.bfloat16

X, Y, Z, ZALL = 4, 4, 8, 16
D = 1024
DK = 128
DV = 256
SEQ = 1024
OWN = 128
HALF = 64
BLOCK = 256
UNIT = 32
FFP = 384
FFOWN = 352
EPS = 1e-6
NT = (((1,), (1,)), ((), ()))
TN = (((0,), (0,)), ((), ()))


def rotation_tables():
    frequency = 10000.0 ** (-np.arange(64, dtype=np.float64) / 64)

    def pair(positions):
        angles = positions[:, None] * frequency[None, :]
        cosine, sine = np.cos(angles), np.sin(angles)
        return np.concatenate([cosine, cosine], 1), np.concatenate([-sine, sine], 1)

    inner = np.concatenate(pair(np.arange(BLOCK, dtype=np.float64)), 1)
    outer = np.concatenate(pair(BLOCK * np.repeat(np.arange(X, dtype=np.float64), 8)), 1)
    return inner.astype(np.float32), outer.astype(np.float32)


def dot(a, b, dims=None):
    if dims is None:
        return jnp.dot(a, b, preferred_element_type=F32)
    return lax.dot_general(a, b, dims, preferred_element_type=F32)


def rms(values, gain):
    return values * lax.rsqrt(jnp.mean(values * values, axis=-1, keepdims=True) + EPS) * gain


def kernel(
    tok, g_in, wq, wk, wv, wg, logits, wo, g_mo, g_ci, w_gelu, w_linear, k_gelu, k_linear,
    b_gelu, b_linear, wd, g_co, inner, outer,
    out,
    xn, ch, w1, w2, wb, qs, ins, us, st, dmat, lead, tail, pf, ps, pr, rs_send, rs_recv,
    ms_send, ms_recv, up, hid, after, taps,
    ag_s, ag_r, wy_s, wy_r, wz_s, wz_r, bz_s, bz_r, by_s, by_r, pp_s, pp_r, rr_s, rr_r, mm_s, mm_r,
):
    rep, fs, tp = lax.axis_index("rep"), lax.axis_index("fs"), lax.axis_index("tp")
    x, c = tp // 2, tp % 2
    z, y = fs // Y, fs % Y
    zz = rep * Z + z

    def x_dev(step):
        return (rep, fs, lax.rem(x + step, X) * 2 + c)

    def y_dev(step):
        return (rep, z * Y + lax.rem(y + step, Y), tp)

    def z_dev(step):
        there = lax.rem(zz + step, ZALL)
        return (there // Z, lax.rem(there, Z) * Y + y, tp)

    sibling = (rep, fs, x * 2 + (1 - c))
    x_next, x_prev = x_dev(1), x_dev(X - 1)
    y_next, y_prev, y_far = y_dev(1), y_dev(Y - 1), y_dev(2)
    z_next, z_prev = z_dev(1), z_dev(ZALL - 1)

    barrier = pltpu.get_barrier_semaphore()
    for peer in (x_next, x_prev, sibling, y_next, y_prev, y_far, z_next, z_prev):
        pl.semaphore_signal(barrier, inc=1, device_id=peer, device_id_type=MESH)

    sent = []

    def send(src, dst, send_sem, recv_sem, peer):
        copy = pltpu.make_async_remote_copy(
            src_ref=src, dst_ref=dst, send_sem=send_sem, recv_sem=recv_sem,
            device_id=peer, device_id_type=MESH,
        )
        copy.start()
        sent.append(copy)

    def received(dst, send_sem, recv_sem):
        pltpu.make_async_remote_copy(
            src_ref=dst, dst_ref=dst, send_sem=send_sem, recv_sem=recv_sem,
            device_id=sibling, device_id_type=MESH,
        ).wait_recv()

    def rows(first, count):
        return pl.ds(pl.multiple_of(first, count), count)

    def ag_place(buf, d, core, half):
        chip = lax.rem(x + d, X)
        return buf.at[rows((chip * 2 + core) * OWN + half * HALF, HALF)]

    def ag_send(t, buf, k, d, half, peer):
        here = ag_place(buf, d, c, half)
        send(here, here, ag_s.at[t, k], ag_r.at[t, k], peer)

    def ag_wait(t, buf, k, d, core, half):
        received(ag_place(buf, d, core, half), ag_s.at[t, k], ag_r.at[t, k])

    def ag_start(t, buf, half):
        ag_send(t, buf, half, 0, half, x_next)
        ag_send(t, buf, 2 + half, 0, half, x_prev)
        ag_send(t, buf, 6 + half, 0, half, sibling)

    def ag_first(t, buf, half):
        ag_wait(t, buf, half, 3, c, half)
        if half == 0:
            ag_send(t, buf, 4, 3, 0, x_next)
        ag_wait(t, buf, 2 + half, 1, c, half)
        if half == 1:
            ag_send(t, buf, 5, 1, 1, x_prev)
        ag_send(t, buf, 6 + 6 + half, 3, half, sibling)
        ag_send(t, buf, 6 + 2 + half, 1, half, sibling)

    def ag_second(t, buf, half):
        ag_wait(t, buf, 4 + half, 2, c, half)
        ag_send(t, buf, 6 + 4 + half, 2, half, sibling)

    def ag_sibling(t, buf, d):
        for half in (0, 1):
            ag_wait(t, buf, 6 + 2 * d + half, d, 1 - c, half)

    def wa_y_start(t, buf):
        here = buf.at[rows(fs * UNIT, UNIT)]
        for k, peer in ((0, y_next), (1, y_prev), (2, y_far)):
            send(here, here, wy_s.at[t, k], wy_r.at[t, k], peer)

    def wa_y_wait(t, buf):
        for k, step in ((0, Y - 1), (1, 1), (2, 2)):
            there = buf.at[rows((z * Y + lax.rem(y + step, Y)) * UNIT, UNIT)]
            received(there, wy_s.at[t, k], wy_r.at[t, k])

    def wa_slab(buf, off, half):
        return buf.at[rows(lax.rem(z + off + Z, Z) * (Y * UNIT) + half * HALF, HALF)]

    def wa_z_send(t, buf, s, half, way):
        here = wa_slab(buf, -(s - 1) if way == 0 else s - 1, half)
        k = way * 8 + (s - 1) * 2 + half
        send(here, here, wz_s.at[t, k], wz_r.at[t, k], z_next if way == 0 else z_prev)

    def wa_z_wait(t, buf, s, half, way):
        k = way * 8 + (s - 1) * 2 + half
        received(wa_slab(buf, -s if way == 0 else s, half), wz_s.at[t, k], wz_r.at[t, k])

    def wa_z_start(t, buf):
        for half in (0, 1):
            for way in (0, 1):
                wa_z_send(t, buf, 1, half, way)

    def wa_z_step(t, buf, s, half):
        for way in (0, 1):
            wa_z_wait(t, buf, s, half, way)
            if s < 3 or half == way:
                wa_z_send(t, buf, s + 1, half, way)

    def wa_z_end(t, buf):
        for way in (0, 1):
            wa_z_wait(t, buf, 4, way, way)

    offsets = (0, -1, 1, -2, 2, -3, 3, 4)

    def wb_unit(off, y_at):
        return (lax.rem(z + off + Z, Z) * Y + y_at) * UNIT

    def bz_send(s, way):
        first = wb_unit(-(s - 1) if way == 0 else s - 1, y)
        if s == 4:
            here = wb.at[rows(first + way * 16, 16)]
        else:
            here = wb.at[rows(first, UNIT)]
        k = way * 4 + s - 1
        send(here, here, bz_s.at[k], bz_r.at[k], z_next if way == 0 else z_prev)

    def bz_wait(s, way):
        first = wb_unit(-s if way == 0 else s, y)
        if s == 4:
            here = wb.at[rows(first + way * 16, 16)]
        else:
            here = wb.at[rows(first, UNIT)]
        k = way * 4 + s - 1
        received(here, bz_s.at[k], bz_r.at[k])

    def by_send(j, k, y_step, peer):
        here = wb.at[rows(wb_unit(offsets[j], lax.rem(y + y_step, Y)), UNIT)]
        send(here, here, by_s.at[j, k], by_r.at[j, k], peer)

    def by_wait(j, k, y_step):
        here = wb.at[rows(wb_unit(offsets[j], lax.rem(y + y_step, Y)), UNIT)]
        received(here, by_s.at[j, k], by_r.at[j, k])

    def by_start(j):
        by_send(j, 0, 0, y_next)
        by_send(j, 1, 0, y_prev)

    def by_relay(j):
        by_wait(j, 0, 3)
        by_wait(j, 1, 1)
        if j % 2 == 0:
            by_send(j, 2, 3, y_next)
        else:
            by_send(j, 2, 1, y_prev)

    def bz_step(s):
        for way in (0, 1):
            bz_wait(s, way)
            if s < 4:
                bz_send(s + 1, way)
        if s < 4:
            by_start(2 * s - 1)
            by_start(2 * s)
        else:
            by_start(7)

    tokens = tok[...].astype(F32)
    xn[rows(tp * OWN, OWN)] = rms(tokens, g_in[...]).astype(BF16)
    own = rows(fs * UNIT, UNIT)
    w1[own, 0:128] = wq[...]
    w1[own, 128:256] = wk[...]
    w1[own, 256:512] = wv[...]
    w2[own, 0:256] = wg[...]
    eye = (
        lax.broadcasted_iota(jnp.int32, (UNIT, UNIT), 0)
        == lax.broadcasted_iota(jnp.int32, (UNIT, UNIT), 1)
    ).astype(F32).astype(BF16)
    w2[own, 256:512] = dot(eye, wo[...], NT).astype(BF16)
    wb[own] = jnp.zeros((UNIT, 3 * FFP), BF16)
    wb[own, 0:FFOWN] = w_gelu[...]
    wb[own, FFP : FFP + FFOWN] = w_linear[...]
    wb[own, 2 * FFP : 2 * FFP + FFOWN] = dot(eye, wd[...], NT).astype(BF16)

    pl.semaphore_wait(barrier, 8)

    ag_start(0, xn, 0)
    wa_y_start(0, w1)
    ag_start(0, xn, 1)
    bz_send(1, 0)
    bz_send(1, 1)
    wa_y_start(1, w2)
    by_start(0)

    log_f = -jnp.log1p(jnp.exp(-logits[0:1, 0:1]))
    log_b = -jnp.log1p(jnp.exp(-logits[1:2, 0:1]))
    at = lax.broadcasted_iota(jnp.int32, (BLOCK, BLOCK), 0)
    lane = lax.broadcasted_iota(jnp.int32, (BLOCK, BLOCK), 1)
    apart = (at - lane).astype(F32)
    dmat[...] = jnp.exp(jnp.where(at >= lane, apart * log_f, -apart * log_b))
    ahead = at.astype(F32)
    lead[...] = jnp.exp(
        jnp.where(lane < DK, (ahead + 1.0) * log_f, (float(BLOCK) - ahead) * log_b)
    )
    tail[...] = jnp.exp(jnp.where(lane < DK, (BLOCK - 1.0 - ahead) * log_f, ahead * log_b))
    step_f, step_b = jnp.exp(BLOCK * log_f), jnp.exp(BLOCK * log_b)
    taps[...] = jnp.zeros((16, FFP), F32)
    taps[0:3, 0:FFOWN] = k_gelu[...]
    taps[3:4, 0:FFOWN] = b_gelu[...]
    taps[8:11, 0:FFOWN] = k_linear[...]
    taps[11:12, 0:FFOWN] = b_linear[...]
    up[0:8] = jnp.zeros((8, 2 * FFP), F32)
    up[SEQ + 8 : SEQ + 16] = jnp.zeros((8, 2 * FFP), F32)

    wa_y_wait(0, w1)
    wa_z_start(0, w1)
    ag_first(0, xn, 0)
    wa_z_step(0, w1, 1, 0)
    wa_z_step(0, w1, 1, 1)
    ag_first(0, xn, 1)
    wa_z_step(0, w1, 2, 0)
    wa_z_step(0, w1, 2, 1)
    ag_second(0, xn, 0)
    ag_second(0, xn, 1)
    wa_z_step(0, w1, 3, 0)
    wa_z_step(0, w1, 3, 1)
    wa_y_wait(1, w2)
    wa_z_start(1, w2)
    for d in (0, 1, 3, 2):
        ag_sibling(0, xn, d)
    wa_z_end(0, w1)

    w2_tasks = [
        functools.partial(wa_z_step, 1, w2, s, half) for s in (1, 2, 3) for half in (0, 1)
    ]
    ff_tasks = [functools.partial(bz_step, s) for s in (1, 2, 3, 4)]
    ff_tasks += [functools.partial(by_relay, j) for j in range(8)]

    def pump(tasks, count):
        for _ in range(count):
            if tasks:
                tasks.pop(0)()

    for n, d in enumerate((0, 1, 3, 2)):
        i = lax.rem(x + d, X)
        here = rows(i * BLOCK, BLOCK)
        base = outer[rows(i * 8, 8)][0:1]
        base_cos, base_sin = base[:, 0:128], base[:, 128:256]
        cosine = base_cos * inner[:, 0:128] - base_sin * inner[:, 128:256]
        sine = base_sin * inner[:, 0:128] + base_cos * inner[:, 128:256]
        qk = dot(xn[here], w1[:, 0:256])
        q, k = qk[:, 0:128], qk[:, 128:256]
        q = (q * cosine + pltpu.roll(q, 64, 1) * sine).astype(BF16)
        k = ((k * cosine + pltpu.roll(k, 64, 1) * sine) * DK**-0.5).astype(BF16)
        qs[here] = q
        v = dot(xn[here], w1[:, 256:512]).astype(BF16)
        scores = (dot(q, k, NT) * dmat[...]).astype(BF16)
        ins[here] = dot(scores, v)
        kf = k.astype(F32)
        k_two = (jnp.concatenate([kf, kf], axis=1) * tail[...]).astype(BF16)
        us[here] = dot(k_two, v, TN)
        pump(w2_tasks, 1)

    total = jnp.zeros((DK, DV), F32)
    for i in range(X):
        st[i * BLOCK : i * BLOCK + DK] = total.astype(BF16)
        total = step_f * total + us[i * BLOCK : i * BLOCK + DK]
    total = jnp.zeros((DK, DV), F32)
    for i in reversed(range(X)):
        st[i * BLOCK + DK : (i + 1) * BLOCK] = total.astype(BF16)
        total = step_b * total + us[i * BLOCK + DK : (i + 1) * BLOCK]

    pump(w2_tasks, 2)
    wa_z_end(1, w2)
    pump(ff_tasks, 1)

    def rs_block(t, d, left, weights, first, width):
        for j in range(4):
            part = dot(left, weights[j * 256 : (j + 1) * 256, first : first + width], NT)
            pf[d * BLOCK : (d + 1) * BLOCK, j * 256 : (j + 1) * 256] = part
            ps[t, d * BLOCK : (d + 1) * BLOCK, j * 256 : (j + 1) * 256] = part.astype(BF16)
        send(
            ps.at[t, rows(d * BLOCK + (1 - c) * OWN, OWN)],
            pr.at[t, d], pp_s.at[t, d], pp_r.at[t, d], sibling,
        )

    def rs_pair_wait(t, d):
        received(pr.at[t, d], pp_s.at[t, d], pp_r.at[t, d])

    def rs_pair(t, d, half):
        mine = pf[rows(d * BLOCK + c * OWN + half * HALF, HALF)]
        return mine + pr[t, d, half * HALF : (half + 1) * HALF].astype(F32)

    def rs_far(t):
        rs_pair_wait(t, 2)
        for half, peer in ((0, x_next), (1, x_prev)):
            rs_send[t, half] = rs_pair(t, 2, half).astype(BF16)
            send(rs_send.at[t, half], rs_recv.at[t, half], rr_s.at[t, half], rr_r.at[t, half], peer)

    def rs_near(t, way, half, relay):
        d = 1 if way == 0 else 3
        total = rs_pair(t, d, half)
        if relay:
            received(rs_recv.at[t, half], rr_s.at[t, half], rr_r.at[t, half])
            total = total + rs_recv[t, half].astype(F32)
        k = way * 2 + half
        ms_send[t, k] = total.astype(BF16)
        peer = x_next if way == 0 else x_prev
        send(ms_send.at[t, k], ms_recv.at[t, k], mm_s.at[t, k], mm_r.at[t, k], peer)

    def rs_final(t, half):
        total = rs_pair(t, 0, half)
        for way in (0, 1):
            k = way * 2 + half
            received(ms_recv.at[t, k], mm_s.at[t, k], mm_r.at[t, k])
            total = total + ms_recv[t, k].astype(F32)
        return total

    def reduce_scatter(t, block, weights, first, width, between):
        for n, d in enumerate((2, 1, 3, 0)):
            rs_block(t, d, block(d), weights, first, width)
            if n == 1:
                rs_far(t)
            if n == 2:
                rs_pair_wait(t, 1)
                rs_near(t, 0, 1, False)
            if n == 3:
                rs_pair_wait(t, 3)
                rs_near(t, 1, 0, False)
            between(n)
        rs_near(t, 0, 0, True)
        rs_near(t, 1, 1, True)
        rs_pair_wait(t, 0)

    def mixer_block(d):
        i = lax.rem(x + d, X)
        here = rows(i * BLOCK, BLOCK)
        q = qs[here].astype(F32)
        q_two = (jnp.concatenate([q, q], axis=1) * lead[...]).astype(BF16)
        retained = ins[here] + dot(q_two, st[here])
        centred = retained - jnp.mean(retained, axis=-1, keepdims=True)
        normal = centred * lax.rsqrt(jnp.mean(centred * centred, axis=-1, keepdims=True) + EPS)
        gates = dot(xn[here], w2[:, 0:256])
        return (normal * (gates / (1.0 + jnp.exp(-gates)))).astype(BF16)

    reduce_scatter(0, mixer_block, w2, 256, 256, lambda n: pump(ff_tasks, 1))
    for half in (0, 1):
        part = slice(half * HALF, (half + 1) * HALF)
        mixed = rs_final(0, half)
        summed = (tok[part].astype(F32) + rms(mixed, g_mo[...])).astype(BF16).astype(F32)
        after[part] = summed
        ch[rows(tp * OWN + half * HALF, HALF)] = rms(summed, g_ci[...]).astype(BF16)
        ag_start(1, ch, half)

    ag_first(1, ch, 0)
    pump(ff_tasks, 4)
    ag_first(1, ch, 1)
    pump(ff_tasks, 4)
    for j in range(8):
        by_wait(j, 2, 2)
    ag_second(1, ch, 0)
    ag_second(1, ch, 1)

    for d in (0, 1, 3, 2):
        ag_sibling(1, ch, d)
        i = lax.rem(x + d, X)
        for j in range(3):
            up[pl.ds(pl.multiple_of(i * BLOCK + 8, 8), BLOCK), j * 256 : (j + 1) * 256] = dot(
                ch[rows(i * BLOCK, BLOCK)], wb[:, j * 256 : (j + 1) * 256]
            )

    def conv(first, column, at):
        near = up[pl.ds(pl.multiple_of(first, 8), 80), column : column + FFP]
        before = pltpu.roll(near, 1, 0)[8:72]
        behind = pltpu.roll(near, 79, 0)[8:72]
        return (
            taps[at : at + 1] * before
            + taps[at + 1 : at + 2] * near[8:72]
            + taps[at + 2 : at + 3] * behind
            + taps[at + 3 : at + 4]
        )

    def channel_block(d):
        i = lax.rem(x + d, X)

        def tile(n, carry):
            first = i * BLOCK + n * HALF
            g = conv(first, 0, 0)
            act = 0.5 * g * (1.0 + jnp.tanh(0.7978845608028654 * (g + 0.044715 * g * g * g)))
            hid[pl.ds(pl.multiple_of(n * HALF, HALF), HALF)] = (
                act * conv(first, FFP, 8)
            ).astype(BF16)
            return carry

        lax.fori_loop(0, BLOCK // HALF, tile, 0)
        return hid[...]

    reduce_scatter(1, channel_block, wb, 2 * FFP, FFP, lambda n: None)
    for half in (0, 1):
        part = slice(half * HALF, (half + 1) * HALF)
        out[part] = (after[part] + rms(rs_final(1, half), g_co[...])).astype(BF16)

    for copy in sent:
        copy.wait_send()


def layer(
    tokens, mixer_in_gain, query_weight, key_weight, value_weight, gate_weight, decay_logits,
    mixer_output, mixer_out_gain, channel_in_gain, gelu_weight, linear_weight, gelu_kernel,
    linear_kernel, gelu_bias, linear_bias, down_weight, channel_out_gain,
):
    inner, outer = rotation_tables()

    def row(v):
        return v.reshape(1, -1)

    operands = (
        tokens[0], row(mixer_in_gain), query_weight, key_weight, value_weight, gate_weight,
        decay_logits, mixer_output, row(mixer_out_gain), row(channel_in_gain), gelu_weight,
        linear_weight, gelu_kernel, linear_kernel, row(gelu_bias), row(linear_bias), down_weight,
        row(channel_out_gain), jnp.asarray(inner), jnp.asarray(outer),
    )
    dma = pltpu.SemaphoreType.DMA
    result = pl.pallas_call(
        kernel,
        out_shape=jax.ShapeDtypeStruct((OWN, D), BF16),
        in_specs=[pl.BlockSpec(memory_space=pltpu.VMEM)] * len(operands),
        out_specs=pl.BlockSpec(memory_space=pltpu.VMEM),
        scratch_shapes=[
            pltpu.VMEM((SEQ, D), BF16),
            pltpu.VMEM((SEQ, D), BF16),
            pltpu.VMEM((D, 512), BF16),
            pltpu.VMEM((D, 512), BF16),
            pltpu.VMEM((D, 3 * FFP), BF16),
            pltpu.VMEM((SEQ, DK), BF16),
            pltpu.VMEM((SEQ, DV), F32),
            pltpu.VMEM((SEQ, DV), F32),
            pltpu.VMEM((SEQ, DV), BF16),
            pltpu.VMEM((BLOCK, BLOCK), F32),
            pltpu.VMEM((BLOCK, BLOCK), F32),
            pltpu.VMEM((BLOCK, BLOCK), F32),
            pltpu.VMEM((SEQ, D), F32),
            pltpu.VMEM((2, SEQ, D), BF16),
            pltpu.VMEM((2, 4, OWN, D), BF16),
            pltpu.VMEM((2, 2, HALF, D), BF16),
            pltpu.VMEM((2, 2, HALF, D), BF16),
            pltpu.VMEM((2, 4, HALF, D), BF16),
            pltpu.VMEM((2, 4, HALF, D), BF16),
            pltpu.VMEM((SEQ + 16, 2 * FFP), F32),
            pltpu.VMEM((BLOCK, FFP), BF16),
            pltpu.VMEM((OWN, D), F32),
            pltpu.VMEM((16, FFP), F32),
            dma((2, 14)), dma((2, 14)),
            dma((2, 3)), dma((2, 3)),
            dma((2, 16)), dma((2, 16)),
            dma((8,)), dma((8,)),
            dma((8, 3)), dma((8, 3)),
            dma((2, 4)), dma((2, 4)),
            dma((2, 2)), dma((2, 2)),
            dma((2, 4)), dma((2, 4)),
        ],
        compiler_params=pltpu.CompilerParams(
            collective_id=0, has_side_effects=True, vmem_limit_bytes=60 * 1024 * 1024
        ),
        name="layer",
    )(*operands)
    return result[None]


def solution(mesh):
    by_position = P(("rep", "fs"), "tp", None)
    up_rows, down_rows = P("fs", "tp"), P("tp", "fs")
    in_specs = (
        by_position, P(), up_rows, up_rows, up_rows, up_rows, P(None, "tp"), down_rows, P(), P(),
        up_rows, up_rows, P(None, "tp"), P(None, "tp"), P("tp"), P("tp"), down_rows, P(),
    )
    return jax.shard_map(
        layer, mesh=mesh, in_specs=in_specs, out_specs=by_position, check_vma=False
    )
```

```python
import jax
import jax.numpy as jnp
import numpy as np
from jax import lax
from jax.experimental import pallas as pl
from jax.experimental.pallas import tpu as pltpu
from jax.sharding import PartitionSpec as P

MESH = pl.DeviceIdType.MESH
F32 = jnp.float32
BF16 = jnp.bfloat16

X, Y, Z, ZALL = 4, 4, 8, 16
D = 1024
DK = 128
DV = 256
SEQ = 1024
OWN = 128
HALF = 64
PIECE = 32
BLOCK = 256
UNIT = 32
FFP = 384
FFOWN = 352
EPS = 1e-6
NT = (((1,), (1,)), ((), ()))
TN = (((0,), (0,)), ((), ()))


def rotation_tables():
    frequency = 10000.0 ** (-np.arange(64, dtype=np.float64) / 64)

    def pair(positions):
        angles = positions[:, None] * frequency[None, :]
        cosine, sine = np.cos(angles), np.sin(angles)
        return np.concatenate([cosine, cosine], 1), np.concatenate([-sine, sine], 1)

    inner = np.concatenate(pair(np.arange(BLOCK, dtype=np.float64)), 1)
    outer = np.concatenate(pair(BLOCK * np.repeat(np.arange(X, dtype=np.float64), 8)), 1)
    return inner.astype(np.float32), outer.astype(np.float32)


def dot(a, b, dims=None):
    if dims is None:
        return jnp.dot(a, b, preferred_element_type=F32)
    return lax.dot_general(a, b, dims, preferred_element_type=F32)


def rms(values, gain):
    return values * lax.rsqrt(jnp.mean(values * values, axis=-1, keepdims=True) + EPS) * gain


def kernel(
    h_tok, h_g_in, h_wq, h_wk, h_wv, h_wg, h_logits, h_wo, h_g_mo, h_g_ci, h_gelu, h_linear,
    h_k_gelu, h_k_linear, h_b_gelu, h_b_linear, h_wd, h_g_co, h_inner, h_outer,
    out,
    tok, g_in, logits, g_mo, g_ci, k_gelu, k_linear, bias_g, bias_l, g_co, inner, outer,
    s_u, s_l, s_d,
    xn, ch, b_q, b_g, b_u, b_kv, b_o, b_ld, qs, ins, us, st, dmat, lead, tail, pf, ps, pr, rs_send, rs_recv,
    ms_send, ms_recv, up, hid, after, taps,
    in_s, ag_s, ag_r, ay_s, ay_r, az_s, az_r, bz_s, bz_r, by_s, by_r, fz_s, fz_r, pp_s, pp_r, rr_s, rr_r, mm_s, mm_r,
):
    rep, fs, tp = lax.axis_index("rep"), lax.axis_index("fs"), lax.axis_index("tp")
    x, c = tp // 2, tp % 2
    z, y = fs // Y, fs % Y
    zz = rep * Z + z

    def x_dev(step):
        return (rep, fs, lax.rem(x + step, X) * 2 + c)

    def y_dev(step):
        return (rep, z * Y + lax.rem(y + step, Y), tp)

    def z_dev(step):
        there = lax.rem(zz + step, ZALL)
        return (there // Z, lax.rem(there, Z) * Y + y, tp)

    sibling = (rep, fs, x * 2 + (1 - c))
    x_next, x_prev = x_dev(1), x_dev(X - 1)
    y_next, y_prev, y_far = y_dev(1), y_dev(Y - 1), y_dev(2)
    z_next, z_prev = z_dev(1), z_dev(ZALL - 1)
    z_two = (z_dev(2), z_dev(ZALL - 2))

    barrier = pltpu.get_barrier_semaphore()
    for peer in (x_next, x_prev, sibling, y_next, y_prev, y_far, z_next, z_prev, *z_two):
        pl.semaphore_signal(barrier, inc=1, device_id=peer, device_id_type=MESH)

    def rows(first, count):
        return pl.ds(pl.multiple_of(first, count), count)

    own = rows(fs * UNIT, UNIT)
    loads = [
        pltpu.make_async_copy(src, dst, in_s.at[k])
        for k, (src, dst) in enumerate((
            (h_tok, tok), (h_g_in, g_in), (h_wq, b_q.at[own]), (h_wk, b_kv.at[own, 0:128]),
            (h_wv, b_kv.at[own, 128:384]), (h_wg, b_g.at[own]), (h_wo, b_o.at[own]), (h_logits, logits),
            (h_gelu, s_u), (h_linear, s_l), (h_wd, s_d), (h_k_gelu, k_gelu), (h_k_linear, k_linear),
            (h_b_gelu, bias_g), (h_b_linear, bias_l), (h_g_mo, g_mo), (h_g_ci, g_ci), (h_g_co, g_co),
            (h_inner, inner), (h_outer, outer),
        ))
    ]
    for load in loads:
        load.start()

    sent = []

    def send(src, dst, send_sem, recv_sem, peer):
        copy = pltpu.make_async_remote_copy(
            src_ref=src, dst_ref=dst, send_sem=send_sem, recv_sem=recv_sem,
            device_id=peer, device_id_type=MESH,
        )
        copy.start()
        sent.append(copy)

    def received(dst, send_sem, recv_sem):
        pltpu.make_async_remote_copy(
            src_ref=dst, dst_ref=dst, send_sem=send_sem, recv_sem=recv_sem,
            device_id=sibling, device_id_type=MESH,
        ).wait_recv()

    def ag_place(buf, d, core, p):
        chip = lax.rem(x + d, X)
        return buf.at[rows((chip * 2 + core) * OWN + p * PIECE, PIECE)]

    def ag_send(t, buf, k, d, p, peer):
        here = ag_place(buf, d, c, p)
        send(here, here, ag_s.at[t, k], ag_r.at[t, k], peer)

    def ag_wait(t, buf, k, d, core, p):
        received(ag_place(buf, d, core, p), ag_s.at[t, k], ag_r.at[t, k])

    def ag_start(t, buf, *pieces):
        for p in pieces:
            ag_send(t, buf, p, 0, p, x_next)
            ag_send(t, buf, 4 + p, 0, p, x_prev)
            ag_send(t, buf, 12 + p, 0, p, sibling)

    def ag_first(t, buf, *pieces):
        for p in pieces:
            ag_wait(t, buf, p, 3, c, p)
            if p < 2:
                ag_send(t, buf, 8 + p, 3, p, x_next)
            ag_send(t, buf, 24 + p, 3, p, sibling)
            ag_wait(t, buf, 4 + p, 1, c, p)
            if p >= 2:
                ag_send(t, buf, 8 + p, 1, p, x_prev)
            ag_send(t, buf, 16 + p, 1, p, sibling)

    def ag_second(t, buf, *pieces):
        for p in pieces:
            ag_wait(t, buf, 8 + p, 2, c, p)
            ag_send(t, buf, 20 + p, 2, p, sibling)

    def ag_sibling(t, buf, d):
        for p in range(4):
            ag_wait(t, buf, 12 + 4 * d + p, d, 1 - c, p)

    class FastZ:
        def hop(self, off, k, peer, piece=None):
            here = self.piece(off, piece)
            send(here, here, fz_s.at[self.f, k], fz_r.at[self.f, k], peer)

        def landed(self, off, k, piece=None):
            received(self.piece(off, piece), fz_s.at[self.f, k], fz_r.at[self.f, k])

        def fast_start(self):
            for way, one, two in ((0, z_next, z_two[0]), (1, z_prev, z_two[1])):
                self.hop(0, way * 4 + 1, two)
                self.hop(0, way * 4, one)

        def fast_one(self):
            self.landed(-1, 0)
            self.landed(1, 4)

        def fast_relay(self):
            self.landed(-2, 1)
            self.hop(-2, 3, z_two[0], 0)
            self.hop(-2, 2, z_next)
            self.landed(2, 5)
            self.hop(2, 7, z_two[1], 1)
            self.hop(2, 6, z_prev)

        def fast_end(self):
            self.landed(-3, 2)
            self.landed(3, 6)
            self.landed(4, 3, 0)
            self.landed(4, 7, 1)

    class OverYZ(FastZ):
        def __init__(self, n, buf, f=None):
            self.n, self.buf, self.f = n, buf, f

        def piece(self, off, half):
            first = lax.rem(z + off + Z, Z) * (Y * UNIT)
            if half is None:
                return self.buf.at[rows(first, Y * UNIT)]
            return self.buf.at[rows(first + half * HALF, HALF)]

        def y_start(self):
            here = self.buf.at[rows(fs * UNIT, UNIT)]
            for k, peer in ((0, y_next), (1, y_prev), (2, y_far)):
                send(here, here, ay_s.at[self.n, k], ay_r.at[self.n, k], peer)

        def y_wait(self):
            for k, step in ((0, Y - 1), (1, 1), (2, 2)):
                there = self.buf.at[rows((z * Y + lax.rem(y + step, Y)) * UNIT, UNIT)]
                received(there, ay_s.at[self.n, k], ay_r.at[self.n, k])

        def slab(self, off, half):
            first = lax.rem(z + off + Z, Z) * (Y * UNIT) + half * HALF
            return self.buf.at[rows(first, HALF)]

        def z_send(self, s, half, way):
            here = self.slab(-(s - 1) if way == 0 else s - 1, half)
            k = way * 8 + (s - 1) * 2 + half
            peer = z_next if way == 0 else z_prev
            send(here, here, az_s.at[self.n, k], az_r.at[self.n, k], peer)

        def z_wait(self, s, half, way):
            k = way * 8 + (s - 1) * 2 + half
            there = self.slab(-s if way == 0 else s, half)
            received(there, az_s.at[self.n, k], az_r.at[self.n, k])

        def z_start(self):
            self.y_wait()
            for half in (0, 1):
                for way in (0, 1):
                    self.z_send(1, half, way)

        def z_step(self, s):
            for half in (0, 1):
                for way in (0, 1):
                    self.z_wait(s, half, way)
                    if s < 3 or half == way:
                        self.z_send(s + 1, half, way)

        def z_end(self):
            for way in (0, 1):
                self.z_wait(4, way, way)

    offsets = (0, -1, 1, -2, 2, -3, 3, 4)

    class OverZY(FastZ):
        def __init__(self, n, buf, f=None):
            self.n, self.buf, self.f = n, buf, f

        def piece(self, off, half):
            first = self.unit(off, 0)
            if half is None:
                return self.buf.at[rows(first, UNIT)]
            return self.buf.at[rows(first + half * 16, 16)]

        def unit(self, off, y_step):
            return (lax.rem(z + off + Z, Z) * Y + lax.rem(y + y_step, Y)) * UNIT

        def z_part(self, off, s, way):
            if s == 4:
                return self.buf.at[rows(self.unit(off, 0) + way * 16, 16)]
            return self.buf.at[rows(self.unit(off, 0), UNIT)]

        def z_send(self, s, way):
            here = self.z_part(-(s - 1) if way == 0 else s - 1, s, way)
            k = way * 4 + s - 1
            peer = z_next if way == 0 else z_prev
            send(here, here, bz_s.at[self.n, k], bz_r.at[self.n, k], peer)

        def z_start(self):
            self.z_send(1, 0)
            self.z_send(1, 1)

        def z_step(self, s):
            for way in (0, 1):
                there = self.z_part(-s if way == 0 else s, s, way)
                received(there, bz_s.at[self.n, way * 4 + s - 1], bz_r.at[self.n, way * 4 + s - 1])
                if s < 4:
                    self.z_send(s + 1, way)
            self.y_start(*((2 * s - 1, 2 * s) if s < 4 else (7,)))

        def y_send(self, j, k, y_step, peer):
            here = self.buf.at[rows(self.unit(offsets[j], y_step), UNIT)]
            send(here, here, by_s.at[self.n, j, k], by_r.at[self.n, j, k], peer)

        def y_wait(self, j, k, y_step):
            there = self.buf.at[rows(self.unit(offsets[j], y_step), UNIT)]
            received(there, by_s.at[self.n, j, k], by_r.at[self.n, j, k])

        def y_start(self, *slots):
            for j in slots:
                self.y_send(j, 0, 0, y_next)
                self.y_send(j, 1, 0, y_prev)

        def y_relay(self, *slots):
            for j in slots:
                if j % 2 == 0:
                    self.y_wait(j, 0, 3)
                    self.y_send(j, 2, 3, y_next)
                    self.y_wait(j, 1, 1)
                else:
                    self.y_wait(j, 1, 1)
                    self.y_send(j, 2, 1, y_prev)
                    self.y_wait(j, 0, 3)

        def y_end(self, *slots):
            for j in slots:
                self.y_wait(j, 2, 2)

    w_q, w_g, w_u = OverYZ(0, b_q, 0), OverYZ(1, b_g), OverYZ(2, b_u)
    w_kv, w_o, w_ld = OverZY(0, b_kv, 1), OverZY(1, b_o, 2), OverZY(2, b_ld)

    for k in (0, 1, 2, 3, 4, 5, 6, 7):
        loads[k].wait()
    tokens = tok[...].astype(F32)
    xn[rows(tp * OWN, OWN)] = rms(tokens, g_in[...]).astype(BF16)
    for k in range(8, len(loads)):
        loads[k].wait()
    b_u[own] = jnp.zeros((UNIT, FFP), BF16)
    b_u[own, 0:FFOWN] = s_u[...]
    b_ld[own] = jnp.zeros((UNIT, 2 * FFP), BF16)
    b_ld[own, 0:FFOWN] = s_l[...]
    b_ld[own, FFP : FFP + FFOWN] = s_d[...]

    pl.semaphore_wait(barrier, 10)

    ag_start(0, xn, 0, 2)
    w_q.y_start()
    w_kv.fast_start()
    w_kv.y_start(0)
    ag_start(0, xn, 1, 3)
    w_o.fast_start()
    w_g.y_start()

    log_f = -jnp.log1p(jnp.exp(-logits[0:1, 0:1]))
    log_b = -jnp.log1p(jnp.exp(-logits[0:1, 1:2]))
    at = lax.broadcasted_iota(jnp.int32, (BLOCK, BLOCK), 0)
    lane = lax.broadcasted_iota(jnp.int32, (BLOCK, BLOCK), 1)
    apart = (at - lane).astype(F32)
    dmat[...] = jnp.exp(jnp.where(at >= lane, apart * log_f, -apart * log_b))
    ahead = at.astype(F32)
    lead[...] = jnp.exp(
        jnp.where(lane < DK, (ahead + 1.0) * log_f, (float(BLOCK) - ahead) * log_b)
    )
    tail[...] = jnp.exp(jnp.where(lane < DK, (BLOCK - 1.0 - ahead) * log_f, ahead * log_b))
    step_f, step_b = jnp.exp(BLOCK * log_f), jnp.exp(BLOCK * log_b)
    taps[...] = jnp.zeros((16, FFP), F32)
    taps[0:3, 0:FFOWN] = k_gelu[...]
    taps[3:4, 0:FFOWN] = bias_g[...].reshape(1, FFOWN)
    taps[8:11, 0:FFOWN] = k_linear[...]
    taps[11:12, 0:FFOWN] = bias_l[...].reshape(1, FFOWN)
    up[0:8] = jnp.zeros((8, 2 * FFP), F32)
    up[SEQ + 8 : SEQ + 16] = jnp.zeros((8, 2 * FFP), F32)

    w_q.y_wait()
    w_q.fast_start()
    w_kv.fast_one()
    w_kv.fast_relay()
    w_kv.y_start(1, 2, 3, 4)
    ag_first(0, xn, 0, 2)
    w_o.fast_one()
    w_o.fast_relay()
    w_g.z_start()
    w_kv.y_relay(0)
    w_o.y_start(0, 1, 2)
    ag_first(0, xn, 1, 3)
    w_q.fast_relay()
    w_kv.y_relay(1, 2, 3, 4)
    w_kv.fast_end()
    w_kv.y_start(5, 6, 7)
    w_g.z_step(1)
    w_o.y_start(3, 4)
    w_o.fast_end()
    w_o.y_start(5, 6, 7)
    w_ld.z_start()
    w_u.y_start()
    w_ld.y_start(0)
    ag_second(0, xn, 0, 2, 1, 3)
    ag_sibling(0, xn, 0)
    ag_sibling(0, xn, 1)
    ag_sibling(0, xn, 3)
    w_q.fast_one()
    w_q.fast_end()
    w_kv.y_relay(5, 6, 7)
    w_o.y_relay(0, 1, 2, 3, 4)
    w_g.z_step(2)
    ag_sibling(0, xn, 2)
    w_kv.y_end(*range(8))

    def between_qkv(n):
        if n == 0:
            w_ld.z_step(1)
        elif n == 1:
            w_o.y_relay(5, 6, 7)
        elif n == 2:
            w_g.z_step(3)
        else:
            w_u.z_start()
            w_ld.y_relay(0)

    def between_mixer(n):
        if n == 0:
            w_ld.z_step(2)
        elif n == 1:
            w_ld.y_relay(1, 2)
        elif n == 2:
            w_u.z_step(1)
        else:
            w_ld.z_step(3)

    for n, d in enumerate((0, 1, 3, 2)):
        i = lax.rem(x + d, X)
        here = rows(i * BLOCK, BLOCK)
        base = outer[rows(i * 8, 8)][0:1]
        base_cos, base_sin = base[:, 0:128], base[:, 128:256]
        cosine = base_cos * inner[:, 0:128] - base_sin * inner[:, 128:256]
        sine = base_sin * inner[:, 0:128] + base_cos * inner[:, 128:256]
        q = dot(xn[here], b_q[...])
        kv = dot(xn[here], b_kv[...])
        k = kv[:, 0:128]
        q = (q * cosine + pltpu.roll(q, 64, 1) * sine).astype(BF16)
        k = ((k * cosine + pltpu.roll(k, 64, 1) * sine) * DK**-0.5).astype(BF16)
        qs[here] = q
        v = kv[:, 128:384].astype(BF16)
        scores = (dot(q, k, NT) * dmat[...]).astype(BF16)
        ins[here] = dot(scores, v)
        kf = k.astype(F32)
        k_two = (jnp.concatenate([kf, kf], axis=1) * tail[...]).astype(BF16)
        us[here] = dot(k_two, v, TN)
        between_qkv(n)

    total = jnp.zeros((DK, DV), F32)
    for i in range(X):
        st[i * BLOCK : i * BLOCK + DK] = total.astype(BF16)
        total = step_f * total + us[i * BLOCK : i * BLOCK + DK]
    total = jnp.zeros((DK, DV), F32)
    for i in reversed(range(X)):
        st[i * BLOCK + DK : (i + 1) * BLOCK] = total.astype(BF16)
        total = step_b * total + us[i * BLOCK + DK : (i + 1) * BLOCK]

    w_g.z_end()
    w_o.y_end(*range(8))

    def rs_block(t, d, left, weights, first, width):
        for j in range(4):
            part = dot(left, weights[j * 256 : (j + 1) * 256, first : first + width], NT)
            pf[d * BLOCK : (d + 1) * BLOCK, j * 256 : (j + 1) * 256] = part
            ps[t, d * BLOCK : (d + 1) * BLOCK, j * 256 : (j + 1) * 256] = part.astype(BF16)
        send(
            ps.at[t, rows(d * BLOCK + (1 - c) * OWN, OWN)],
            pr.at[t, d], pp_s.at[t, d], pp_r.at[t, d], sibling,
        )

    def rs_pair_wait(t, d):
        received(pr.at[t, d], pp_s.at[t, d], pp_r.at[t, d])

    def rs_pair(t, d, p):
        mine = pf[rows(d * BLOCK + c * OWN + p * PIECE, PIECE)]
        return mine + pr[t, d, p * PIECE : (p + 1) * PIECE].astype(F32)

    def rs_far(t):
        rs_pair_wait(t, 2)
        for p in (0, 2, 1, 3):
            rs_send[t, p] = rs_pair(t, 2, p).astype(BF16)
            peer = x_next if p < 2 else x_prev
            send(rs_send.at[t, p], rs_recv.at[t, p], rr_s.at[t, p], rr_r.at[t, p], peer)

    def rs_near(t, way, p, relay):
        total = rs_pair(t, 1 if way == 0 else 3, p)
        if relay:
            received(rs_recv.at[t, p], rr_s.at[t, p], rr_r.at[t, p])
            total = total + rs_recv[t, p].astype(F32)
        k = way * 4 + p
        ms_send[t, k] = total.astype(BF16)
        peer = x_next if way == 0 else x_prev
        send(ms_send.at[t, k], ms_recv.at[t, k], mm_s.at[t, k], mm_r.at[t, k], peer)

    def rs_final(t, p):
        total = rs_pair(t, 0, p)
        for k in (p, 4 + p):
            received(ms_recv.at[t, k], mm_s.at[t, k], mm_r.at[t, k])
            total = total + ms_recv[t, k].astype(F32)
        return total

    def reduce_scatter(t, block, weights, first, width, between):
        for n, d in enumerate((2, 1, 3, 0)):
            rs_block(t, d, block(d), weights, first, width)
            if n == 1:
                rs_far(t)
            if n == 2:
                rs_pair_wait(t, 1)
                rs_near(t, 0, 2, False)
                rs_near(t, 0, 3, False)
            if n == 3:
                rs_pair_wait(t, 3)
                rs_near(t, 1, 0, False)
                rs_near(t, 1, 1, False)
            between(n)
        for p in (0, 2, 1, 3):
            rs_near(t, 0 if p < 2 else 1, p, True)
        rs_pair_wait(t, 0)

    def mixer_block(d):
        i = lax.rem(x + d, X)
        here = rows(i * BLOCK, BLOCK)
        q = qs[here].astype(F32)
        q_two = (jnp.concatenate([q, q], axis=1) * lead[...]).astype(BF16)
        retained = ins[here] + dot(q_two, st[here])
        centred = retained - jnp.mean(retained, axis=-1, keepdims=True)
        normal = centred * lax.rsqrt(jnp.mean(centred * centred, axis=-1, keepdims=True) + EPS)
        gates = dot(xn[here], b_g[...])
        return (normal * (gates / (1.0 + jnp.exp(-gates)))).astype(BF16)

    reduce_scatter(0, mixer_block, b_o, 0, 256, between_mixer)
    for p in (0, 2, 1, 3):
        part = slice(p * PIECE, (p + 1) * PIECE)
        mixed = rs_final(0, p)
        summed = (tok[part].astype(F32) + rms(mixed, g_mo[...])).astype(BF16).astype(F32)
        after[part] = summed
        ch[rows(tp * OWN + p * PIECE, PIECE)] = rms(summed, g_ci[...]).astype(BF16)
        ag_start(1, ch, p)

    w_ld.z_step(4)
    w_u.z_step(2)
    w_ld.y_relay(3, 4)
    ag_first(1, ch, 0, 2)
    w_ld.y_relay(5, 6)
    w_u.z_step(3)
    w_ld.y_relay(7)
    ag_first(1, ch, 1, 3)
    w_u.z_end()
    w_ld.y_end(*range(8))
    ag_second(1, ch, 0, 2, 1, 3)

    for d in (0, 1, 3, 2):
        ag_sibling(1, ch, d)
        i = lax.rem(x + d, X)
        there = pl.ds(pl.multiple_of(i * BLOCK + 8, 8), BLOCK)
        up[there, 0:FFP] = dot(ch[rows(i * BLOCK, BLOCK)], b_u[...])
        up[there, FFP:] = dot(ch[rows(i * BLOCK, BLOCK)], b_ld[:, 0:FFP])

    def conv(first, column, at):
        near = up[pl.ds(pl.multiple_of(first, 8), 80), column : column + FFP]
        before = pltpu.roll(near, 1, 0)[8:72]
        behind = pltpu.roll(near, 79, 0)[8:72]
        return (
            taps[at : at + 1] * before
            + taps[at + 1 : at + 2] * near[8:72]
            + taps[at + 2 : at + 3] * behind
            + taps[at + 3 : at + 4]
        )

    def channel_block(d):
        i = lax.rem(x + d, X)

        def tile(n, carry):
            first = i * BLOCK + n * HALF
            g = conv(first, 0, 0)
            act = 0.5 * g * (1.0 + jnp.tanh(0.7978845608028654 * (g + 0.044715 * g * g * g)))
            hid[pl.ds(pl.multiple_of(n * HALF, HALF), HALF)] = (
                act * conv(first, FFP, 8)
            ).astype(BF16)
            return carry

        lax.fori_loop(0, BLOCK // HALF, tile, 0)
        return hid[...]

    reduce_scatter(1, channel_block, b_ld, FFP, FFP, lambda n: None)
    for p in (0, 2, 1, 3):
        part = slice(p * PIECE, (p + 1) * PIECE)
        out[part] = (after[part] + rms(rs_final(1, p), g_co[...])).astype(BF16)

    for copy in sent:
        copy.wait_send()


def layer(
    tokens, mixer_in_gain, query_weight, key_weight, value_weight, gate_weight, decay_logits,
    mixer_output, mixer_out_gain, channel_in_gain, gelu_weight, linear_weight, gelu_kernel,
    linear_kernel, gelu_bias, linear_bias, down_weight, channel_out_gain,
):
    inner, outer = rotation_tables()

    def row(v):
        return v.reshape(1, -1)

    operands = (
        tokens[0], row(mixer_in_gain), query_weight, key_weight, value_weight, gate_weight,
        decay_logits.T, mixer_output.T, row(mixer_out_gain), row(channel_in_gain), gelu_weight,
        linear_weight, gelu_kernel, linear_kernel, gelu_bias, linear_bias, down_weight.T,
        row(channel_out_gain), jnp.asarray(inner), jnp.asarray(outer),
    )
    dma = pltpu.SemaphoreType.DMA
    result = pl.pallas_call(
        kernel,
        out_shape=jax.ShapeDtypeStruct((OWN, D), BF16),
        in_specs=[pl.BlockSpec(memory_space=pl.ANY)] * len(operands),
        out_specs=pl.BlockSpec(memory_space=pltpu.VMEM),
        scratch_shapes=[
            pltpu.VMEM((OWN, D), BF16),
            pltpu.VMEM((1, D), F32),
            pltpu.VMEM((1, 2), F32),
            pltpu.VMEM((1, D), F32),
            pltpu.VMEM((1, D), F32),
            pltpu.VMEM((3, FFOWN), F32),
            pltpu.VMEM((3, FFOWN), F32),
            pltpu.VMEM((FFOWN,), F32),
            pltpu.VMEM((FFOWN,), F32),
            pltpu.VMEM((1, D), F32),
            pltpu.VMEM((BLOCK, 256), F32),
            pltpu.VMEM((8 * X, 256), F32),
            pltpu.VMEM((UNIT, FFOWN), BF16),
            pltpu.VMEM((UNIT, FFOWN), BF16),
            pltpu.VMEM((UNIT, FFOWN), BF16),
            pltpu.VMEM((SEQ, D), BF16),
            pltpu.VMEM((SEQ, D), BF16),
            pltpu.VMEM((D, 128), BF16),
            pltpu.VMEM((D, 256), BF16),
            pltpu.VMEM((D, FFP), BF16),
            pltpu.VMEM((D, 384), BF16),
            pltpu.VMEM((D, 256), BF16),
            pltpu.VMEM((D, 2 * FFP), BF16),
            pltpu.VMEM((SEQ, DK), BF16),
            pltpu.VMEM((SEQ, DV), F32),
            pltpu.VMEM((SEQ, DV), F32),
            pltpu.VMEM((SEQ, DV), BF16),
            pltpu.VMEM((BLOCK, BLOCK), F32),
            pltpu.VMEM((BLOCK, BLOCK), F32),
            pltpu.VMEM((BLOCK, BLOCK), F32),
            pltpu.VMEM((SEQ, D), F32),
            pltpu.VMEM((2, SEQ, D), BF16),
            pltpu.VMEM((2, 4, OWN, D), BF16),
            pltpu.VMEM((2, 4, PIECE, D), BF16),
            pltpu.VMEM((2, 4, PIECE, D), BF16),
            pltpu.VMEM((2, 8, PIECE, D), BF16),
            pltpu.VMEM((2, 8, PIECE, D), BF16),
            pltpu.VMEM((SEQ + 16, 2 * FFP), F32),
            pltpu.VMEM((BLOCK, FFP), BF16),
            pltpu.VMEM((OWN, D), F32),
            pltpu.VMEM((16, FFP), F32),
            dma((20,)),
            dma((2, 28)), dma((2, 28)),
            dma((3, 3)), dma((3, 3)),
            dma((3, 16)), dma((3, 16)),
            dma((3, 8)), dma((3, 8)),
            dma((3, 8, 3)), dma((3, 8, 3)),
            dma((3, 8)), dma((3, 8)),
            dma((2, 4)), dma((2, 4)),
            dma((2, 4)), dma((2, 4)),
            dma((2, 8)), dma((2, 8)),
        ],
        compiler_params=pltpu.CompilerParams(
            collective_id=0, has_side_effects=True, vmem_limit_bytes=60 * 1024 * 1024
        ),
        name="layer",
    )(*operands)
    return result[None]


def solution(mesh):
    by_position = P(("rep", "fs"), "tp", None)
    up_rows, down_rows = P("fs", "tp"), P("tp", "fs")
    in_specs = (
        by_position, P(), up_rows, up_rows, up_rows, up_rows, P(None, "tp"), down_rows, P(), P(),
        up_rows, up_rows, P(None, "tp"), P(None, "tp"), P("tp"), P("tp"), down_rows, P(),
    )
    return jax.shard_map(
        layer, mesh=mesh, in_specs=in_specs, out_specs=by_position, check_vma=False
    )
```

```python
import jax
import jax.numpy as jnp
import numpy as np
from jax import lax
from jax.experimental import pallas as pl
from jax.experimental.pallas import tpu as pltpu
from jax.sharding import PartitionSpec as P

MESH = pl.DeviceIdType.MESH
F32 = jnp.float32
BF16 = jnp.bfloat16

X, Y, Z, ZALL = 4, 4, 8, 16
D = 1024
DK = 128
DV = 256
SEQ = 1024
OWN = 128
HALF = 64
PIECE = 32
BLOCK = 256
UNIT = 32
FFP = 384
FFOWN = 352
EPS = 1e-6
NT = (((1,), (1,)), ((), ()))
TN = (((0,), (0,)), ((), ()))


def rotation_tables():
    frequency = 10000.0 ** (-np.arange(64, dtype=np.float64) / 64)

    def pair(positions):
        angles = positions[:, None] * frequency[None, :]
        cosine, sine = np.cos(angles), np.sin(angles)
        return np.concatenate([cosine, cosine], 1), np.concatenate([-sine, sine], 1)

    inner = np.concatenate(pair(np.arange(BLOCK, dtype=np.float64)), 1)
    outer = np.concatenate(pair(BLOCK * np.repeat(np.arange(X, dtype=np.float64), 8)), 1)
    return inner.astype(np.float32), outer.astype(np.float32)


def dot(a, b, dims=None):
    if dims is None:
        return jnp.dot(a, b, preferred_element_type=F32)
    return lax.dot_general(a, b, dims, preferred_element_type=F32)


def rms(values, gain):
    return values * lax.rsqrt(jnp.mean(values * values, axis=-1, keepdims=True) + EPS) * gain


def kernel(
    h_tok, h_g_in, h_wq, h_wk, h_wv, h_wg, h_logits, h_wo, h_g_mo, h_g_ci, h_gelu, h_linear,
    h_k_gelu, h_k_linear, h_b_gelu, h_b_linear, h_wd, h_g_co, h_inner, h_outer,
    out,
    tok, g_in, logits, g_mo, g_ci, k_gelu, k_linear, bias_g, bias_l, g_co, inner, outer,
    s_u, s_l, s_d,
    xn, ch, b_k, b_g, b_u, b_v, b_qo, b_ld, ks, vs, us, st, dmat, lead, tail, pf, ps, pr, rs_send, rs_recv,
    ms_send, ms_recv, up, hid, after, taps,
    in_s, ag_s, ag_r, ay_s, ay_r, by_s, by_r, fz_s, fz_r, pp_s, pp_r, rr_s, rr_r, mm_s, mm_r,
):
    rep, fs, tp = lax.axis_index("rep"), lax.axis_index("fs"), lax.axis_index("tp")
    x, c = tp // 2, tp % 2
    z, y = fs // Y, fs % Y
    zz = rep * Z + z

    def x_dev(step):
        return (rep, fs, lax.rem(x + step, X) * 2 + c)

    def y_dev(step):
        return (rep, z * Y + lax.rem(y + step, Y), tp)

    def z_dev(step):
        there = lax.rem(zz + step, ZALL)
        return (there // Z, lax.rem(there, Z) * Y + y, tp)

    sibling = (rep, fs, x * 2 + (1 - c))
    x_next, x_prev = x_dev(1), x_dev(X - 1)
    y_next, y_prev, y_far = y_dev(1), y_dev(Y - 1), y_dev(2)
    z_next, z_prev = z_dev(1), z_dev(ZALL - 1)
    z_two = (z_dev(2), z_dev(ZALL - 2))

    barrier = pltpu.get_barrier_semaphore()
    for peer in (x_next, x_prev, sibling, y_next, y_prev, y_far, z_next, z_prev, *z_two):
        pl.semaphore_signal(barrier, inc=1, device_id=peer, device_id_type=MESH)

    def rows(first, count):
        return pl.ds(pl.multiple_of(first, count), count)

    own = rows(fs * UNIT, UNIT)
    loads = [
        pltpu.make_async_copy(src, dst, in_s.at[k])
        for k, (src, dst) in enumerate((
            (h_tok, tok), (h_g_in, g_in), (h_wq, b_qo.at[own, 0:128]), (h_wk, b_k.at[own]),
            (h_wv, b_v.at[own]), (h_wg, b_g.at[own]), (h_wo, b_qo.at[own, 128:384]), (h_logits, logits),
            (h_gelu, s_u), (h_linear, s_l), (h_wd, s_d), (h_k_gelu, k_gelu), (h_k_linear, k_linear),
            (h_b_gelu, bias_g), (h_b_linear, bias_l), (h_g_mo, g_mo), (h_g_ci, g_ci), (h_g_co, g_co),
            (h_inner, inner), (h_outer, outer),
        ))
    ]
    for load in loads:
        load.start()

    sent = []

    def send(src, dst, send_sem, recv_sem, peer):
        copy = pltpu.make_async_remote_copy(
            src_ref=src, dst_ref=dst, send_sem=send_sem, recv_sem=recv_sem,
            device_id=peer, device_id_type=MESH,
        )
        copy.start()
        sent.append(copy)

    def received(dst, send_sem, recv_sem):
        pltpu.make_async_remote_copy(
            src_ref=dst, dst_ref=dst, send_sem=send_sem, recv_sem=recv_sem,
            device_id=sibling, device_id_type=MESH,
        ).wait_recv()

    def ag_place(buf, d, core, p):
        chip = lax.rem(x + d, X)
        return buf.at[rows((chip * 2 + core) * OWN + p * PIECE, PIECE)]

    def ag_send(t, buf, k, d, p, peer):
        here = ag_place(buf, d, c, p)
        send(here, here, ag_s.at[t, k], ag_r.at[t, k], peer)

    def ag_wait(t, buf, k, d, core, p):
        received(ag_place(buf, d, core, p), ag_s.at[t, k], ag_r.at[t, k])

    def ag_start(t, buf, *pieces):
        for p in pieces:
            ag_send(t, buf, p, 0, p, x_next)
            ag_send(t, buf, 4 + p, 0, p, x_prev)
            ag_send(t, buf, 12 + p, 0, p, sibling)

    def ag_first(t, buf, *pieces):
        for p in pieces:
            ag_wait(t, buf, p, 3, c, p)
            if p < 2:
                ag_send(t, buf, 8 + p, 3, p, x_next)
            ag_send(t, buf, 24 + p, 3, p, sibling)
            ag_wait(t, buf, 4 + p, 1, c, p)
            if p >= 2:
                ag_send(t, buf, 8 + p, 1, p, x_prev)
            ag_send(t, buf, 16 + p, 1, p, sibling)

    def ag_second(t, buf, *pieces):
        for p in pieces:
            ag_wait(t, buf, 8 + p, 2, c, p)
            ag_send(t, buf, 20 + p, 2, p, sibling)

    def ag_sibling(t, buf, d):
        for p in range(4):
            ag_wait(t, buf, 12 + 4 * d + p, d, 1 - c, p)

    class FastZ:
        def hop(self, off, k, peer, piece=None):
            here = self.piece(off, piece)
            send(here, here, fz_s.at[self.f, k], fz_r.at[self.f, k], peer)

        def landed(self, off, k, piece=None):
            received(self.piece(off, piece), fz_s.at[self.f, k], fz_r.at[self.f, k])

        def start_two(self):
            self.hop(0, 1, z_two[0])
            self.hop(0, 5, z_two[1])

        def start_one(self):
            self.hop(0, 0, z_next)
            self.hop(0, 4, z_prev)

        def fast_start(self):
            self.start_two()
            self.start_one()

        def fast_one(self):
            self.landed(-1, 0)
            self.landed(1, 4)

        def fast_relay(self):
            self.landed(-2, 1)
            self.hop(-2, 3, z_two[0], 0)
            self.hop(-2, 2, z_next)
            self.landed(2, 5)
            self.hop(2, 7, z_two[1], 1)
            self.hop(2, 6, z_prev)

        def fast_end(self):
            self.landed(-3, 2)
            self.landed(3, 6)
            self.landed(4, 3, 0)
            self.landed(4, 7, 1)

    class OverYZ(FastZ):
        def __init__(self, n, buf, f=None):
            self.n, self.buf, self.f = n, buf, f

        def piece(self, off, half):
            first = lax.rem(z + off + Z, Z) * (Y * UNIT)
            if half is None:
                return self.buf.at[rows(first, Y * UNIT)]
            return self.buf.at[rows(first + half * HALF, HALF)]

        def y_start(self):
            here = self.buf.at[rows(fs * UNIT, UNIT)]
            for k, peer in ((0, y_next), (1, y_prev), (2, y_far)):
                send(here, here, ay_s.at[self.n, k], ay_r.at[self.n, k], peer)

        def y_wait(self):
            for k, step in ((0, Y - 1), (1, 1), (2, 2)):
                there = self.buf.at[rows((z * Y + lax.rem(y + step, Y)) * UNIT, UNIT)]
                received(there, ay_s.at[self.n, k], ay_r.at[self.n, k])

    offsets = (0, -1, 1, -2, 2, -3, 3, 4)

    class OverZY(FastZ):
        def __init__(self, n, buf, f=None):
            self.n, self.buf, self.f = n, buf, f

        def piece(self, off, half):
            first = self.unit(off, 0)
            if half is None:
                return self.buf.at[rows(first, UNIT)]
            return self.buf.at[rows(first + half * 16, 16)]

        def unit(self, off, y_step):
            return (lax.rem(z + off + Z, Z) * Y + lax.rem(y + y_step, Y)) * UNIT

        def y_send(self, j, k, y_step, peer):
            here = self.buf.at[rows(self.unit(offsets[j], y_step), UNIT)]
            send(here, here, by_s.at[self.n, j, k], by_r.at[self.n, j, k], peer)

        def y_wait(self, j, k, y_step):
            there = self.buf.at[rows(self.unit(offsets[j], y_step), UNIT)]
            received(there, by_s.at[self.n, j, k], by_r.at[self.n, j, k])

        def y_start(self, *slots):
            for j in slots:
                self.y_send(j, 0, 0, y_next)
                self.y_send(j, 1, 0, y_prev)

        def y_relay(self, *slots):
            for j in slots:
                if j % 2 == 0:
                    self.y_wait(j, 0, 3)
                    self.y_send(j, 2, 3, y_next)
                    self.y_wait(j, 1, 1)
                else:
                    self.y_wait(j, 1, 1)
                    self.y_send(j, 2, 1, y_prev)
                    self.y_wait(j, 0, 3)

        def y_end(self, *slots):
            for j in slots:
                self.y_wait(j, 2, 2)

    w_k, w_g, w_u = OverYZ(0, b_k, 0), OverYZ(1, b_g, 1), OverYZ(2, b_u, 2)
    w_v, w_qo, w_ld = OverZY(0, b_v, 3), OverZY(1, b_qo, 4), OverZY(2, b_ld, 5)

    for k in (0, 1, 2, 3, 4, 5, 6, 7):
        loads[k].wait()
    tokens = tok[...].astype(F32)
    xn[rows(tp * OWN, OWN)] = rms(tokens, g_in[...]).astype(BF16)
    for k in range(8, len(loads)):
        loads[k].wait()
    b_u[own] = jnp.zeros((UNIT, FFP), BF16)
    b_u[own, 0:FFOWN] = s_u[...]
    b_ld[own] = jnp.zeros((UNIT, 2 * FFP), BF16)
    b_ld[own, 0:FFOWN] = s_l[...]
    b_ld[own, FFP : FFP + FFOWN] = s_d[...]

    pl.semaphore_wait(barrier, 10)

    ag_start(0, xn, 0, 2)
    w_v.fast_start()
    w_k.y_start()
    w_v.y_start(0)
    ag_start(0, xn, 1, 3)
    w_qo.fast_start()
    w_g.y_start()
    w_qo.y_start(0)

    log_f = -jnp.log1p(jnp.exp(-logits[0:1, 0:1]))
    log_b = -jnp.log1p(jnp.exp(-logits[0:1, 1:2]))
    at = lax.broadcasted_iota(jnp.int32, (BLOCK, BLOCK), 0)
    lane = lax.broadcasted_iota(jnp.int32, (BLOCK, BLOCK), 1)
    apart = (at - lane).astype(F32)
    dmat[...] = jnp.exp(jnp.where(at >= lane, apart * log_f, -apart * log_b))
    ahead = at.astype(F32)
    lead[...] = jnp.exp(
        jnp.where(lane < DK, (ahead + 1.0) * log_f, (float(BLOCK) - ahead) * log_b)
    )
    tail[...] = jnp.exp(jnp.where(lane < DK, (BLOCK - 1.0 - ahead) * log_f, ahead * log_b))
    step_f, step_b = jnp.exp(BLOCK * log_f), jnp.exp(BLOCK * log_b)
    taps[...] = jnp.zeros((16, FFP), F32)
    taps[0:3, 0:FFOWN] = k_gelu[...]
    taps[3:4, 0:FFOWN] = bias_g[...].reshape(1, FFOWN)
    taps[8:11, 0:FFOWN] = k_linear[...]
    taps[11:12, 0:FFOWN] = bias_l[...].reshape(1, FFOWN)
    up[0:8] = jnp.zeros((8, 2 * FFP), F32)
    up[SEQ + 8 : SEQ + 16] = jnp.zeros((8, 2 * FFP), F32)

    w_v.fast_relay()
    w_v.fast_one()
    w_v.y_start(1, 2, 3, 4)
    w_k.y_wait()
    w_k.fast_start()
    ag_first(0, xn, 0, 2)
    w_qo.fast_relay()
    w_qo.fast_one()
    w_qo.y_start(1, 2, 3, 4)
    w_g.y_wait()
    w_g.start_two()
    w_v.y_relay(0)
    ag_first(0, xn, 1, 3)
    w_v.fast_end()
    w_v.y_start(5, 6, 7)
    w_v.y_relay(1, 2, 3, 4)
    w_qo.y_relay(0)
    w_k.fast_relay()
    w_g.start_one()
    w_qo.fast_end()
    w_qo.y_start(5, 6, 7)
    ag_second(0, xn, 0, 2)
    w_v.y_relay(5, 6, 7)
    ag_second(0, xn, 1, 3)
    w_qo.y_relay(1, 2, 3, 4)
    w_g.fast_relay()
    ag_sibling(0, xn, 0)
    ag_sibling(0, xn, 1)
    ag_sibling(0, xn, 3)
    ag_sibling(0, xn, 2)
    w_k.fast_one()
    w_k.fast_end()
    w_v.y_end(*range(8))

    def between_keys(n):
        if n == 0:
            w_qo.y_relay(5, 6, 7)
            w_u.y_start()
            w_ld.fast_start()
        elif n == 2:
            w_ld.y_start(0)

    def between_mixer(n):
        if n == 0:
            w_ld.fast_relay()
            w_u.y_wait()
            w_u.fast_start()
        elif n == 1:
            w_ld.fast_one()
            w_ld.y_start(1, 2, 3, 4)

    def turn(values, i):
        base = outer[rows(i * 8, 8)][0:1]
        base_cos, base_sin = base[:, 0:128], base[:, 128:256]
        cosine = base_cos * inner[:, 0:128] - base_sin * inner[:, 128:256]
        sine = base_sin * inner[:, 0:128] + base_cos * inner[:, 128:256]
        return values * cosine + pltpu.roll(values, 64, 1) * sine

    for n, d in enumerate((0, 1, 3, 2)):
        i = lax.rem(x + d, X)
        here = rows(i * BLOCK, BLOCK)
        k = (turn(dot(xn[here], b_k[...]), i) * DK**-0.5).astype(BF16)
        v = dot(xn[here], b_v[...]).astype(BF16)
        ks[here] = k
        vs[here] = v
        kf = k.astype(F32)
        k_two = (jnp.concatenate([kf, kf], axis=1) * tail[...]).astype(BF16)
        us[here] = dot(k_two, v, TN)
        between_keys(n)

    total = jnp.zeros((DK, DV), F32)
    for i in range(X):
        st[i * BLOCK : i * BLOCK + DK] = total.astype(BF16)
        total = step_f * total + us[i * BLOCK : i * BLOCK + DK]
    total = jnp.zeros((DK, DV), F32)
    for i in reversed(range(X)):
        st[i * BLOCK + DK : (i + 1) * BLOCK] = total.astype(BF16)
        total = step_b * total + us[i * BLOCK + DK : (i + 1) * BLOCK]


    w_g.fast_one()
    w_g.fast_end()
    w_qo.y_end(*range(8))

    def rs_block(t, d, left, weights, first, width):
        for j in range(4):
            part = dot(left, weights[j * 256 : (j + 1) * 256, first : first + width], NT)
            pf[d * BLOCK : (d + 1) * BLOCK, j * 256 : (j + 1) * 256] = part
            ps[t, d * BLOCK : (d + 1) * BLOCK, j * 256 : (j + 1) * 256] = part.astype(BF16)
        send(
            ps.at[t, rows(d * BLOCK + (1 - c) * OWN, OWN)],
            pr.at[t, d], pp_s.at[t, d], pp_r.at[t, d], sibling,
        )

    def rs_pair_wait(t, d):
        received(pr.at[t, d], pp_s.at[t, d], pp_r.at[t, d])

    def rs_pair(t, d, p):
        mine = pf[rows(d * BLOCK + c * OWN + p * PIECE, PIECE)]
        return mine + pr[t, d, p * PIECE : (p + 1) * PIECE].astype(F32)

    def rs_far(t):
        rs_pair_wait(t, 2)
        for p in (0, 2, 1, 3):
            rs_send[t, p] = rs_pair(t, 2, p).astype(BF16)
            peer = x_next if p < 2 else x_prev
            send(rs_send.at[t, p], rs_recv.at[t, p], rr_s.at[t, p], rr_r.at[t, p], peer)

    def rs_near(t, way, p, relay):
        total = rs_pair(t, 1 if way == 0 else 3, p)
        if relay:
            received(rs_recv.at[t, p], rr_s.at[t, p], rr_r.at[t, p])
            total = total + rs_recv[t, p].astype(F32)
        k = way * 4 + p
        ms_send[t, k] = total.astype(BF16)
        peer = x_next if way == 0 else x_prev
        send(ms_send.at[t, k], ms_recv.at[t, k], mm_s.at[t, k], mm_r.at[t, k], peer)

    def rs_final(t, p):
        total = rs_pair(t, 0, p)
        for k in (p, 4 + p):
            received(ms_recv.at[t, k], mm_s.at[t, k], mm_r.at[t, k])
            total = total + ms_recv[t, k].astype(F32)
        return total

    def reduce_scatter(t, block, weights, first, width, between):
        for n, d in enumerate((2, 1, 3, 0)):
            rs_block(t, d, block(d), weights, first, width)
            if n == 1:
                rs_far(t)
            if n == 2:
                rs_pair_wait(t, 1)
                rs_near(t, 0, 2, False)
                rs_near(t, 0, 3, False)
            if n == 3:
                rs_pair_wait(t, 3)
                rs_near(t, 1, 0, False)
                rs_near(t, 1, 1, False)
            between(n)
        for p in (0, 2, 1, 3):
            rs_near(t, 0 if p < 2 else 1, p, True)
        rs_pair_wait(t, 0)

    def mixer_block(d):
        i = lax.rem(x + d, X)
        here = rows(i * BLOCK, BLOCK)
        q = turn(dot(xn[here], b_qo[:, 0:DK]), i).astype(BF16)
        scores = (dot(q, ks[here], NT) * dmat[...]).astype(BF16)
        qf = q.astype(F32)
        q_two = (jnp.concatenate([qf, qf], axis=1) * lead[...]).astype(BF16)
        retained = dot(scores, vs[here]) + dot(q_two, st[here])
        centred = retained - jnp.mean(retained, axis=-1, keepdims=True)
        normal = centred * lax.rsqrt(jnp.mean(centred * centred, axis=-1, keepdims=True) + EPS)
        gates = dot(xn[here], b_g[...])
        return (normal * (gates / (1.0 + jnp.exp(-gates)))).astype(BF16)

    reduce_scatter(0, mixer_block, b_qo, DK, DV, between_mixer)
    w_ld.fast_end()
    w_ld.y_start(5, 6, 7)
    for n, p in enumerate((0, 2, 1, 3)):
        part = slice(p * PIECE, (p + 1) * PIECE)
        mixed = rs_final(0, p)
        summed = (tok[part].astype(F32) + rms(mixed, g_mo[...])).astype(BF16).astype(F32)
        after[part] = summed
        ch[rows(tp * OWN + p * PIECE, PIECE)] = rms(summed, g_ci[...]).astype(BF16)
        ag_start(1, ch, p)
        if n == 0:
            w_ld.y_relay(0, 1, 2)
        elif n == 1:
            w_u.fast_relay()
        elif n == 2:
            w_ld.y_relay(3, 4)

    w_ld.y_relay(5, 6, 7)
    ag_first(1, ch, 0, 2)
    ag_first(1, ch, 1, 3)

    def expand(d):
        ag_sibling(1, ch, d)
        i = lax.rem(x + d, X)
        there = pl.ds(pl.multiple_of(i * BLOCK + 8, 8), BLOCK)
        up[there, 0:FFP] = dot(ch[rows(i * BLOCK, BLOCK)], b_u[...])
        up[there, FFP:] = dot(ch[rows(i * BLOCK, BLOCK)], b_ld[:, 0:FFP])

    w_u.fast_one()
    w_u.fast_end()
    w_ld.y_end(*range(8))
    expand(0)
    ag_second(1, ch, 0, 2)
    expand(1)
    ag_second(1, ch, 1, 3)
    expand(3)
    expand(2)

    def conv(first, column, at):
        near = up[pl.ds(pl.multiple_of(first, 8), 80), column : column + FFP]
        before = pltpu.roll(near, 1, 0)[8:72]
        behind = pltpu.roll(near, 79, 0)[8:72]
        return (
            taps[at : at + 1] * before
            + taps[at + 1 : at + 2] * near[8:72]
            + taps[at + 2 : at + 3] * behind
            + taps[at + 3 : at + 4]
        )

    def channel_block(d):
        i = lax.rem(x + d, X)

        def tile(n, carry):
            first = i * BLOCK + n * HALF
            g = conv(first, 0, 0)
            act = 0.5 * g * (1.0 + jnp.tanh(0.7978845608028654 * (g + 0.044715 * g * g * g)))
            hid[pl.ds(pl.multiple_of(n * HALF, HALF), HALF)] = (
                act * conv(first, FFP, 8)
            ).astype(BF16)
            return carry

        lax.fori_loop(0, BLOCK // HALF, tile, 0)
        return hid[...]

    reduce_scatter(1, channel_block, b_ld, FFP, FFP, lambda n: None)
    for p in (0, 2, 1, 3):
        part = slice(p * PIECE, (p + 1) * PIECE)
        out[part] = (after[part] + rms(rs_final(1, p), g_co[...])).astype(BF16)

    for copy in sent:
        copy.wait_send()


def layer(
    tokens, mixer_in_gain, query_weight, key_weight, value_weight, gate_weight, decay_logits,
    mixer_output, mixer_out_gain, channel_in_gain, gelu_weight, linear_weight, gelu_kernel,
    linear_kernel, gelu_bias, linear_bias, down_weight, channel_out_gain,
):
    inner, outer = rotation_tables()

    def row(v):
        return v.reshape(1, -1)

    operands = (
        tokens[0], row(mixer_in_gain), query_weight, key_weight, value_weight, gate_weight,
        decay_logits.T, mixer_output.T, row(mixer_out_gain), row(channel_in_gain), gelu_weight,
        linear_weight, gelu_kernel, linear_kernel, gelu_bias, linear_bias, down_weight.T,
        row(channel_out_gain), jnp.asarray(inner), jnp.asarray(outer),
    )
    dma = pltpu.SemaphoreType.DMA
    result = pl.pallas_call(
        kernel,
        out_shape=jax.ShapeDtypeStruct((OWN, D), BF16),
        in_specs=[pl.BlockSpec(memory_space=pl.ANY)] * len(operands),
        out_specs=pl.BlockSpec(memory_space=pltpu.VMEM),
        scratch_shapes=[
            pltpu.VMEM((OWN, D), BF16),
            pltpu.VMEM((1, D), F32),
            pltpu.VMEM((1, 2), F32),
            pltpu.VMEM((1, D), F32),
            pltpu.VMEM((1, D), F32),
            pltpu.VMEM((3, FFOWN), F32),
            pltpu.VMEM((3, FFOWN), F32),
            pltpu.VMEM((FFOWN,), F32),
            pltpu.VMEM((FFOWN,), F32),
            pltpu.VMEM((1, D), F32),
            pltpu.VMEM((BLOCK, 256), F32),
            pltpu.VMEM((8 * X, 256), F32),
            pltpu.VMEM((UNIT, FFOWN), BF16),
            pltpu.VMEM((UNIT, FFOWN), BF16),
            pltpu.VMEM((UNIT, FFOWN), BF16),
            pltpu.VMEM((SEQ, D), BF16),
            pltpu.VMEM((SEQ, D), BF16),
            pltpu.VMEM((D, DK), BF16),
            pltpu.VMEM((D, DV), BF16),
            pltpu.VMEM((D, FFP), BF16),
            pltpu.VMEM((D, DV), BF16),
            pltpu.VMEM((D, DK + DV), BF16),
            pltpu.VMEM((D, 2 * FFP), BF16),
            pltpu.VMEM((SEQ, DK), BF16),
            pltpu.VMEM((SEQ, DV), BF16),
            pltpu.VMEM((SEQ, DV), F32),
            pltpu.VMEM((SEQ, DV), BF16),
            pltpu.VMEM((BLOCK, BLOCK), F32),
            pltpu.VMEM((BLOCK, BLOCK), F32),
            pltpu.VMEM((BLOCK, BLOCK), F32),
            pltpu.VMEM((SEQ, D), F32),
            pltpu.VMEM((2, SEQ, D), BF16),
            pltpu.VMEM((2, 4, OWN, D), BF16),
            pltpu.VMEM((2, 4, PIECE, D), BF16),
            pltpu.VMEM((2, 4, PIECE, D), BF16),
            pltpu.VMEM((2, 8, PIECE, D), BF16),
            pltpu.VMEM((2, 8, PIECE, D), BF16),
            pltpu.VMEM((SEQ + 16, 2 * FFP), F32),
            pltpu.VMEM((BLOCK, FFP), BF16),
            pltpu.VMEM((OWN, D), F32),
            pltpu.VMEM((16, FFP), F32),
            dma((20,)),
            dma((2, 28)), dma((2, 28)),
            dma((3, 3)), dma((3, 3)),
            dma((3, 8, 3)), dma((3, 8, 3)),
            dma((6, 8)), dma((6, 8)),
            dma((2, 4)), dma((2, 4)),
            dma((2, 4)), dma((2, 4)),
            dma((2, 8)), dma((2, 8)),
        ],
        compiler_params=pltpu.CompilerParams(
            collective_id=0, has_side_effects=True, vmem_limit_bytes=60 * 1024 * 1024
        ),
        name="layer",
    )(*operands)
    return result[None]


def solution(mesh):
    by_position = P(("rep", "fs"), "tp", None)
    up_rows, down_rows = P("fs", "tp"), P("tp", "fs")
    in_specs = (
        by_position, P(), up_rows, up_rows, up_rows, up_rows, P(None, "tp"), down_rows, P(), P(),
        up_rows, up_rows, P(None, "tp"), P(None, "tp"), P("tp"), P("tp"), down_rows, P(),
    )
    return jax.shard_map(
        layer, mesh=mesh, in_specs=in_specs, out_specs=by_position, check_vma=False
    )
```

```python
import jax
import jax.numpy as jnp
import numpy as np
from jax import lax
from jax.experimental import pallas as pl
from jax.experimental.pallas import tpu as pltpu
from jax.sharding import PartitionSpec as P

MESH = pl.DeviceIdType.MESH
F32 = jnp.float32
BF16 = jnp.bfloat16

X, Y, Z, ZALL = 4, 4, 8, 16
D = 1024
DK = 128
DV = 256
SEQ = 1024
OWN = 128
HALF = 64
PIECE = 32
BLOCK = 256
UNIT = 32
FFP = 384
FFOWN = 352
EPS = 1e-6
NT = (((1,), (1,)), ((), ()))
TN = (((0,), (0,)), ((), ()))


def rotation_tables():
    frequency = 10000.0 ** (-np.arange(64, dtype=np.float64) / 64)

    def pair(positions):
        angles = positions[:, None] * frequency[None, :]
        cosine, sine = np.cos(angles), np.sin(angles)
        return np.concatenate([cosine, cosine], 1), np.concatenate([-sine, sine], 1)

    inner = np.concatenate(pair(np.arange(BLOCK, dtype=np.float64)), 1)
    outer = np.concatenate(pair(BLOCK * np.repeat(np.arange(X, dtype=np.float64), 8)), 1)
    return inner.astype(np.float32), outer.astype(np.float32)


def dot(a, b, dims=None):
    if dims is None:
        return jnp.dot(a, b, preferred_element_type=F32)
    return lax.dot_general(a, b, dims, preferred_element_type=F32)


def rms(values, gain):
    return values * lax.rsqrt(jnp.mean(values * values, axis=-1, keepdims=True) + EPS) * gain


def kernel(
    h_tok, h_g_in, h_wq, h_wk, h_wv, h_wg, h_logits, h_wo, h_g_mo, h_g_ci, h_gelu, h_linear,
    h_k_gelu, h_k_linear, h_b_gelu, h_b_linear, h_wd, h_g_co, h_inner, h_outer,
    out,
    tok, g_in, logits, g_mo, g_ci, k_gelu, k_linear, bias_g, bias_l, g_co, inner, outer,
    s_u, s_l, s_d,
    xn, ch, b_k, b_g, b_u, b_v, b_qo, b_ld, ks, vs, silu, us, st, dmat, lead, tail, pf, ps, pr, rs_send, rs_recv,
    ms_send, ms_recv, up, hid, after, taps,
    in_s, ag_s, ag_r, ay_s, ay_r, by_s, by_r, fz_s, fz_r, pp_s, pp_r, rr_s, rr_r, mm_s, mm_r,
):
    rep, fs, tp = lax.axis_index("rep"), lax.axis_index("fs"), lax.axis_index("tp")
    x, c = tp // 2, tp % 2
    z, y = fs // Y, fs % Y
    zz = rep * Z + z

    def x_dev(step):
        return (rep, fs, lax.rem(x + step, X) * 2 + c)

    def y_dev(step):
        return (rep, z * Y + lax.rem(y + step, Y), tp)

    def z_dev(step):
        there = lax.rem(zz + step, ZALL)
        return (there // Z, lax.rem(there, Z) * Y + y, tp)

    sibling = (rep, fs, x * 2 + (1 - c))
    x_next, x_prev = x_dev(1), x_dev(X - 1)
    y_next, y_prev, y_far = y_dev(1), y_dev(Y - 1), y_dev(2)
    z_next, z_prev = z_dev(1), z_dev(ZALL - 1)
    z_two = (z_dev(2), z_dev(ZALL - 2))

    barrier = pltpu.get_barrier_semaphore()
    for peer in (x_next, x_prev, sibling, y_next, y_prev, y_far, z_next, z_prev, *z_two):
        pl.semaphore_signal(barrier, inc=1, device_id=peer, device_id_type=MESH)

    def rows(first, count):
        return pl.ds(pl.multiple_of(first, count), count)

    own = rows(fs * UNIT, UNIT)
    loads = [
        pltpu.make_async_copy(src, dst, in_s.at[k])
        for k, (src, dst) in enumerate((
            (h_tok, tok), (h_g_in, g_in), (h_wq, b_qo.at[own, 0:128]), (h_wk, b_k.at[own]),
            (h_wv, b_v.at[own]), (h_wg, b_g.at[own]), (h_wo, b_qo.at[own, 128:384]), (h_logits, logits),
            (h_gelu, s_u), (h_linear, s_l), (h_wd, s_d), (h_k_gelu, k_gelu), (h_k_linear, k_linear),
            (h_b_gelu, bias_g), (h_b_linear, bias_l), (h_g_mo, g_mo), (h_g_ci, g_ci), (h_g_co, g_co),
            (h_inner, inner), (h_outer, outer),
        ))
    ]
    for load in loads:
        load.start()

    sent = []

    def send(src, dst, send_sem, recv_sem, peer):
        copy = pltpu.make_async_remote_copy(
            src_ref=src, dst_ref=dst, send_sem=send_sem, recv_sem=recv_sem,
            device_id=peer, device_id_type=MESH,
        )
        copy.start()
        sent.append(copy)

    def received(dst, send_sem, recv_sem):
        pltpu.make_async_remote_copy(
            src_ref=dst, dst_ref=dst, send_sem=send_sem, recv_sem=recv_sem,
            device_id=sibling, device_id_type=MESH,
        ).wait_recv()

    def ag_place(buf, d, core, p):
        chip = lax.rem(x + d, X)
        return buf.at[rows((chip * 2 + core) * OWN + p * PIECE, PIECE)]

    def ag_send(t, buf, k, d, p, peer):
        here = ag_place(buf, d, c, p)
        send(here, here, ag_s.at[t, k], ag_r.at[t, k], peer)

    def ag_wait(t, buf, k, d, core, p):
        received(ag_place(buf, d, core, p), ag_s.at[t, k], ag_r.at[t, k])

    def ag_start(t, buf, *pieces):
        for p in pieces:
            ag_send(t, buf, p, 0, p, x_next)
            ag_send(t, buf, 4 + p, 0, p, x_prev)
            ag_send(t, buf, 12 + p, 0, p, sibling)

    def ag_first(t, buf, *pieces):
        for p in pieces:
            ag_wait(t, buf, p, 3, c, p)
            if p < 2:
                ag_send(t, buf, 8 + p, 3, p, x_next)
            ag_send(t, buf, 24 + p, 3, p, sibling)
            ag_wait(t, buf, 4 + p, 1, c, p)
            if p >= 2:
                ag_send(t, buf, 8 + p, 1, p, x_prev)
            ag_send(t, buf, 16 + p, 1, p, sibling)

    def ag_second(t, buf, *pieces):
        for p in pieces:
            ag_wait(t, buf, 8 + p, 2, c, p)
            ag_send(t, buf, 20 + p, 2, p, sibling)

    def ag_sibling(t, buf, d):
        for p in range(4):
            ag_wait(t, buf, 12 + 4 * d + p, d, 1 - c, p)

    class FastZ:
        def hop(self, off, k, peer, piece=None):
            here = self.piece(off, piece)
            send(here, here, fz_s.at[self.f, k], fz_r.at[self.f, k], peer)

        def landed(self, off, k, piece=None):
            received(self.piece(off, piece), fz_s.at[self.f, k], fz_r.at[self.f, k])

        def start_two(self):
            self.hop(0, 1, z_two[0])
            self.hop(0, 5, z_two[1])

        def start_one(self):
            self.hop(0, 0, z_next)
            self.hop(0, 4, z_prev)

        def fast_start(self):
            self.start_two()
            self.start_one()

        def fast_one(self):
            self.landed(-1, 0)
            self.landed(1, 4)

        def fast_relay(self):
            self.landed(-2, 1)
            self.hop(-2, 3, z_two[0], 0)
            self.hop(-2, 2, z_next)
            self.landed(2, 5)
            self.hop(2, 7, z_two[1], 1)
            self.hop(2, 6, z_prev)

        def fast_end(self):
            self.landed(-3, 2)
            self.landed(3, 6)
            self.landed(4, 3, 0)
            self.landed(4, 7, 1)

    class OverYZ(FastZ):
        def __init__(self, n, buf, f=None):
            self.n, self.buf, self.f = n, buf, f

        def piece(self, off, half):
            first = lax.rem(z + off + Z, Z) * (Y * UNIT)
            if half is None:
                return self.buf.at[rows(first, Y * UNIT)]
            return self.buf.at[rows(first + half * HALF, HALF)]

        def y_start(self):
            here = self.buf.at[rows(fs * UNIT, UNIT)]
            for k, peer in ((0, y_next), (1, y_prev), (2, y_far)):
                send(here, here, ay_s.at[self.n, k], ay_r.at[self.n, k], peer)

        def y_wait(self):
            for k, step in ((0, Y - 1), (1, 1), (2, 2)):
                there = self.buf.at[rows((z * Y + lax.rem(y + step, Y)) * UNIT, UNIT)]
                received(there, ay_s.at[self.n, k], ay_r.at[self.n, k])

    offsets = (0, -1, 1, -2, 2, -3, 3, 4)

    class OverZY(FastZ):
        def __init__(self, n, buf, f=None):
            self.n, self.buf, self.f = n, buf, f

        def piece(self, off, half):
            first = self.unit(off, 0)
            if half is None:
                return self.buf.at[rows(first, UNIT)]
            return self.buf.at[rows(first + half * 16, 16)]

        def unit(self, off, y_step):
            return (lax.rem(z + off + Z, Z) * Y + lax.rem(y + y_step, Y)) * UNIT

        def y_send(self, j, k, y_step, peer):
            here = self.buf.at[rows(self.unit(offsets[j], y_step), UNIT)]
            send(here, here, by_s.at[self.n, j, k], by_r.at[self.n, j, k], peer)

        def y_wait(self, j, k, y_step):
            there = self.buf.at[rows(self.unit(offsets[j], y_step), UNIT)]
            received(there, by_s.at[self.n, j, k], by_r.at[self.n, j, k])

        def y_start(self, *slots):
            for j in slots:
                self.y_send(j, 0, 0, y_next)
                self.y_send(j, 1, 0, y_prev)

        def y_relay(self, *slots):
            for j in slots:
                if j % 2 == 0:
                    self.y_wait(j, 0, 3)
                    self.y_send(j, 2, 3, y_next)
                    self.y_wait(j, 1, 1)
                else:
                    self.y_wait(j, 1, 1)
                    self.y_send(j, 2, 1, y_prev)
                    self.y_wait(j, 0, 3)

        def y_end(self, *slots):
            for j in slots:
                self.y_wait(j, 2, 2)

    w_k, w_g, w_u = OverYZ(0, b_k, 0), OverYZ(1, b_g, 1), OverYZ(2, b_u, 2)
    w_v, w_qo, w_ld = OverZY(0, b_v, 3), OverZY(1, b_qo, 4), OverZY(2, b_ld, 5)

    for k in (0, 1, 2, 3, 4, 5, 6, 7):
        loads[k].wait()
    tokens = tok[...].astype(F32)
    xn[rows(tp * OWN, OWN)] = rms(tokens, g_in[...]).astype(BF16)
    for k in range(8, len(loads)):
        loads[k].wait()
    b_u[own] = jnp.zeros((UNIT, FFP), BF16)
    b_u[own, 0:FFOWN] = s_u[...]
    b_ld[own] = jnp.zeros((UNIT, 2 * FFP), BF16)
    b_ld[own, 0:FFOWN] = s_l[...]
    b_ld[own, FFP : FFP + FFOWN] = s_d[...]

    pl.semaphore_wait(barrier, 10)

    ag_start(0, xn, 0, 2)
    w_v.fast_start()
    w_k.y_start()
    w_v.y_start(0)
    ag_start(0, xn, 1, 3)
    w_qo.fast_start()
    w_g.y_start()
    w_qo.y_start(0)

    log_f = -jnp.log1p(jnp.exp(-logits[0:1, 0:1]))
    log_b = -jnp.log1p(jnp.exp(-logits[0:1, 1:2]))
    at = lax.broadcasted_iota(jnp.int32, (BLOCK, BLOCK), 0)
    lane = lax.broadcasted_iota(jnp.int32, (BLOCK, BLOCK), 1)
    apart = (at - lane).astype(F32)
    dmat[...] = jnp.exp(jnp.where(at >= lane, apart * log_f, -apart * log_b))
    ahead = at.astype(F32)
    lead[...] = jnp.exp(
        jnp.where(lane < DK, (ahead + 1.0) * log_f, (float(BLOCK) - ahead) * log_b)
    )
    tail[...] = jnp.exp(jnp.where(lane < DK, (BLOCK - 1.0 - ahead) * log_f, ahead * log_b))
    step_f, step_b = jnp.exp(BLOCK * log_f), jnp.exp(BLOCK * log_b)
    taps[...] = jnp.zeros((16, FFP), F32)
    taps[0:3, 0:FFOWN] = k_gelu[...]
    taps[3:4, 0:FFOWN] = bias_g[...].reshape(1, FFOWN)
    taps[8:11, 0:FFOWN] = k_linear[...]
    taps[11:12, 0:FFOWN] = bias_l[...].reshape(1, FFOWN)
    up[0:8] = jnp.zeros((8, 2 * FFP), F32)
    up[SEQ + 8 : SEQ + 16] = jnp.zeros((8, 2 * FFP), F32)

    w_v.fast_relay()
    w_v.fast_one()
    w_v.y_start(1, 2, 3, 4)
    w_k.y_wait()
    w_k.fast_start()
    ag_first(0, xn, 0, 2)
    w_qo.fast_relay()
    w_qo.fast_one()
    w_qo.y_start(1, 2, 3, 4)
    w_g.y_wait()
    w_g.start_two()
    w_v.y_relay(0)
    ag_first(0, xn, 1, 3)
    w_v.fast_end()
    w_v.y_start(5, 6, 7)
    w_v.y_relay(1, 2, 3, 4)
    w_qo.y_relay(0)
    w_k.fast_relay()
    w_g.start_one()
    w_qo.fast_end()
    w_qo.y_start(5, 6, 7)
    ag_second(0, xn, 0, 2)
    w_v.y_relay(5, 6, 7)
    ag_second(0, xn, 1, 3)
    w_qo.y_relay(1, 2, 3, 4)
    w_g.fast_relay()
    ag_sibling(0, xn, 0)
    ag_sibling(0, xn, 1)
    ag_sibling(0, xn, 3)
    ag_sibling(0, xn, 2)
    w_k.fast_one()
    w_k.fast_end()
    w_v.y_end(*range(8))
    w_qo.y_relay(5, 6, 7)

    def between_mixer(n):
        if n == 1:
            w_ld.fast_relay()
            w_u.y_wait()
            w_u.fast_start()
        elif n == 2:
            w_ld.fast_one()
            w_ld.y_start(1, 2, 3, 4)

    def turn(values, i):
        base = outer[rows(i * 8, 8)][0:1]
        base_cos, base_sin = base[:, 0:128], base[:, 128:256]
        cosine = base_cos * inner[:, 0:128] - base_sin * inner[:, 128:256]
        sine = base_sin * inner[:, 0:128] + base_cos * inner[:, 128:256]
        return values * cosine + pltpu.roll(values, 64, 1) * sine

    for pair in range(2):
        wide = slice(pair * 2 * BLOCK, (pair + 1) * 2 * BLOCK)
        k_wide = dot(xn[wide], b_k[...])
        v_wide = dot(xn[wide], b_v[...]).astype(BF16)
        vs[wide] = v_wide
        for n in range(2):
            i = 2 * pair + n
            here, inside = slice(i * BLOCK, (i + 1) * BLOCK), slice(n * BLOCK, (n + 1) * BLOCK)
            k = (turn(k_wide[inside], i) * DK**-0.5).astype(BF16)
            ks[here] = k
            kf = k.astype(F32)
            k_two = (jnp.concatenate([kf, kf], axis=1) * tail[...]).astype(BF16)
            us[here] = dot(k_two, v_wide[inside], TN)
        if pair == 0:
            w_u.y_start()
            w_ld.fast_start()
            w_ld.y_start(0)

    total = jnp.zeros((DK, DV), F32)
    for i in range(X):
        st[i * BLOCK : i * BLOCK + DK] = total.astype(BF16)
        total = step_f * total + us[i * BLOCK : i * BLOCK + DK]
    total = jnp.zeros((DK, DV), F32)
    for i in reversed(range(X)):
        st[i * BLOCK + DK : (i + 1) * BLOCK] = total.astype(BF16)
        total = step_b * total + us[i * BLOCK + DK : (i + 1) * BLOCK]


    w_g.fast_one()
    w_g.fast_end()
    for pair in range(2):
        wide = slice(pair * 2 * BLOCK, (pair + 1) * 2 * BLOCK)
        gates = dot(xn[wide], b_g[...])
        silu[wide] = gates / (1.0 + jnp.exp(-gates))
    w_qo.y_end(*range(8))

    def rs_block(t, d, left, weights, first, width):
        for j in range(4):
            part = dot(left, weights[j * 256 : (j + 1) * 256, first : first + width], NT)
            pf[d * BLOCK : (d + 1) * BLOCK, j * 256 : (j + 1) * 256] = part
            ps[t, d * BLOCK : (d + 1) * BLOCK, j * 256 : (j + 1) * 256] = part.astype(BF16)
        for p in (0, 2, 1, 3):
            send(
                ps.at[t, rows(d * BLOCK + (1 - c) * OWN + p * PIECE, PIECE)],
                pr.at[t, d, pl.ds(p * PIECE, PIECE)], pp_s.at[t, d, p], pp_r.at[t, d, p], sibling,
            )

    def rs_pair(t, d, p):
        received(pr.at[t, d, pl.ds(p * PIECE, PIECE)], pp_s.at[t, d, p], pp_r.at[t, d, p])
        mine = pf[rows(d * BLOCK + c * OWN + p * PIECE, PIECE)]
        return mine + pr[t, d, p * PIECE : (p + 1) * PIECE].astype(F32)

    def rs_far(t):
        for p in (0, 2, 1, 3):
            rs_send[t, p] = rs_pair(t, 2, p).astype(BF16)
            peer = x_next if p < 2 else x_prev
            send(rs_send.at[t, p], rs_recv.at[t, p], rr_s.at[t, p], rr_r.at[t, p], peer)

    def rs_near(t, way, p, relay):
        total = rs_pair(t, 1 if way == 0 else 3, p)
        if relay:
            received(rs_recv.at[t, p], rr_s.at[t, p], rr_r.at[t, p])
            total = total + rs_recv[t, p].astype(F32)
        k = way * 4 + p
        ms_send[t, k] = total.astype(BF16)
        peer = x_next if way == 0 else x_prev
        send(ms_send.at[t, k], ms_recv.at[t, k], mm_s.at[t, k], mm_r.at[t, k], peer)

    def rs_final(t, p):
        total = rs_pair(t, 0, p)
        for k in (p, 4 + p):
            received(ms_recv.at[t, k], mm_s.at[t, k], mm_r.at[t, k])
            total = total + ms_recv[t, k].astype(F32)
        return total

    def reduce_scatter(t, block, weights, first, width, between):
        for n, d in enumerate((2, 1, 3, 0)):
            rs_block(t, d, block(d), weights, first, width)
            if n == 1:
                rs_far(t)
            if n == 2:
                rs_near(t, 0, 2, False)
            if n == 3:
                rs_near(t, 1, 0, False)
            between(n)
        rs_near(t, 0, 0, True)
        rs_near(t, 1, 2, True)
        rs_near(t, 0, 3, False)
        rs_near(t, 1, 1, False)
        rs_near(t, 0, 1, True)
        rs_near(t, 1, 3, True)

    def mixer_block(d):
        i = lax.rem(x + d, X)
        here = rows(i * BLOCK, BLOCK)
        q = turn(dot(xn[here], b_qo[:, 0:DK]), i).astype(BF16)
        scores = (dot(q, ks[here], NT) * dmat[...]).astype(BF16)
        qf = q.astype(F32)
        q_two = (jnp.concatenate([qf, qf], axis=1) * lead[...]).astype(BF16)
        retained = dot(scores, vs[here]) + dot(q_two, st[here])
        centred = retained - jnp.mean(retained, axis=-1, keepdims=True)
        normal = centred * lax.rsqrt(jnp.mean(centred * centred, axis=-1, keepdims=True) + EPS)
        return (normal * silu[here]).astype(BF16)

    reduce_scatter(0, mixer_block, b_qo, DK, DV, between_mixer)
    w_ld.fast_end()
    w_ld.y_start(5, 6, 7)
    for n, p in enumerate((0, 2, 1, 3)):
        part = slice(p * PIECE, (p + 1) * PIECE)
        mixed = rs_final(0, p)
        summed = (tok[part].astype(F32) + rms(mixed, g_mo[...])).astype(BF16).astype(F32)
        after[part] = summed
        ch[rows(tp * OWN + p * PIECE, PIECE)] = rms(summed, g_ci[...]).astype(BF16)
        ag_start(1, ch, p)
        if n == 0:
            w_ld.y_relay(0, 1, 2)
        elif n == 1:
            w_u.fast_relay()
        elif n == 2:
            w_ld.y_relay(3, 4)

    w_ld.y_relay(5, 6, 7)
    ag_first(1, ch, 0, 2)
    ag_first(1, ch, 1, 3)

    def expand(d):
        ag_sibling(1, ch, d)
        i = lax.rem(x + d, X)
        there = pl.ds(pl.multiple_of(i * BLOCK + 8, 8), BLOCK)
        left = ch[rows(i * BLOCK, BLOCK)]
        up[there, 0:256] = dot(left, b_u[:, 0:256])
        up[there, 256:512] = dot(left, jnp.concatenate([b_u[:, 256:384], b_ld[:, 0:128]], axis=1))
        up[there, 512:768] = dot(left, b_ld[:, 128:384])

    w_u.fast_one()
    w_u.fast_end()
    w_ld.y_end(*range(8))
    expand(0)
    ag_second(1, ch, 0, 2)
    expand(1)
    ag_second(1, ch, 1, 3)
    expand(3)
    expand(2)

    def conv(first, column, at):
        near = up[pl.ds(pl.multiple_of(first, 8), 80), column : column + FFP]
        before = pltpu.roll(near, 1, 0)[8:72]
        behind = pltpu.roll(near, 79, 0)[8:72]
        return (
            taps[at : at + 1] * before
            + taps[at + 1 : at + 2] * near[8:72]
            + taps[at + 2 : at + 3] * behind
            + taps[at + 3 : at + 4]
        )

    def channel_block(d):
        i = lax.rem(x + d, X)

        def tile(n, carry):
            first = i * BLOCK + n * HALF
            g = conv(first, 0, 0)
            act = 0.5 * g * (1.0 + jnp.tanh(0.7978845608028654 * (g + 0.044715 * g * g * g)))
            hid[pl.ds(pl.multiple_of(n * HALF, HALF), HALF)] = (
                act * conv(first, FFP, 8)
            ).astype(BF16)
            return carry

        lax.fori_loop(0, BLOCK // HALF, tile, 0)
        return hid[...]

    reduce_scatter(1, channel_block, b_ld, FFP, FFP, lambda n: None)
    for p in (0, 2, 1, 3):
        part = slice(p * PIECE, (p + 1) * PIECE)
        out[part] = (after[part] + rms(rs_final(1, p), g_co[...])).astype(BF16)

    for copy in sent:
        copy.wait_send()


def layer(
    tokens, mixer_in_gain, query_weight, key_weight, value_weight, gate_weight, decay_logits,
    mixer_output, mixer_out_gain, channel_in_gain, gelu_weight, linear_weight, gelu_kernel,
    linear_kernel, gelu_bias, linear_bias, down_weight, channel_out_gain,
):
    inner, outer = rotation_tables()

    def row(v):
        return v.reshape(1, -1)

    operands = (
        tokens[0], row(mixer_in_gain), query_weight, key_weight, value_weight, gate_weight,
        decay_logits.T, mixer_output.T, row(mixer_out_gain), row(channel_in_gain), gelu_weight,
        linear_weight, gelu_kernel, linear_kernel, gelu_bias, linear_bias, down_weight.T,
        row(channel_out_gain), jnp.asarray(inner), jnp.asarray(outer),
    )
    operands = [pltpu.with_memory_space_constraint(v, pltpu.HBM) for v in operands]
    dma = pltpu.SemaphoreType.DMA
    result = pl.pallas_call(
        kernel,
        out_shape=pltpu.VMEM((OWN, D), BF16),
        in_specs=[pl.BlockSpec(memory_space=pltpu.HBM)] * len(operands),
        out_specs=pl.BlockSpec(memory_space=pltpu.VMEM),
        scratch_shapes=[
            pltpu.VMEM((OWN, D), BF16),
            pltpu.VMEM((1, D), F32),
            pltpu.VMEM((1, 2), F32),
            pltpu.VMEM((1, D), F32),
            pltpu.VMEM((1, D), F32),
            pltpu.VMEM((3, FFOWN), F32),
            pltpu.VMEM((3, FFOWN), F32),
            pltpu.VMEM((FFOWN,), F32),
            pltpu.VMEM((FFOWN,), F32),
            pltpu.VMEM((1, D), F32),
            pltpu.VMEM((BLOCK, 256), F32),
            pltpu.VMEM((8 * X, 256), F32),
            pltpu.VMEM((UNIT, FFOWN), BF16),
            pltpu.VMEM((UNIT, FFOWN), BF16),
            pltpu.VMEM((UNIT, FFOWN), BF16),
            pltpu.VMEM((SEQ, D), BF16),
            pltpu.VMEM((SEQ, D), BF16),
            pltpu.VMEM((D, DK), BF16),
            pltpu.VMEM((D, DV), BF16),
            pltpu.VMEM((D, FFP), BF16),
            pltpu.VMEM((D, DV), BF16),
            pltpu.VMEM((D, DK + DV), BF16),
            pltpu.VMEM((D, 2 * FFP), BF16),
            pltpu.VMEM((SEQ, DK), BF16),
            pltpu.VMEM((SEQ, DV), BF16),
            pltpu.VMEM((SEQ, DV), F32),
            pltpu.VMEM((SEQ, DV), F32),
            pltpu.VMEM((SEQ, DV), BF16),
            pltpu.VMEM((BLOCK, BLOCK), F32),
            pltpu.VMEM((BLOCK, BLOCK), F32),
            pltpu.VMEM((BLOCK, BLOCK), F32),
            pltpu.VMEM((SEQ, D), F32),
            pltpu.VMEM((2, SEQ, D), BF16),
            pltpu.VMEM((2, 4, OWN, D), BF16),
            pltpu.VMEM((2, 4, PIECE, D), BF16),
            pltpu.VMEM((2, 4, PIECE, D), BF16),
            pltpu.VMEM((2, 8, PIECE, D), BF16),
            pltpu.VMEM((2, 8, PIECE, D), BF16),
            pltpu.VMEM((SEQ + 16, 2 * FFP), F32),
            pltpu.VMEM((BLOCK, FFP), BF16),
            pltpu.VMEM((OWN, D), F32),
            pltpu.VMEM((16, FFP), F32),
            dma((20,)),
            dma((2, 28)), dma((2, 28)),
            dma((3, 3)), dma((3, 3)),
            dma((3, 8, 3)), dma((3, 8, 3)),
            dma((6, 8)), dma((6, 8)),
            dma((2, 4, 4)), dma((2, 4, 4)),
            dma((2, 4)), dma((2, 4)),
            dma((2, 8)), dma((2, 8)),
        ],
        compiler_params=pltpu.CompilerParams(
            collective_id=0, has_side_effects=True, vmem_limit_bytes=40 * 1024 * 1024
        ),
        name="layer",
    )(*operands)
    return result[None]


def solution(mesh):
    by_position = P(("rep", "fs"), "tp", None)
    up_rows, down_rows = P("fs", "tp"), P("tp", "fs")
    in_specs = (
        by_position, P(), up_rows, up_rows, up_rows, up_rows, P(None, "tp"), down_rows, P(), P(),
        up_rows, up_rows, P(None, "tp"), P(None, "tp"), P("tp"), P("tp"), down_rows, P(),
    )
    return jax.shard_map(
        layer, mesh=mesh, in_specs=in_specs, out_specs=by_position, check_vma=False
    )
```

```python
import jax
import jax.numpy as jnp
import numpy as np
from jax import lax
from jax.experimental import pallas as pl
from jax.experimental.pallas import tpu as pltpu
from jax.sharding import PartitionSpec as P

MESH = pl.DeviceIdType.MESH
F32 = jnp.float32
BF16 = jnp.bfloat16

X, Y, Z, ZALL = 4, 4, 8, 16
D = 1024
DK = 128
DV = 256
SEQ = 1024
OWN = 128
HALF = 64
PIECE = 32
BLOCK = 256
UNIT = 32
FFP = 384
FFOWN = 352
EPS = 1e-6
NT = (((1,), (1,)), ((), ()))
TN = (((0,), (0,)), ((), ()))


def rotation_tables():
    frequency = 10000.0 ** (-np.arange(64, dtype=np.float64) / 64)

    def pair(positions):
        angles = positions[:, None] * frequency[None, :]
        cosine, sine = np.cos(angles), np.sin(angles)
        return np.concatenate([cosine, cosine], 1), np.concatenate([-sine, sine], 1)

    inner = np.concatenate(pair(np.arange(BLOCK, dtype=np.float64)), 1)
    outer = np.concatenate(pair(BLOCK * np.repeat(np.arange(X, dtype=np.float64), 8)), 1)
    return inner.astype(np.float32), outer.astype(np.float32)


def dot(a, b, dims=None):
    if dims is None:
        return jnp.dot(a, b, preferred_element_type=F32)
    return lax.dot_general(a, b, dims, preferred_element_type=F32)


def rms(values, gain):
    return values * lax.rsqrt(jnp.mean(values * values, axis=-1, keepdims=True) + EPS) * gain


def kernel(
    h_tok, h_g_in, h_wq, h_wk, h_wv, h_wg, h_logits, h_wo, h_g_mo, h_g_ci, h_gelu, h_linear,
    h_k_gelu, h_k_linear, h_b_gelu, h_b_linear, h_wd, h_g_co, h_inner, h_outer,
    out,
    tok, g_in, logits, g_mo, g_ci, k_gelu, k_linear, bias_g, bias_l, g_co, inner, outer,
    s_u, s_l, s_d,
    xn, ch, b_k, b_g, b_u, b_v, b_qo, b_ld, ks, vs, silu, us, st, dmat, lead, tail, pf, ps, pr, rs_send, rs_recv,
    ms_send, ms_recv, up, hid, gated, after, taps,
    in_s, ag_s, ag_r, ay_s, ay_r, by_s, by_r, fz_s, fz_r, pp_s, pp_r, rr_s, rr_r, mm_s, mm_r,
):
    rep, fs, tp = lax.axis_index("rep"), lax.axis_index("fs"), lax.axis_index("tp")
    x, c = tp // 2, tp % 2
    z, y = fs // Y, fs % Y
    zz = rep * Z + z

    def x_dev(step):
        return (rep, fs, lax.rem(x + step, X) * 2 + c)

    def y_dev(step):
        return (rep, z * Y + lax.rem(y + step, Y), tp)

    def z_dev(step):
        there = lax.rem(zz + step, ZALL)
        return (there // Z, lax.rem(there, Z) * Y + y, tp)

    sibling = (rep, fs, x * 2 + (1 - c))
    x_next, x_prev = x_dev(1), x_dev(X - 1)
    y_next, y_prev, y_far = y_dev(1), y_dev(Y - 1), y_dev(2)
    z_next, z_prev = z_dev(1), z_dev(ZALL - 1)
    z_two = (z_dev(2), z_dev(ZALL - 2))

    barrier = pltpu.get_barrier_semaphore()
    for peer in (x_next, x_prev, sibling, y_next, y_prev, y_far, z_next, z_prev, *z_two):
        pl.semaphore_signal(barrier, inc=1, device_id=peer, device_id_type=MESH)

    def rows(first, count):
        return pl.ds(pl.multiple_of(first, count), count)

    own = rows(fs * UNIT, UNIT)
    loads = [
        pltpu.make_async_copy(src, dst, in_s.at[k])
        for k, (src, dst) in enumerate((
            (h_tok, tok), (h_g_in, g_in), (h_wq, b_qo.at[own, 0:128]), (h_wk, b_k.at[own]),
            (h_wv, b_v.at[own]), (h_wg, b_g.at[own]), (h_wo, b_qo.at[own, 128:384]), (h_logits, logits),
            (h_gelu, s_u), (h_linear, s_l), (h_wd, s_d), (h_k_gelu, k_gelu), (h_k_linear, k_linear),
            (h_b_gelu, bias_g), (h_b_linear, bias_l), (h_g_mo, g_mo), (h_g_ci, g_ci), (h_g_co, g_co),
            (h_inner, inner), (h_outer, outer),
        ))
    ]
    for load in loads:
        load.start()

    sent = []

    def drain(count):
        for copy in sent[:count]:
            copy.wait_send()
        del sent[:count]


    held = [None]

    def send(src, dst, send_sem, recv_sem, peer):
        copy = pltpu.make_async_remote_copy(
            src_ref=src, dst_ref=dst, send_sem=send_sem, recv_sem=recv_sem,
            device_id=peer, device_id_type=MESH,
        )
        sent.append(copy)
        if held[0] is None:
            copy.start()
        else:
            held[0].append(copy)

    def prepare(*sends):
        held[0] = []
        for one in sends:
            one()
        copies, held[0] = held[0], None
        return copies

    def start_on(core, copies):
        @pl.when(c == core)
        def _():
            for copy in copies:
                copy.start()

    def received(dst, send_sem, recv_sem):
        pltpu.make_async_remote_copy(
            src_ref=dst, dst_ref=dst, send_sem=send_sem, recv_sem=recv_sem,
            device_id=sibling, device_id_type=MESH,
        ).wait_recv()

    def ag_place(buf, d, core, p):
        chip = lax.rem(x + d, X)
        return buf.at[rows((chip * 2 + core) * OWN + p * PIECE, PIECE)]

    def ag_send(t, buf, k, d, p, peer):
        here = ag_place(buf, d, c, p)
        send(here, here, ag_s.at[t, k], ag_r.at[t, k], peer)

    def ag_wait(t, buf, k, d, core, p):
        received(ag_place(buf, d, core, p), ag_s.at[t, k], ag_r.at[t, k])

    def ag_start(t, buf, *pieces):
        for p in pieces:
            ag_send(t, buf, p, 0, p, x_next)
            ag_send(t, buf, 4 + p, 0, p, x_prev)
            ag_send(t, buf, 12 + p, 0, p, sibling)

    def ag_first(t, buf, *pieces):
        for p in pieces:
            ag_wait(t, buf, p, 3, c, p)
            if p < 2:
                ag_send(t, buf, 8 + p, 3, p, x_next)
            ag_send(t, buf, 24 + p, 3, p, sibling)
            ag_wait(t, buf, 4 + p, 1, c, p)
            if p >= 2:
                ag_send(t, buf, 8 + p, 1, p, x_prev)
            ag_send(t, buf, 16 + p, 1, p, sibling)

    def ag_second(t, buf, *pieces):
        for p in pieces:
            ag_wait(t, buf, 8 + p, 2, c, p)
            ag_send(t, buf, 20 + p, 2, p, sibling)

    def ag_sibling(t, buf, d):
        for p in range(4):
            ag_wait(t, buf, 12 + 4 * d + p, d, 1 - c, p)

    class FastZ:
        def hop(self, off, k, peer, piece=None):
            here = self.piece(off, piece)
            send(here, here, fz_s.at[self.f, k], fz_r.at[self.f, k], peer)

        def landed(self, off, k, piece=None):
            received(self.piece(off, piece), fz_s.at[self.f, k], fz_r.at[self.f, k])

        def start_two(self):
            self.hop(0, 1, z_two[0])
            self.hop(0, 5, z_two[1])

        def start_one(self):
            self.hop(0, 0, z_next)
            self.hop(0, 4, z_prev)

        def fast_start(self):
            self.start_two()
            self.start_one()

        def fast_one(self):
            self.landed(-1, 0)
            self.landed(1, 4)

        def fast_relay(self):
            self.landed(-2, 1)
            self.hop(-2, 3, z_two[0], 0)
            self.hop(-2, 2, z_next)
            self.landed(2, 5)
            self.hop(2, 7, z_two[1], 1)
            self.hop(2, 6, z_prev)

        def fast_end(self):
            self.landed(-3, 2)
            self.landed(3, 6)
            self.landed(4, 3, 0)
            self.landed(4, 7, 1)

    class OverYZ(FastZ):
        def __init__(self, n, buf, f=None):
            self.n, self.buf, self.f = n, buf, f

        def piece(self, off, half):
            first = lax.rem(z + off + Z, Z) * (Y * UNIT)
            if half is None:
                return self.buf.at[rows(first, Y * UNIT)]
            return self.buf.at[rows(first + half * HALF, HALF)]

        def y_start(self):
            here = self.buf.at[rows(fs * UNIT, UNIT)]
            for k, peer in ((0, y_next), (1, y_prev), (2, y_far)):
                send(here, here, ay_s.at[self.n, k], ay_r.at[self.n, k], peer)

        def y_wait(self):
            for k, step in ((0, Y - 1), (1, 1), (2, 2)):
                there = self.buf.at[rows((z * Y + lax.rem(y + step, Y)) * UNIT, UNIT)]
                received(there, ay_s.at[self.n, k], ay_r.at[self.n, k])

    offsets = (0, -1, 1, -2, 2, -3, 3, 4)

    class OverZY(FastZ):
        def __init__(self, n, buf, f=None):
            self.n, self.buf, self.f = n, buf, f

        def piece(self, off, half):
            first = self.unit(off, 0)
            if half is None:
                return self.buf.at[rows(first, UNIT)]
            return self.buf.at[rows(first + half * 16, 16)]

        def unit(self, off, y_step):
            return (lax.rem(z + off + Z, Z) * Y + lax.rem(y + y_step, Y)) * UNIT

        def y_send(self, j, k, y_step, peer):
            here = self.buf.at[rows(self.unit(offsets[j], y_step), UNIT)]
            send(here, here, by_s.at[self.n, j, k], by_r.at[self.n, j, k], peer)

        def y_wait(self, j, k, y_step):
            there = self.buf.at[rows(self.unit(offsets[j], y_step), UNIT)]
            received(there, by_s.at[self.n, j, k], by_r.at[self.n, j, k])

        def y_start(self, *slots):
            for j in slots:
                self.y_send(j, 0, 0, y_next)
                self.y_send(j, 1, 0, y_prev)

        def y_relay(self, *slots):
            for j in slots:
                if j % 2 == 0:
                    self.y_wait(j, 0, 3)
                    self.y_send(j, 2, 3, y_next)
                    self.y_wait(j, 1, 1)
                else:
                    self.y_wait(j, 1, 1)
                    self.y_send(j, 2, 1, y_prev)
                    self.y_wait(j, 0, 3)

        def y_end(self, *slots):
            for j in slots:
                self.y_wait(j, 2, 2)

    w_k, w_g, w_u = OverYZ(0, b_k, 0), OverYZ(1, b_g, 1), OverYZ(2, b_u, 2)
    w_v, w_qo, w_ld = OverZY(0, b_v, 3), OverZY(1, b_qo, 4), OverZY(2, b_ld, 5)

    for k in (0, 1, 2, 3, 4, 5, 6, 7):
        loads[k].wait()
    tokens = tok[...].astype(F32)
    xn[rows(tp * OWN, OWN)] = rms(tokens, g_in[...]).astype(BF16)
    for k in range(8, len(loads)):
        loads[k].wait()
    b_u[own] = jnp.zeros((UNIT, FFP), BF16)
    b_u[own, 0:FFOWN] = s_u[...]
    b_ld[own] = jnp.zeros((UNIT, 2 * FFP), BF16)
    b_ld[own, 0:FFOWN] = s_l[...]
    b_ld[own, FFP : FFP + FFOWN] = s_d[...]

    pl.semaphore_wait(barrier, 10)

    ag_start(0, xn, 0, 2)
    w_v.fast_start()
    w_k.y_start()
    w_v.y_start(0)
    ag_start(0, xn, 1, 3)
    w_qo.fast_start()
    w_g.y_start()
    w_qo.y_start(0)

    log_f = -jnp.log1p(jnp.exp(-logits[0:1, 0:1]))
    log_b = -jnp.log1p(jnp.exp(-logits[0:1, 1:2]))
    at = lax.broadcasted_iota(jnp.int32, (BLOCK, BLOCK), 0)
    lane = lax.broadcasted_iota(jnp.int32, (BLOCK, BLOCK), 1)
    apart = (at - lane).astype(F32)
    dmat[...] = jnp.exp(jnp.where(at >= lane, apart * log_f, -apart * log_b))
    ahead = at.astype(F32)
    lead[...] = jnp.exp(
        jnp.where(lane < DK, (ahead + 1.0) * log_f, (float(BLOCK) - ahead) * log_b)
    )
    tail[...] = jnp.exp(jnp.where(lane < DK, (BLOCK - 1.0 - ahead) * log_f, ahead * log_b))
    step_f, step_b = jnp.exp(BLOCK * log_f), jnp.exp(BLOCK * log_b)
    taps[...] = jnp.zeros((16, FFP), F32)
    taps[0:3, 0:FFOWN] = k_gelu[...]
    taps[3:4, 0:FFOWN] = bias_g[...].reshape(1, FFOWN)
    taps[8:11, 0:FFOWN] = k_linear[...]
    taps[11:12, 0:FFOWN] = bias_l[...].reshape(1, FFOWN)
    up[0:8] = jnp.zeros((8, 2 * FFP), F32)
    up[SEQ + 8 : SEQ + 16] = jnp.zeros((8, 2 * FFP), F32)

    w_v.fast_relay()
    w_v.fast_one()
    w_v.y_start(1, 2, 3, 4)
    w_k.y_wait()
    w_k.fast_start()
    ag_first(0, xn, 0, 2)
    w_qo.fast_relay()
    w_qo.fast_one()
    qo_y = prepare(lambda: w_qo.y_start(1, 2, 3, 4))
    start_on(0, qo_y)
    w_g.y_wait()
    w_g.start_two()
    w_v.y_relay(0)
    ag_first(0, xn, 1, 3)
    w_v.fast_end()
    w_v.y_start(5, 6, 7)
    w_v.y_relay(1, 2, 3, 4)
    start_on(1, qo_y)
    w_qo.y_relay(0)
    w_k.fast_relay()
    w_g.start_one()
    w_qo.fast_end()
    w_qo.y_start(5, 6, 7)
    ag_second(0, xn, 0, 2)
    w_v.y_relay(5, 6, 7)
    ag_second(0, xn, 1, 3)
    w_qo.y_relay(1, 2, 3, 4)
    w_g.fast_relay()
    ag_sibling(0, xn, 0)
    ag_sibling(0, xn, 1)
    ag_sibling(0, xn, 3)
    ag_sibling(0, xn, 2)
    w_k.fast_one()
    w_k.fast_end()
    w_v.y_end(*range(8))
    w_qo.y_relay(5, 6, 7)

    def between_mixer(n):
        if n == 1:
            w_ld.fast_relay()
            w_u.y_wait()
            w_u.fast_start()
        elif n == 2:
            w_ld.fast_one()
            w_ld.y_start(1, 2, 3, 4)

    def turn(values, i):
        base = outer[rows(i * 8, 8)][0:1]
        base_cos, base_sin = base[:, 0:128], base[:, 128:256]
        cosine = base_cos * inner[:, 0:128] - base_sin * inner[:, 128:256]
        sine = base_sin * inner[:, 0:128] + base_cos * inner[:, 128:256]
        return values * cosine + pltpu.roll(values, 64, 1) * sine

    for pair in range(2):
        wide = slice(pair * 2 * BLOCK, (pair + 1) * 2 * BLOCK)
        k_wide = dot(xn[wide], b_k[...])
        v_wide = dot(xn[wide], b_v[...]).astype(BF16)
        vs[wide] = v_wide
        for n in range(2):
            i = 2 * pair + n
            here, inside = slice(i * BLOCK, (i + 1) * BLOCK), slice(n * BLOCK, (n + 1) * BLOCK)
            k = (turn(k_wide[inside], i) * DK**-0.5).astype(BF16)
            ks[here] = k
            kf = k.astype(F32)
            k_two = (jnp.concatenate([kf, kf], axis=1) * tail[...]).astype(BF16)
            us[here] = dot(k_two, v_wide[inside], TN)
        if pair == 0:
            w_u.y_start()
            w_ld.fast_start()
            w_ld.y_start(0)

    total = jnp.zeros((DK, DV), F32)
    for i in range(X):
        st[i * BLOCK : i * BLOCK + DK] = total.astype(BF16)
        total = step_f * total + us[i * BLOCK : i * BLOCK + DK]
    total = jnp.zeros((DK, DV), F32)
    for i in reversed(range(X)):
        st[i * BLOCK + DK : (i + 1) * BLOCK] = total.astype(BF16)
        total = step_b * total + us[i * BLOCK + DK : (i + 1) * BLOCK]


    w_g.fast_one()
    w_g.fast_end()
    for pair in range(2):
        wide = slice(pair * 2 * BLOCK, (pair + 1) * 2 * BLOCK)
        gates = dot(xn[wide], b_g[...])
        silu[wide] = gates / (1.0 + jnp.exp(-gates))
    w_qo.y_end(*range(8))

    first_sends = len(sent)

    def rs_block(t, d, left, weights, first, width):
        left = jnp.concatenate([left[rows((1 - c) * OWN, OWN)], left[rows(c * OWN, OWN)]], axis=0)
        there = slice(d * OWN, (d + 1) * OWN)
        for j in range(4):
            columns = slice(j * 256, (j + 1) * 256)
            part = dot(left, weights[columns, first : first + width], NT)
            ps[t, there, columns] = part[:OWN].astype(BF16)
            pf[there, columns] = part[OWN:]
        for p in (0, 2, 1, 3):
            send(
                ps.at[t, pl.ds(d * OWN + p * PIECE, PIECE)],
                pr.at[t, d, pl.ds(p * PIECE, PIECE)], pp_s.at[t, d, p], pp_r.at[t, d, p], sibling,
            )

    def rs_pair(t, d, p):
        received(pr.at[t, d, pl.ds(p * PIECE, PIECE)], pp_s.at[t, d, p], pp_r.at[t, d, p])
        mine = pf[d * OWN + p * PIECE : d * OWN + (p + 1) * PIECE]
        return mine + pr[t, d, p * PIECE : (p + 1) * PIECE].astype(F32)

    def rs_far(t):
        for p in (0, 2, 1, 3):
            rs_send[t, p] = rs_pair(t, 2, p).astype(BF16)
            peer = x_next if p < 2 else x_prev
            send(rs_send.at[t, p], rs_recv.at[t, p], rr_s.at[t, p], rr_r.at[t, p], peer)

    def rs_near(t, way, p, relay):
        total = rs_pair(t, 1 if way == 0 else 3, p)
        if relay:
            received(rs_recv.at[t, p], rr_s.at[t, p], rr_r.at[t, p])
            total = total + rs_recv[t, p].astype(F32)
        k = way * 4 + p
        ms_send[t, k] = total.astype(BF16)
        peer = x_next if way == 0 else x_prev
        send(ms_send.at[t, k], ms_recv.at[t, k], mm_s.at[t, k], mm_r.at[t, k], peer)

    def rs_final(t, p):
        total = rs_pair(t, 0, p)
        for k in (p, 4 + p):
            received(ms_recv.at[t, k], mm_s.at[t, k], mm_r.at[t, k])
            total = total + ms_recv[t, k].astype(F32)
        return total

    def reduce_scatter(t, block, weights, first, width, between):
        for n, d in enumerate((2, 1, 3, 0)):
            rs_block(t, d, block(d), weights, first, width)
            if n == 1:
                rs_far(t)
            if n == 2:
                rs_near(t, 0, 2, False)
            if n == 3:
                rs_near(t, 1, 0, False)
            between(n)
        rs_near(t, 0, 0, True)
        rs_near(t, 1, 2, True)
        rs_near(t, 0, 3, False)
        rs_near(t, 1, 1, False)
        rs_near(t, 0, 1, True)
        rs_near(t, 1, 3, True)

    def mixer_block(d):
        i = lax.rem(x + d, X)
        here = rows(i * BLOCK, BLOCK)
        q = turn(dot(xn[here], b_qo[:, 0:DK]), i).astype(BF16)
        scores = (dot(q, ks[here], NT) * dmat[...]).astype(BF16)
        qf = q.astype(F32)
        q_two = (jnp.concatenate([qf, qf], axis=1) * lead[...]).astype(BF16)
        retained = dot(scores, vs[here]) + dot(q_two, st[here])
        centred = retained - jnp.mean(retained, axis=-1, keepdims=True)
        normal = centred * lax.rsqrt(jnp.mean(centred * centred, axis=-1, keepdims=True) + EPS)
        gated[...] = (normal * silu[here]).astype(BF16)
        return gated

    reduce_scatter(0, mixer_block, b_qo, DK, DV, between_mixer)
    w_ld.fast_end()
    w_ld.y_start(5, 6, 7)
    for n, p in enumerate((0, 2, 1, 3)):
        part = slice(p * PIECE, (p + 1) * PIECE)
        mixed = rs_final(0, p)
        summed = (tok[part].astype(F32) + rms(mixed, g_mo[...])).astype(BF16).astype(F32)
        after[part] = summed
        ch[rows(tp * OWN + p * PIECE, PIECE)] = rms(summed, g_ci[...]).astype(BF16)
        ag_start(1, ch, p)
        if n == 0:
            w_ld.y_relay(0, 1, 2)
        elif n == 1:
            w_u.fast_relay()
        elif n == 2:
            w_ld.y_relay(3, 4)

    w_ld.y_relay(5, 6, 7)
    drain(first_sends)
    before_last = len(sent)
    ag_first(1, ch, 0, 2)
    ag_first(1, ch, 1, 3)

    def expand(d):
        ag_sibling(1, ch, d)
        i = lax.rem(x + d, X)
        there = pl.ds(pl.multiple_of(i * BLOCK + 8, 8), BLOCK)
        left = ch[rows(i * BLOCK, BLOCK)]
        up[there, 0:256] = dot(left, b_u[:, 0:256])
        up[there, 256:512] = dot(left, jnp.concatenate([b_u[:, 256:384], b_ld[:, 0:128]], axis=1))
        up[there, 512:768] = dot(left, b_ld[:, 128:384])

    w_u.fast_one()
    w_u.fast_end()
    w_ld.y_end(*range(8))
    expand(0)
    ag_second(1, ch, 0, 2)
    expand(1)
    ag_second(1, ch, 1, 3)
    expand(3)
    expand(2)

    def conv(first, column, at):
        near = up[pl.ds(pl.multiple_of(first, 8), 80), column : column + FFP]
        before = pltpu.roll(near, 1, 0)[8:72]
        behind = pltpu.roll(near, 79, 0)[8:72]
        return (
            taps[at : at + 1] * before
            + taps[at + 1 : at + 2] * near[8:72]
            + taps[at + 2 : at + 3] * behind
            + taps[at + 3 : at + 4]
        )

    def channel_block(d):
        i = lax.rem(x + d, X)

        def tile(n, carry):
            first = i * BLOCK + n * HALF
            g = conv(first, 0, 0)
            act = 0.5 * g * (1.0 + jnp.tanh(0.7978845608028654 * (g + 0.044715 * g * g * g)))
            hid[pl.ds(pl.multiple_of(n * HALF, HALF), HALF)] = (
                act * conv(first, FFP, 8)
            ).astype(BF16)
            return carry

        lax.fori_loop(0, BLOCK // HALF, tile, 0)
        return hid

    reduce_scatter(1, channel_block, b_ld, FFP, FFP, lambda n: None)
    drain(before_last)
    for p in (0, 2, 1, 3):
        part = slice(p * PIECE, (p + 1) * PIECE)
        out[part] = (after[part] + rms(rs_final(1, p), g_co[...])).astype(BF16)

    for copy in sent:
        copy.wait_send()


def layer(
    tokens, mixer_in_gain, query_weight, key_weight, value_weight, gate_weight, decay_logits,
    mixer_output, mixer_out_gain, channel_in_gain, gelu_weight, linear_weight, gelu_kernel,
    linear_kernel, gelu_bias, linear_bias, down_weight, channel_out_gain,
):
    inner, outer = rotation_tables()

    def row(v):
        return v.reshape(1, -1)

    operands = (
        tokens[0], row(mixer_in_gain), query_weight, key_weight, value_weight, gate_weight,
        decay_logits.T, mixer_output.T, row(mixer_out_gain), row(channel_in_gain), gelu_weight,
        linear_weight, gelu_kernel, linear_kernel, gelu_bias, linear_bias, down_weight.T,
        row(channel_out_gain), jnp.asarray(inner), jnp.asarray(outer),
    )
    operands = [pltpu.with_memory_space_constraint(v, pltpu.HBM) for v in operands]
    dma = pltpu.SemaphoreType.DMA
    result = pl.pallas_call(
        kernel,
        out_shape=pltpu.VMEM((OWN, D), BF16),
        in_specs=[pl.BlockSpec(memory_space=pltpu.HBM)] * len(operands),
        out_specs=pl.BlockSpec(memory_space=pltpu.VMEM),
        scratch_shapes=[
            pltpu.VMEM((OWN, D), BF16),
            pltpu.VMEM((1, D), F32),
            pltpu.VMEM((1, 2), F32),
            pltpu.VMEM((1, D), F32),
            pltpu.VMEM((1, D), F32),
            pltpu.VMEM((3, FFOWN), F32),
            pltpu.VMEM((3, FFOWN), F32),
            pltpu.VMEM((FFOWN,), F32),
            pltpu.VMEM((FFOWN,), F32),
            pltpu.VMEM((1, D), F32),
            pltpu.VMEM((BLOCK, 256), F32),
            pltpu.VMEM((8 * X, 256), F32),
            pltpu.VMEM((UNIT, FFOWN), BF16),
            pltpu.VMEM((UNIT, FFOWN), BF16),
            pltpu.VMEM((UNIT, FFOWN), BF16),
            pltpu.VMEM((SEQ, D), BF16),
            pltpu.VMEM((SEQ, D), BF16),
            pltpu.VMEM((D, DK), BF16),
            pltpu.VMEM((D, DV), BF16),
            pltpu.VMEM((D, FFP), BF16),
            pltpu.VMEM((D, DV), BF16),
            pltpu.VMEM((D, DK + DV), BF16),
            pltpu.VMEM((D, 2 * FFP), BF16),
            pltpu.VMEM((SEQ, DK), BF16),
            pltpu.VMEM((SEQ, DV), BF16),
            pltpu.VMEM((SEQ, DV), F32),
            pltpu.VMEM((SEQ, DV), F32),
            pltpu.VMEM((SEQ, DV), BF16),
            pltpu.VMEM((BLOCK, BLOCK), F32),
            pltpu.VMEM((BLOCK, BLOCK), F32),
            pltpu.VMEM((BLOCK, BLOCK), F32),
            pltpu.VMEM((4 * OWN, D), F32),
            pltpu.VMEM((2, 4 * OWN, D), BF16),
            pltpu.VMEM((2, 4, OWN, D), BF16),
            pltpu.VMEM((2, 4, PIECE, D), BF16),
            pltpu.VMEM((2, 4, PIECE, D), BF16),
            pltpu.VMEM((2, 8, PIECE, D), BF16),
            pltpu.VMEM((2, 8, PIECE, D), BF16),
            pltpu.VMEM((SEQ + 16, 2 * FFP), F32),
            pltpu.VMEM((BLOCK, FFP), BF16),
            pltpu.VMEM((BLOCK, DV), BF16),
            pltpu.VMEM((OWN, D), F32),
            pltpu.VMEM((16, FFP), F32),
            dma((20,)),
            dma((2, 28)), dma((2, 28)),
            dma((3, 3)), dma((3, 3)),
            dma((3, 8, 3)), dma((3, 8, 3)),
            dma((6, 8)), dma((6, 8)),
            dma((2, 4, 4)), dma((2, 4, 4)),
            dma((2, 4)), dma((2, 4)),
            dma((2, 8)), dma((2, 8)),
        ],
        compiler_params=pltpu.CompilerParams(
            collective_id=0, has_side_effects=True, vmem_limit_bytes=40 * 1024 * 1024
        ),
        name="layer",
    )(*operands)
    return result[None]


def solution(mesh):
    by_position = P(("rep", "fs"), "tp", None)
    up_rows, down_rows = P("fs", "tp"), P("tp", "fs")
    in_specs = (
        by_position, P(), up_rows, up_rows, up_rows, up_rows, P(None, "tp"), down_rows, P(), P(),
        up_rows, up_rows, P(None, "tp"), P(None, "tp"), P("tp"), P("tp"), down_rows, P(),
    )
    return jax.shard_map(
        layer, mesh=mesh, in_specs=in_specs, out_specs=by_position, check_vma=False
    )
```

```python
import jax
import jax.numpy as jnp
import numpy as np
from jax import lax
from jax.experimental import pallas as pl
from jax.experimental.pallas import tpu as pltpu
from jax.sharding import PartitionSpec as P

MESH = pl.DeviceIdType.MESH
F32 = jnp.float32
BF16 = jnp.bfloat16

X, Y, Z, ZALL = 4, 4, 8, 16
D = 1024
DK = 128
DV = 256
SEQ = 1024
OWN = 128
HALF = 64
PIECE = 32
BLOCK = 256
UNIT = 32
FFP = 384
FFOWN = 352
EPS = 1e-6
NT = (((1,), (1,)), ((), ()))
TN = (((0,), (0,)), ((), ()))


def rotation_tables():
    frequency = 10000.0 ** (-np.arange(64, dtype=np.float64) / 64)

    def pair(positions):
        angles = positions[:, None] * frequency[None, :]
        cosine, sine = np.cos(angles), np.sin(angles)
        return np.concatenate([cosine, cosine], 1), np.concatenate([-sine, sine], 1)

    inner = np.concatenate(pair(np.arange(BLOCK, dtype=np.float64)), 1)
    outer = np.concatenate(pair(BLOCK * np.repeat(np.arange(X, dtype=np.float64), 8)), 1)
    return inner.astype(np.float32), outer.astype(np.float32)


def dot(a, b, dims=None):
    if dims is None:
        return jnp.dot(a, b, preferred_element_type=F32)
    return lax.dot_general(a, b, dims, preferred_element_type=F32)


def rms(values, gain):
    return values * lax.rsqrt(jnp.mean(values * values, axis=-1, keepdims=True) + EPS) * gain


def kernel(
    h_tok, h_g_in, h_wq, h_wk, h_wv, h_wg, h_logits, h_wo, h_g_mo, h_g_ci, h_gelu, h_linear,
    h_k_gelu, h_k_linear, h_b_gelu, h_b_linear, h_wd, h_g_co, h_inner, h_outer,
    out,
    tok, g_in, logits, g_mo, g_ci, k_gelu, k_linear, bias_g, bias_l, g_co, inner, outer,
    s_u, s_l, s_d,
    xn, ch, b_k, b_g, b_u, b_v, b_qo, b_ld, ks, vs, silu, us, st, dmat, lead, tail, pf, ps, pr, rs_send, rs_recv,
    ms_send, ms_recv, up, hid, gated, after, taps,
    in_s, ag_s, ag_r, ay_s, ay_r, by_s, by_r, fz_s, fz_r, pp_s, pp_r, rr_s, rr_r, mm_s, mm_r,
):
    rep, fs, tp = lax.axis_index("rep"), lax.axis_index("fs"), lax.axis_index("tp")
    x, c = tp // 2, tp % 2
    z, y = fs // Y, fs % Y
    zz = rep * Z + z

    def x_dev(step):
        return (rep, fs, lax.rem(x + step, X) * 2 + c)

    def y_dev(step):
        return (rep, z * Y + lax.rem(y + step, Y), tp)

    def z_dev(step):
        there = lax.rem(zz + step, ZALL)
        return (there // Z, lax.rem(there, Z) * Y + y, tp)

    sibling = (rep, fs, x * 2 + (1 - c))
    x_next, x_prev = x_dev(1), x_dev(X - 1)
    y_next, y_prev, y_far = y_dev(1), y_dev(Y - 1), y_dev(2)
    z_next, z_prev = z_dev(1), z_dev(ZALL - 1)
    z_two = (z_dev(2), z_dev(ZALL - 2))

    barrier = pltpu.get_barrier_semaphore()
    for peer in (x_next, x_prev, sibling, y_next, y_prev, y_far, z_next, z_prev, *z_two):
        pl.semaphore_signal(barrier, inc=1, device_id=peer, device_id_type=MESH)

    def rows(first, count):
        return pl.ds(pl.multiple_of(first, count), count)

    own = rows(fs * UNIT, UNIT)
    loads = [
        pltpu.make_async_copy(src, dst, in_s.at[k])
        for k, (src, dst) in enumerate((
            (h_tok, tok), (h_g_in, g_in), (h_wq, b_qo.at[own, 0:128]), (h_wk, b_k.at[own]),
            (h_wv, b_v.at[own]), (h_wg, b_g.at[own]), (h_wo, b_qo.at[own, 128:384]), (h_logits, logits),
            (h_gelu, s_u), (h_linear, s_l), (h_wd, s_d), (h_k_gelu, k_gelu), (h_k_linear, k_linear),
            (h_b_gelu, bias_g), (h_b_linear, bias_l), (h_g_mo, g_mo), (h_g_ci, g_ci), (h_g_co, g_co),
            (h_inner, inner), (h_outer, outer),
        ))
    ]
    for load in loads:
        load.start()

    sent = []

    def drain(count):
        for copy in sent[:count]:
            copy.wait_send()
        del sent[:count]


    held = [None]

    def send(src, dst, send_sem, recv_sem, peer):
        copy = pltpu.make_async_remote_copy(
            src_ref=src, dst_ref=dst, send_sem=send_sem, recv_sem=recv_sem,
            device_id=peer, device_id_type=MESH,
        )
        sent.append(copy)
        if held[0] is None:
            copy.start()
        else:
            held[0].append(copy)

    def prepare(*sends):
        held[0] = []
        for one in sends:
            one()
        copies, held[0] = held[0], None
        return copies

    def start_on(core, copies):
        @pl.when(c == core)
        def _():
            for copy in copies:
                copy.start()

    def received(dst, send_sem, recv_sem):
        pltpu.make_async_remote_copy(
            src_ref=dst, dst_ref=dst, send_sem=send_sem, recv_sem=recv_sem,
            device_id=sibling, device_id_type=MESH,
        ).wait_recv()

    def ag_place(buf, d, core, p):
        chip = lax.rem(x + d, X)
        return buf.at[rows((chip * 2 + core) * OWN + p * PIECE, PIECE)]

    def ag_send(t, buf, k, d, p, peer):
        here = ag_place(buf, d, c, p)
        send(here, here, ag_s.at[t, k], ag_r.at[t, k], peer)

    def ag_wait(t, buf, k, d, core, p):
        received(ag_place(buf, d, core, p), ag_s.at[t, k], ag_r.at[t, k])

    def ag_start(t, buf, *pieces):
        for p in pieces:
            ag_send(t, buf, p, 0, p, x_next)
            ag_send(t, buf, 4 + p, 0, p, x_prev)
            ag_send(t, buf, 12 + p, 0, p, sibling)

    def ag_first(t, buf, *pieces):
        for p in pieces:
            ag_wait(t, buf, p, 3, c, p)
            if p < 2:
                ag_send(t, buf, 8 + p, 3, p, x_next)
            ag_send(t, buf, 24 + p, 3, p, sibling)
            ag_wait(t, buf, 4 + p, 1, c, p)
            if p >= 2:
                ag_send(t, buf, 8 + p, 1, p, x_prev)
            ag_send(t, buf, 16 + p, 1, p, sibling)

    def ag_second(t, buf, *pieces):
        for p in pieces:
            ag_wait(t, buf, 8 + p, 2, c, p)
            ag_send(t, buf, 20 + p, 2, p, sibling)

    def ag_sibling(t, buf, d):
        for p in range(4):
            ag_wait(t, buf, 12 + 4 * d + p, d, 1 - c, p)

    class FastZ:
        def hop(self, off, k, peer, piece=None):
            here = self.piece(off, piece)
            send(here, here, fz_s.at[self.f, k], fz_r.at[self.f, k], peer)

        def landed(self, off, k, piece=None):
            received(self.piece(off, piece), fz_s.at[self.f, k], fz_r.at[self.f, k])

        def start_two(self):
            self.hop(0, 1, z_two[0])
            self.hop(0, 5, z_two[1])

        def start_one(self):
            self.hop(0, 0, z_next)
            self.hop(0, 4, z_prev)

        def fast_start(self):
            self.start_two()
            self.start_one()

        def fast_one(self):
            self.landed(-1, 0)
            self.landed(1, 4)

        def fast_relay(self):
            self.landed(-2, 1)
            self.hop(-2, 3, z_two[0], 0)
            self.hop(-2, 2, z_next)
            self.landed(2, 5)
            self.hop(2, 7, z_two[1], 1)
            self.hop(2, 6, z_prev)

        def fast_end(self):
            self.landed(-3, 2)
            self.landed(3, 6)
            self.landed(4, 3, 0)
            self.landed(4, 7, 1)

    class OverYZ(FastZ):
        def __init__(self, n, buf, f=None):
            self.n, self.buf, self.f = n, buf, f

        def piece(self, off, half):
            first = lax.rem(z + off + Z, Z) * (Y * UNIT)
            if half is None:
                return self.buf.at[rows(first, Y * UNIT)]
            return self.buf.at[rows(first + half * HALF, HALF)]

        def y_start(self):
            here = self.buf.at[rows(fs * UNIT, UNIT)]
            for k, peer in ((0, y_next), (1, y_prev), (2, y_far)):
                send(here, here, ay_s.at[self.n, k], ay_r.at[self.n, k], peer)

        def y_wait(self):
            for k, step in ((0, Y - 1), (1, 1), (2, 2)):
                there = self.buf.at[rows((z * Y + lax.rem(y + step, Y)) * UNIT, UNIT)]
                received(there, ay_s.at[self.n, k], ay_r.at[self.n, k])

    offsets = (0, -1, 1, -2, 2, -3, 3, 4)

    class OverZY(FastZ):
        def __init__(self, n, buf, f=None):
            self.n, self.buf, self.f = n, buf, f

        def piece(self, off, half):
            first = self.unit(off, 0)
            if half is None:
                return self.buf.at[rows(first, UNIT)]
            return self.buf.at[rows(first + half * 16, 16)]

        def unit(self, off, y_step):
            return (lax.rem(z + off + Z, Z) * Y + lax.rem(y + y_step, Y)) * UNIT

        def y_send(self, j, k, y_step, peer):
            here = self.buf.at[rows(self.unit(offsets[j], y_step), UNIT)]
            send(here, here, by_s.at[self.n, j, k], by_r.at[self.n, j, k], peer)

        def y_wait(self, j, k, y_step):
            there = self.buf.at[rows(self.unit(offsets[j], y_step), UNIT)]
            received(there, by_s.at[self.n, j, k], by_r.at[self.n, j, k])

        def y_start(self, *slots):
            for j in slots:
                self.y_send(j, 0, 0, y_next)
                self.y_send(j, 1, 0, y_prev)

        def y_relay(self, *slots):
            for j in slots:
                if j % 2 == 0:
                    self.y_wait(j, 0, 3)
                    self.y_send(j, 2, 3, y_next)
                    self.y_wait(j, 1, 1)
                else:
                    self.y_wait(j, 1, 1)
                    self.y_send(j, 2, 1, y_prev)
                    self.y_wait(j, 0, 3)

        def y_end(self, *slots):
            for j in slots:
                self.y_wait(j, 2, 2)

    w_k, w_g, w_u = OverYZ(0, b_k, 0), OverYZ(1, b_g, 1), OverYZ(2, b_u, 2)
    w_v, w_qo, w_ld = OverZY(0, b_v, 3), OverZY(1, b_qo, 4), OverZY(2, b_ld, 5)

    for k in (0, 1, 2, 3, 4, 5, 6, 7):
        loads[k].wait()
    tokens = tok[...].astype(F32)
    xn[rows(tp * OWN, OWN)] = rms(tokens, g_in[...]).astype(BF16)
    for k in range(8, len(loads)):
        loads[k].wait()
    b_u[own] = jnp.zeros((UNIT, FFP), BF16)
    b_u[own, 0:FFOWN] = s_u[...]
    b_ld[own] = jnp.zeros((UNIT, 2 * FFP), BF16)
    b_ld[own, 0:FFOWN] = s_l[...]
    b_ld[own, FFP : FFP + FFOWN] = s_d[...]

    pl.semaphore_wait(barrier, 10)

    ag_start(0, xn, 0, 2)
    w_v.fast_start()
    w_k.y_start()
    w_v.y_start(0)
    ag_start(0, xn, 1, 3)
    w_qo.fast_start()
    w_g.y_start()
    w_qo.y_start(0)

    log_f = -jnp.log1p(jnp.exp(-logits[0:1, 0:1]))
    log_b = -jnp.log1p(jnp.exp(-logits[0:1, 1:2]))
    at = lax.broadcasted_iota(jnp.int32, (BLOCK, BLOCK), 0)
    lane = lax.broadcasted_iota(jnp.int32, (BLOCK, BLOCK), 1)
    apart = (at - lane).astype(F32)
    dmat[...] = jnp.exp(jnp.where(at >= lane, apart * log_f, -apart * log_b))
    ahead = at.astype(F32)
    lead[...] = jnp.exp(
        jnp.where(lane < DK, (ahead + 1.0) * log_f, (float(BLOCK) - ahead) * log_b)
    )
    tail[...] = jnp.exp(jnp.where(lane < DK, (BLOCK - 1.0 - ahead) * log_f, ahead * log_b))
    step_f, step_b = jnp.exp(BLOCK * log_f), jnp.exp(BLOCK * log_b)
    taps[...] = jnp.zeros((16, FFP), F32)
    taps[0:3, 0:FFOWN] = k_gelu[...]
    taps[3:4, 0:FFOWN] = bias_g[...].reshape(1, FFOWN)
    taps[8:11, 0:FFOWN] = k_linear[...]
    taps[11:12, 0:FFOWN] = bias_l[...].reshape(1, FFOWN)
    up[0:8] = jnp.zeros((8, 2 * FFP), F32)
    up[SEQ + 8 : SEQ + 16] = jnp.zeros((8, 2 * FFP), F32)

    w_v.fast_relay()
    w_v.fast_one()
    w_v.y_start(1, 2, 3, 4)
    w_k.y_wait()
    w_k.fast_start()
    ag_first(0, xn, 0, 2)
    w_qo.fast_relay()
    w_qo.fast_one()
    qo_y = prepare(lambda: w_qo.y_start(1, 2, 3, 4))
    start_on(0, qo_y)
    w_g.y_wait()
    w_g.start_two()
    w_v.y_relay(0)
    ag_first(0, xn, 1, 3)
    w_v.fast_end()
    w_v.y_start(5, 6, 7)
    w_v.y_relay(1, 2, 3, 4)
    start_on(1, qo_y)
    w_qo.y_relay(0)
    w_k.fast_relay()
    w_g.start_one()
    w_qo.fast_end()
    qo_late = prepare(lambda: w_qo.y_start(5, 6))
    start_on(0, qo_late)
    ag_second(0, xn, 0, 2)
    w_v.y_relay(5, 6, 7)
    start_on(1, qo_late)
    w_qo.y_start(7)
    ag_second(0, xn, 1, 3)
    w_qo.y_relay(1, 2, 3, 4)
    w_g.fast_relay()
    ag_sibling(0, xn, 0)
    ag_sibling(0, xn, 1)
    ag_sibling(0, xn, 3)
    ag_sibling(0, xn, 2)
    w_k.fast_one()
    w_k.fast_end()
    w_v.y_end(*range(8))
    w_qo.y_relay(5, 6, 7)

    def between_mixer(n):
        if n == 1:
            w_ld.fast_relay()
            w_u.y_wait()
            w_u.fast_start()
        elif n == 2:
            w_ld.fast_one()
            w_ld.y_start(1, 2, 3, 4)

    def turn(values, i):
        base = outer[rows(i * 8, 8)][0:1]
        base_cos, base_sin = base[:, 0:128], base[:, 128:256]
        cosine = base_cos * inner[:, 0:128] - base_sin * inner[:, 128:256]
        sine = base_sin * inner[:, 0:128] + base_cos * inner[:, 128:256]
        return values * cosine + pltpu.roll(values, 64, 1) * sine

    for pair in range(2):
        wide = slice(pair * 2 * BLOCK, (pair + 1) * 2 * BLOCK)
        k_wide = dot(xn[wide], b_k[...])
        v_wide = dot(xn[wide], b_v[...]).astype(BF16)
        vs[wide] = v_wide
        for n in range(2):
            i = 2 * pair + n
            here, inside = slice(i * BLOCK, (i + 1) * BLOCK), slice(n * BLOCK, (n + 1) * BLOCK)
            k = (turn(k_wide[inside], i) * DK**-0.5).astype(BF16)
            ks[here] = k
            kf = k.astype(F32)
            k_two = (jnp.concatenate([kf, kf], axis=1) * tail[...]).astype(BF16)
            us[here] = dot(k_two, v_wide[inside], TN)
        if pair == 0:
            w_u.y_start()
            w_ld.fast_start()
            w_ld.y_start(0)

    total = jnp.zeros((DK, DV), F32)
    for i in range(X):
        st[i * BLOCK : i * BLOCK + DK] = total.astype(BF16)
        total = step_f * total + us[i * BLOCK : i * BLOCK + DK]
    total = jnp.zeros((DK, DV), F32)
    for i in reversed(range(X)):
        st[i * BLOCK + DK : (i + 1) * BLOCK] = total.astype(BF16)
        total = step_b * total + us[i * BLOCK + DK : (i + 1) * BLOCK]


    w_g.fast_one()
    w_g.fast_end()
    for pair in range(2):
        wide = slice(pair * 2 * BLOCK, (pair + 1) * 2 * BLOCK)
        gates = dot(xn[wide], b_g[...])
        silu[wide] = gates / (1.0 + jnp.exp(-gates))
    w_qo.y_end(*range(8))

    first_sends = len(sent)

    def rs_block(t, d, left, weights, first, width):
        left = jnp.concatenate([left[rows((1 - c) * OWN, OWN)], left[rows(c * OWN, OWN)]], axis=0)
        there = slice(d * OWN, (d + 1) * OWN)
        for j in range(4):
            columns = slice(j * 256, (j + 1) * 256)
            part = dot(left, weights[columns, first : first + width], NT)
            ps[t, there, columns] = part[:OWN].astype(BF16)
            pf[there, columns] = part[OWN:]
        for p in (0, 2, 1, 3):
            send(
                ps.at[t, pl.ds(d * OWN + p * PIECE, PIECE)],
                pr.at[t, d, pl.ds(p * PIECE, PIECE)], pp_s.at[t, d, p], pp_r.at[t, d, p], sibling,
            )

    def rs_pair(t, d, p):
        received(pr.at[t, d, pl.ds(p * PIECE, PIECE)], pp_s.at[t, d, p], pp_r.at[t, d, p])
        mine = pf[d * OWN + p * PIECE : d * OWN + (p + 1) * PIECE]
        return mine + pr[t, d, p * PIECE : (p + 1) * PIECE].astype(F32)

    def rs_far(t):
        for p in (0, 2, 1, 3):
            rs_send[t, p] = rs_pair(t, 2, p).astype(BF16)
            peer = x_next if p < 2 else x_prev
            send(rs_send.at[t, p], rs_recv.at[t, p], rr_s.at[t, p], rr_r.at[t, p], peer)

    def rs_near(t, way, p, relay):
        total = rs_pair(t, 1 if way == 0 else 3, p)
        if relay:
            received(rs_recv.at[t, p], rr_s.at[t, p], rr_r.at[t, p])
            total = total + rs_recv[t, p].astype(F32)
        k = way * 4 + p
        ms_send[t, k] = total.astype(BF16)
        peer = x_next if way == 0 else x_prev
        send(ms_send.at[t, k], ms_recv.at[t, k], mm_s.at[t, k], mm_r.at[t, k], peer)

    def rs_final(t, p):
        total = rs_pair(t, 0, p)
        for k in (p, 4 + p):
            received(ms_recv.at[t, k], mm_s.at[t, k], mm_r.at[t, k])
            total = total + ms_recv[t, k].astype(F32)
        return total

    def reduce_scatter(t, block, weights, first, width, between):
        for n, d in enumerate((2, 1, 3, 0)):
            rs_block(t, d, block(d), weights, first, width)
            if n == 1:
                rs_far(t)
            if n == 2:
                rs_near(t, 0, 2, False)
            if n == 3:
                rs_near(t, 1, 0, False)
            between(n)
        rs_near(t, 0, 0, True)
        rs_near(t, 1, 2, True)
        rs_near(t, 0, 3, False)
        rs_near(t, 1, 1, False)
        rs_near(t, 0, 1, True)
        rs_near(t, 1, 3, True)

    def mixer_block(d):
        i = lax.rem(x + d, X)
        here = rows(i * BLOCK, BLOCK)
        q = turn(dot(xn[here], b_qo[:, 0:DK]), i).astype(BF16)
        scores = (dot(q, ks[here], NT) * dmat[...]).astype(BF16)
        qf = q.astype(F32)
        q_two = (jnp.concatenate([qf, qf], axis=1) * lead[...]).astype(BF16)
        retained = dot(scores, vs[here]) + dot(q_two, st[here])
        centred = retained - jnp.mean(retained, axis=-1, keepdims=True)
        normal = centred * lax.rsqrt(jnp.mean(centred * centred, axis=-1, keepdims=True) + EPS)
        gated[...] = (normal * silu[here]).astype(BF16)
        return gated

    reduce_scatter(0, mixer_block, b_qo, DK, DV, between_mixer)
    w_ld.fast_end()
    w_ld.y_start(5, 6, 7)
    for n, p in enumerate((0, 2, 1, 3)):
        part = slice(p * PIECE, (p + 1) * PIECE)
        mixed = rs_final(0, p)
        summed = (tok[part].astype(F32) + rms(mixed, g_mo[...])).astype(BF16).astype(F32)
        after[part] = summed
        ch[rows(tp * OWN + p * PIECE, PIECE)] = rms(summed, g_ci[...]).astype(BF16)
        ag_start(1, ch, p)
        if n == 0:
            w_ld.y_relay(0, 1, 2)
        elif n == 1:
            w_u.fast_relay()
        elif n == 2:
            w_ld.y_relay(3, 4)

    w_ld.y_relay(5, 6, 7)
    drain(first_sends)
    before_last = len(sent)
    ag_first(1, ch, 0, 2)
    ag_first(1, ch, 1, 3)

    def expand(d, core=None):
        count = BLOCK if core is None else OWN
        first = lax.rem(x + d, X) * BLOCK + (0 if core is None else core * OWN)
        there = pl.ds(pl.multiple_of(first + 8, 8), count)
        left = ch[rows(first, count)]
        up[there, 0:256] = dot(left, b_u[:, 0:256])
        up[there, 256:512] = dot(left, jnp.concatenate([b_u[:, 256:384], b_ld[:, 0:128]], axis=1))
        up[there, 512:768] = dot(left, b_ld[:, 128:384])

    w_u.fast_one()
    w_u.fast_end()
    w_ld.y_end(*range(8))
    ag_sibling(1, ch, 0)
    expand(0)
    ag_second(1, ch, 0, 2)
    ag_sibling(1, ch, 1)
    expand(1)
    ag_second(1, ch, 1, 3)
    ag_sibling(1, ch, 3)
    expand(3)
    expand(2, c)
    ag_sibling(1, ch, 2)
    expand(2, 1 - c)

    def conv(first, column, at):
        near = up[pl.ds(pl.multiple_of(first, 8), 80), column : column + FFP]
        before = pltpu.roll(near, 1, 0)[8:72]
        behind = pltpu.roll(near, 79, 0)[8:72]
        return (
            taps[at : at + 1] * before
            + taps[at + 1 : at + 2] * near[8:72]
            + taps[at + 2 : at + 3] * behind
            + taps[at + 3 : at + 4]
        )

    def channel_block(d):
        i = lax.rem(x + d, X)

        def tile(n, carry):
            first = i * BLOCK + n * HALF
            g = conv(first, 0, 0)
            act = 0.5 * g * (1.0 + jnp.tanh(0.7978845608028654 * (g + 0.044715 * g * g * g)))
            hid[pl.ds(pl.multiple_of(n * HALF, HALF), HALF)] = (
                act * conv(first, FFP, 8)
            ).astype(BF16)
            return carry

        lax.fori_loop(0, BLOCK // HALF, tile, 0)
        return hid

    reduce_scatter(1, channel_block, b_ld, FFP, FFP, lambda n: None)
    drain(before_last)
    for p in (0, 2, 1, 3):
        part = slice(p * PIECE, (p + 1) * PIECE)
        out[part] = (after[part] + rms(rs_final(1, p), g_co[...])).astype(BF16)

    for copy in sent:
        copy.wait_send()


def layer(
    tokens, mixer_in_gain, query_weight, key_weight, value_weight, gate_weight, decay_logits,
    mixer_output, mixer_out_gain, channel_in_gain, gelu_weight, linear_weight, gelu_kernel,
    linear_kernel, gelu_bias, linear_bias, down_weight, channel_out_gain,
):
    inner, outer = rotation_tables()

    def row(v):
        return v.reshape(1, -1)

    operands = (
        tokens[0], row(mixer_in_gain), query_weight, key_weight, value_weight, gate_weight,
        decay_logits.T, mixer_output.T, row(mixer_out_gain), row(channel_in_gain), gelu_weight,
        linear_weight, gelu_kernel, linear_kernel, gelu_bias, linear_bias, down_weight.T,
        row(channel_out_gain), jnp.asarray(inner), jnp.asarray(outer),
    )
    operands = [pltpu.with_memory_space_constraint(v, pltpu.HBM) for v in operands]
    dma = pltpu.SemaphoreType.DMA
    result = pl.pallas_call(
        kernel,
        out_shape=pltpu.VMEM((OWN, D), BF16),
        in_specs=[pl.BlockSpec(memory_space=pltpu.HBM)] * len(operands),
        out_specs=pl.BlockSpec(memory_space=pltpu.VMEM),
        scratch_shapes=[
            pltpu.VMEM((OWN, D), BF16),
            pltpu.VMEM((1, D), F32),
            pltpu.VMEM((1, 2), F32),
            pltpu.VMEM((1, D), F32),
            pltpu.VMEM((1, D), F32),
            pltpu.VMEM((3, FFOWN), F32),
            pltpu.VMEM((3, FFOWN), F32),
            pltpu.VMEM((FFOWN,), F32),
            pltpu.VMEM((FFOWN,), F32),
            pltpu.VMEM((1, D), F32),
            pltpu.VMEM((BLOCK, 256), F32),
            pltpu.VMEM((8 * X, 256), F32),
            pltpu.VMEM((UNIT, FFOWN), BF16),
            pltpu.VMEM((UNIT, FFOWN), BF16),
            pltpu.VMEM((UNIT, FFOWN), BF16),
            pltpu.VMEM((SEQ, D), BF16),
            pltpu.VMEM((SEQ, D), BF16),
            pltpu.VMEM((D, DK), BF16),
            pltpu.VMEM((D, DV), BF16),
            pltpu.VMEM((D, FFP), BF16),
            pltpu.VMEM((D, DV), BF16),
            pltpu.VMEM((D, DK + DV), BF16),
            pltpu.VMEM((D, 2 * FFP), BF16),
            pltpu.VMEM((SEQ, DK), BF16),
            pltpu.VMEM((SEQ, DV), BF16),
            pltpu.VMEM((SEQ, DV), F32),
            pltpu.VMEM((SEQ, DV), F32),
            pltpu.VMEM((SEQ, DV), BF16),
            pltpu.VMEM((BLOCK, BLOCK), F32),
            pltpu.VMEM((BLOCK, BLOCK), F32),
            pltpu.VMEM((BLOCK, BLOCK), F32),
            pltpu.VMEM((4 * OWN, D), F32),
            pltpu.VMEM((2, 4 * OWN, D), BF16),
            pltpu.VMEM((2, 4, OWN, D), BF16),
            pltpu.VMEM((2, 4, PIECE, D), BF16),
            pltpu.VMEM((2, 4, PIECE, D), BF16),
            pltpu.VMEM((2, 8, PIECE, D), BF16),
            pltpu.VMEM((2, 8, PIECE, D), BF16),
            pltpu.VMEM((SEQ + 16, 2 * FFP), F32),
            pltpu.VMEM((BLOCK, FFP), BF16),
            pltpu.VMEM((BLOCK, DV), BF16),
            pltpu.VMEM((OWN, D), F32),
            pltpu.VMEM((16, FFP), F32),
            dma((20,)),
            dma((2, 28)), dma((2, 28)),
            dma((3, 3)), dma((3, 3)),
            dma((3, 8, 3)), dma((3, 8, 3)),
            dma((6, 8)), dma((6, 8)),
            dma((2, 4, 4)), dma((2, 4, 4)),
            dma((2, 4)), dma((2, 4)),
            dma((2, 8)), dma((2, 8)),
        ],
        compiler_params=pltpu.CompilerParams(
            collective_id=0, has_side_effects=True, vmem_limit_bytes=40 * 1024 * 1024
        ),
        name="layer",
    )(*operands)
    return result[None]


def solution(mesh):
    by_position = P(("rep", "fs"), "tp", None)
    up_rows, down_rows = P("fs", "tp"), P("tp", "fs")
    in_specs = (
        by_position, P(), up_rows, up_rows, up_rows, up_rows, P(None, "tp"), down_rows, P(), P(),
        up_rows, up_rows, P(None, "tp"), P(None, "tp"), P("tp"), P("tp"), down_rows, P(),
    )
    return jax.shard_map(
        layer, mesh=mesh, in_specs=in_specs, out_specs=by_position, check_vma=False
    )
```

```python
import jax
import jax.numpy as jnp
import numpy as np
from jax import lax
from jax.experimental import pallas as pl
from jax.experimental.pallas import tpu as pltpu
from jax.sharding import PartitionSpec as P

MESH = pl.DeviceIdType.MESH
F32 = jnp.float32
BF16 = jnp.bfloat16

X, Y, Z, ZALL = 4, 4, 8, 16
D = 1024
DK = 128
DV = 256
SEQ = 1024
OWN = 128
HALF = 64
PIECE = 32
BLOCK = 256
UNIT = 32
FFP = 384
FFOWN = 352
EPS = 1e-6
NT = (((1,), (1,)), ((), ()))
TN = (((0,), (0,)), ((), ()))


def rotation_tables():
    frequency = 10000.0 ** (-np.arange(64, dtype=np.float64) / 64)

    def pair(positions):
        angles = positions[:, None] * frequency[None, :]
        cosine, sine = np.cos(angles), np.sin(angles)
        return np.concatenate([cosine, cosine], 1), np.concatenate([-sine, sine], 1)

    inner = np.concatenate(pair(np.arange(BLOCK, dtype=np.float64)), 1)
    outer = np.concatenate(pair(BLOCK * np.repeat(np.arange(X, dtype=np.float64), 8)), 1)
    return inner.astype(np.float32), outer.astype(np.float32)


def dot(a, b, dims=None):
    if dims is None:
        return jnp.dot(a, b, preferred_element_type=F32)
    return lax.dot_general(a, b, dims, preferred_element_type=F32)


def rms(values, gain):
    return values * lax.rsqrt(jnp.mean(values * values, axis=-1, keepdims=True) + EPS) * gain


def kernel(
    h_tok, h_g_in, h_wq, h_wk, h_wv, h_wg, h_logits, h_wo, h_g_mo, h_g_ci, h_gelu, h_linear,
    h_k_gelu, h_k_linear, h_b_gelu, h_b_linear, h_wd, h_g_co, h_inner, h_outer,
    out,
    tok, g_in, logits, g_mo, g_ci, k_gelu, k_linear, bias_g, bias_l, g_co, inner, outer,
    s_u, s_l, s_d,
    xn, ch, b_k, b_g, b_u, b_v, b_qo, b_ld, ks, vs, silu, us, st, dmat, lead, tail, pf, ps, pr, rs_send, rs_recv,
    ms_send, ms_recv, up, hid, gated, after, taps,
    in_s, ag_s, ag_r, ay_s, ay_r, by_s, by_r, fz_s, fz_r, pp_s, pp_r, rr_s, rr_r, mm_s, mm_r,
):
    rep, fs, tp = lax.axis_index("rep"), lax.axis_index("fs"), lax.axis_index("tp")
    x, c = tp // 2, tp % 2
    z, y = fs // Y, fs % Y
    zz = rep * Z + z

    def x_dev(step):
        return (rep, fs, lax.rem(x + step, X) * 2 + c)

    def y_dev(step):
        return (rep, z * Y + lax.rem(y + step, Y), tp)

    def z_dev(step):
        there = lax.rem(zz + step, ZALL)
        return (there // Z, lax.rem(there, Z) * Y + y, tp)

    sibling = (rep, fs, x * 2 + (1 - c))
    x_next, x_prev = x_dev(1), x_dev(X - 1)
    y_next, y_prev, y_far = y_dev(1), y_dev(Y - 1), y_dev(2)
    z_next, z_prev = z_dev(1), z_dev(ZALL - 1)
    z_two = (z_dev(2), z_dev(ZALL - 2))

    barrier = pltpu.get_barrier_semaphore()
    for peer in (x_next, x_prev, sibling, y_next, y_prev, y_far, z_next, z_prev, *z_two):
        pl.semaphore_signal(barrier, inc=1, device_id=peer, device_id_type=MESH)

    def rows(first, count):
        return pl.ds(pl.multiple_of(first, count), count)

    own = rows(fs * UNIT, UNIT)
    loads = [
        pltpu.make_async_copy(src, dst, in_s.at[k])
        for k, (src, dst) in enumerate((
            (h_tok, tok), (h_g_in, g_in), (h_wq, b_qo.at[own, 0:128]), (h_wk, b_k.at[own]),
            (h_wv, b_v.at[own]), (h_wg, b_g.at[own]), (h_wo, b_qo.at[own, 128:384]), (h_logits, logits),
            (h_gelu, s_u), (h_linear, s_l), (h_wd, s_d), (h_k_gelu, k_gelu), (h_k_linear, k_linear),
            (h_b_gelu, bias_g), (h_b_linear, bias_l), (h_g_mo, g_mo), (h_g_ci, g_ci), (h_g_co, g_co),
            (h_inner, inner), (h_outer, outer),
        ))
    ]
    for load in loads:
        load.start()

    sent = []

    def drain(count):
        for copy in sent[:count]:
            copy.wait_send()
        del sent[:count]


    held = [None]

    def send(src, dst, send_sem, recv_sem, peer):
        copy = pltpu.make_async_remote_copy(
            src_ref=src, dst_ref=dst, send_sem=send_sem, recv_sem=recv_sem,
            device_id=peer, device_id_type=MESH,
        )
        sent.append(copy)
        if held[0] is None:
            copy.start()
        else:
            held[0].append(copy)

    def prepare(*sends):
        held[0] = []
        for one in sends:
            one()
        copies, held[0] = held[0], None
        return copies

    def start_on(core, copies):
        @pl.when(c == core)
        def _():
            for copy in copies:
                copy.start()

    def received(dst, send_sem, recv_sem):
        pltpu.make_async_remote_copy(
            src_ref=dst, dst_ref=dst, send_sem=send_sem, recv_sem=recv_sem,
            device_id=sibling, device_id_type=MESH,
        ).wait_recv()

    def ag_place(buf, d, core, p):
        chip = lax.rem(x + d, X)
        return buf.at[rows((chip * 2 + core) * OWN + p * PIECE, PIECE)]

    def ag_send(t, buf, k, d, p, peer):
        here = ag_place(buf, d, c, p)
        send(here, here, ag_s.at[t, k], ag_r.at[t, k], peer)

    def ag_wait(t, buf, k, d, core, p):
        received(ag_place(buf, d, core, p), ag_s.at[t, k], ag_r.at[t, k])

    def ag_start(t, buf, *pieces):
        for p in pieces:
            ag_send(t, buf, p, 0, p, x_next)
            ag_send(t, buf, 4 + p, 0, p, x_prev)
            ag_send(t, buf, 12 + p, 0, p, sibling)

    def ag_first(t, buf, *pieces):
        for p in pieces:
            ag_wait(t, buf, p, 3, c, p)
            if p < 2:
                ag_send(t, buf, 8 + p, 3, p, x_next)
            ag_send(t, buf, 24 + p, 3, p, sibling)
            ag_wait(t, buf, 4 + p, 1, c, p)
            if p >= 2:
                ag_send(t, buf, 8 + p, 1, p, x_prev)
            ag_send(t, buf, 16 + p, 1, p, sibling)

    def ag_second(t, buf, *pieces):
        for p in pieces:
            ag_wait(t, buf, 8 + p, 2, c, p)
            ag_send(t, buf, 20 + p, 2, p, sibling)

    def ag_sibling(t, buf, d):
        for p in range(4):
            ag_wait(t, buf, 12 + 4 * d + p, d, 1 - c, p)

    class FastZ:
        def hop(self, off, k, peer, piece=None):
            here = self.piece(off, piece)
            send(here, here, fz_s.at[self.f, k], fz_r.at[self.f, k], peer)

        def landed(self, off, k, piece=None):
            received(self.piece(off, piece), fz_s.at[self.f, k], fz_r.at[self.f, k])

        def start_two(self):
            self.hop(0, 1, z_two[0])
            self.hop(0, 5, z_two[1])

        def start_one(self):
            self.hop(0, 0, z_next)
            self.hop(0, 4, z_prev)

        def fast_start(self):
            self.start_two()
            self.start_one()

        def fast_one(self):
            self.landed(-1, 0)
            self.landed(1, 4)

        def fast_relay(self):
            self.landed(-2, 1)
            self.hop(-2, 3, z_two[0], 0)
            self.hop(-2, 2, z_next)
            self.landed(2, 5)
            self.hop(2, 7, z_two[1], 1)
            self.hop(2, 6, z_prev)

        def fast_end(self):
            self.landed(-3, 2)
            self.landed(3, 6)
            self.landed(4, 3, 0)
            self.landed(4, 7, 1)

    class OverYZ(FastZ):
        def __init__(self, n, buf, f=None):
            self.n, self.buf, self.f = n, buf, f

        def piece(self, off, half):
            first = lax.rem(z + off + Z, Z) * (Y * UNIT)
            if half is None:
                return self.buf.at[rows(first, Y * UNIT)]
            return self.buf.at[rows(first + half * HALF, HALF)]

        def y_start(self):
            here = self.buf.at[rows(fs * UNIT, UNIT)]
            for k, peer in ((0, y_next), (1, y_prev), (2, y_far)):
                send(here, here, ay_s.at[self.n, k], ay_r.at[self.n, k], peer)

        def y_wait(self):
            for k, step in ((0, Y - 1), (1, 1), (2, 2)):
                there = self.buf.at[rows((z * Y + lax.rem(y + step, Y)) * UNIT, UNIT)]
                received(there, ay_s.at[self.n, k], ay_r.at[self.n, k])

    offsets = (0, -1, 1, -2, 2, -3, 3, 4)

    class OverZY(FastZ):
        def __init__(self, n, buf, f=None):
            self.n, self.buf, self.f = n, buf, f

        def piece(self, off, half):
            first = self.unit(off, 0)
            if half is None:
                return self.buf.at[rows(first, UNIT)]
            return self.buf.at[rows(first + half * 16, 16)]

        def unit(self, off, y_step):
            return (lax.rem(z + off + Z, Z) * Y + lax.rem(y + y_step, Y)) * UNIT

        def y_send(self, j, k, y_step, peer):
            here = self.buf.at[rows(self.unit(offsets[j], y_step), UNIT)]
            send(here, here, by_s.at[self.n, j, k], by_r.at[self.n, j, k], peer)

        def y_wait(self, j, k, y_step):
            there = self.buf.at[rows(self.unit(offsets[j], y_step), UNIT)]
            received(there, by_s.at[self.n, j, k], by_r.at[self.n, j, k])

        def y_start(self, *slots):
            for j in slots:
                self.y_send(j, 0, 0, y_next)
                self.y_send(j, 1, 0, y_prev)

        def y_relay(self, *slots):
            for j in slots:
                if j % 2 == 0:
                    self.y_wait(j, 0, 3)
                    self.y_send(j, 2, 3, y_next)
                    self.y_wait(j, 1, 1)
                else:
                    self.y_wait(j, 1, 1)
                    self.y_send(j, 2, 1, y_prev)
                    self.y_wait(j, 0, 3)

        def y_end(self, *slots):
            for j in slots:
                self.y_wait(j, 2, 2)

    w_k, w_g, w_u = OverYZ(0, b_k, 0), OverYZ(1, b_g, 1), OverYZ(2, b_u, 2)
    w_v, w_qo, w_ld = OverZY(0, b_v, 3), OverZY(1, b_qo, 4), OverZY(2, b_ld, 5)

    for k in (0, 1, 2, 3, 4, 5, 6, 7):
        loads[k].wait()
    tokens = tok[...].astype(F32)
    xn[rows(tp * OWN, OWN)] = rms(tokens, g_in[...]).astype(BF16)
    for k in range(8, len(loads)):
        loads[k].wait()
    b_u[own] = jnp.zeros((UNIT, FFP), BF16)
    b_u[own, 0:FFOWN] = s_u[...]
    b_ld[own] = jnp.zeros((UNIT, 2 * FFP), BF16)
    b_ld[own, 0:FFOWN] = s_l[...]
    b_ld[own, FFP : FFP + FFOWN] = s_d[...]

    pl.semaphore_wait(barrier, 10)

    ag_start(0, xn, 0, 2)
    w_v.fast_start()
    w_k.y_start()
    w_v.y_start(0)
    ag_start(0, xn, 1, 3)
    w_qo.fast_start()
    w_g.y_start()
    w_qo.y_start(0)

    log_f = -jnp.log1p(jnp.exp(-logits[0:1, 0:1]))
    log_b = -jnp.log1p(jnp.exp(-logits[0:1, 1:2]))
    at = lax.broadcasted_iota(jnp.int32, (BLOCK, BLOCK), 0)
    lane = lax.broadcasted_iota(jnp.int32, (BLOCK, BLOCK), 1)
    apart = (at - lane).astype(F32)
    dmat[...] = jnp.exp(jnp.where(at >= lane, apart * log_f, -apart * log_b))
    ahead = at.astype(F32)
    lead[...] = jnp.exp(
        jnp.where(lane < DK, (ahead + 1.0) * log_f, (float(BLOCK) - ahead) * log_b)
    )
    tail[...] = jnp.exp(jnp.where(lane < DK, (BLOCK - 1.0 - ahead) * log_f, ahead * log_b))
    step_f, step_b = jnp.exp(BLOCK * log_f), jnp.exp(BLOCK * log_b)
    taps[...] = jnp.zeros((16, FFP), F32)
    taps[0:3, 0:FFOWN] = k_gelu[...]
    taps[3:4, 0:FFOWN] = bias_g[...].reshape(1, FFOWN)
    taps[8:11, 0:FFOWN] = k_linear[...]
    taps[11:12, 0:FFOWN] = bias_l[...].reshape(1, FFOWN)
    up[0:8] = jnp.zeros((8, 2 * FFP), F32)
    up[SEQ + 8 : SEQ + 16] = jnp.zeros((8, 2 * FFP), F32)

    w_v.fast_relay()
    w_v.fast_one()
    w_v.y_start(1, 2, 3, 4)
    w_k.y_wait()
    w_k.fast_start()
    ag_first(0, xn, 0, 2)
    w_qo.fast_relay()
    w_qo.fast_one()
    qo_y = prepare(lambda: w_qo.y_start(1, 2, 3, 4))
    start_on(0, qo_y)
    w_g.y_wait()
    w_g.start_two()
    w_v.y_relay(0)
    w_v.fast_end()
    w_v.y_start(5, 6, 7)
    ag_first(0, xn, 1, 3)
    w_v.y_relay(1, 2, 3, 4)
    start_on(1, qo_y)
    w_qo.y_relay(0)
    w_k.fast_relay()
    w_g.start_one()
    w_qo.fast_end()
    qo_late = prepare(lambda: w_qo.y_start(5, 6))
    start_on(0, qo_late)
    ag_second(0, xn, 0, 2)
    w_v.y_relay(5, 6, 7)
    start_on(1, qo_late)
    w_qo.y_start(7)
    ag_second(0, xn, 1, 3)
    w_qo.y_relay(1, 2, 3, 4)
    w_g.fast_relay()
    ag_sibling(0, xn, 0)
    ag_sibling(0, xn, 1)
    ag_sibling(0, xn, 3)
    ag_sibling(0, xn, 2)
    w_k.fast_one()
    w_k.fast_end()
    w_v.y_end(*range(8))
    w_qo.y_relay(5, 6, 7)

    def between_mixer(n):
        if n == 1:
            w_ld.fast_relay()
            w_u.y_wait()
            w_u.fast_start()
        elif n == 2:
            w_ld.fast_one()
            w_ld.y_start(1, 2, 3, 4)

    def turn(values, i):
        base = outer[rows(i * 8, 8)][0:1]
        base_cos, base_sin = base[:, 0:128], base[:, 128:256]
        cosine = base_cos * inner[:, 0:128] - base_sin * inner[:, 128:256]
        sine = base_sin * inner[:, 0:128] + base_cos * inner[:, 128:256]
        return values * cosine + pltpu.roll(values, 64, 1) * sine

    for pair in range(2):
        wide = slice(pair * 2 * BLOCK, (pair + 1) * 2 * BLOCK)
        k_wide = dot(xn[wide], b_k[...])
        v_wide = dot(xn[wide], b_v[...]).astype(BF16)
        vs[wide] = v_wide
        for n in range(2):
            i = 2 * pair + n
            here, inside = slice(i * BLOCK, (i + 1) * BLOCK), slice(n * BLOCK, (n + 1) * BLOCK)
            k = (turn(k_wide[inside], i) * DK**-0.5).astype(BF16)
            ks[here] = k
            kf = k.astype(F32)
            k_two = (jnp.concatenate([kf, kf], axis=1) * tail[...]).astype(BF16)
            us[here] = dot(k_two, v_wide[inside], TN)
        if pair == 0:
            w_u.y_start()
            w_ld.fast_start()
            w_ld.y_start(0)

    total = jnp.zeros((DK, DV), F32)
    for i in range(X):
        st[i * BLOCK : i * BLOCK + DK] = total.astype(BF16)
        total = step_f * total + us[i * BLOCK : i * BLOCK + DK]
    total = jnp.zeros((DK, DV), F32)
    for i in reversed(range(X)):
        st[i * BLOCK + DK : (i + 1) * BLOCK] = total.astype(BF16)
        total = step_b * total + us[i * BLOCK + DK : (i + 1) * BLOCK]


    w_g.fast_one()
    w_g.fast_end()
    for pair in range(2):
        wide = slice(pair * 2 * BLOCK, (pair + 1) * 2 * BLOCK)
        gates = dot(xn[wide], b_g[...])
        silu[wide] = gates / (1.0 + jnp.exp(-gates))
    w_qo.y_end(*range(8))

    first_sends = len(sent)

    def rs_block(t, d, left, weights, first, width):
        left = jnp.concatenate([left[rows((1 - c) * OWN, OWN)], left[rows(c * OWN, OWN)]], axis=0)
        there = slice(d * OWN, (d + 1) * OWN)
        for j in range(4):
            columns = slice(j * 256, (j + 1) * 256)
            part = dot(left, weights[columns, first : first + width], NT)
            ps[t, there, columns] = part[:OWN].astype(BF16)
            pf[there, columns] = part[OWN:]
        for p in (0, 2, 1, 3):
            send(
                ps.at[t, pl.ds(d * OWN + p * PIECE, PIECE)],
                pr.at[t, d, pl.ds(p * PIECE, PIECE)], pp_s.at[t, d, p], pp_r.at[t, d, p], sibling,
            )

    def rs_pair(t, d, p):
        received(pr.at[t, d, pl.ds(p * PIECE, PIECE)], pp_s.at[t, d, p], pp_r.at[t, d, p])
        mine = pf[d * OWN + p * PIECE : d * OWN + (p + 1) * PIECE]
        return mine + pr[t, d, p * PIECE : (p + 1) * PIECE].astype(F32)

    def rs_far(t):
        for p in (0, 2, 1, 3):
            rs_send[t, p] = rs_pair(t, 2, p).astype(BF16)
            peer = x_next if p < 2 else x_prev
            send(rs_send.at[t, p], rs_recv.at[t, p], rr_s.at[t, p], rr_r.at[t, p], peer)

    def rs_near(t, way, p, relay):
        total = rs_pair(t, 1 if way == 0 else 3, p)
        if relay:
            received(rs_recv.at[t, p], rr_s.at[t, p], rr_r.at[t, p])
            total = total + rs_recv[t, p].astype(F32)
        k = way * 4 + p
        ms_send[t, k] = total.astype(BF16)
        peer = x_next if way == 0 else x_prev
        send(ms_send.at[t, k], ms_recv.at[t, k], mm_s.at[t, k], mm_r.at[t, k], peer)

    def rs_final(t, p):
        total = rs_pair(t, 0, p)
        for k in (p, 4 + p):
            received(ms_recv.at[t, k], mm_s.at[t, k], mm_r.at[t, k])
            total = total + ms_recv[t, k].astype(F32)
        return total

    def reduce_scatter(t, block, weights, first, width, between):
        for n, d in enumerate((2, 1, 3, 0)):
            rs_block(t, d, block(d), weights, first, width)
            if n == 1:
                rs_far(t)
            if n == 2:
                rs_near(t, 0, 2, False)
            if n == 3:
                rs_near(t, 1, 0, False)
            between(n)
        rs_near(t, 0, 0, True)
        rs_near(t, 1, 2, True)
        rs_near(t, 0, 3, False)
        rs_near(t, 1, 1, False)
        rs_near(t, 0, 1, True)
        rs_near(t, 1, 3, True)

    def mixer_block(d):
        i = lax.rem(x + d, X)
        here = rows(i * BLOCK, BLOCK)
        q = turn(dot(xn[here], b_qo[:, 0:DK]), i).astype(BF16)
        scores = (dot(q, ks[here], NT) * dmat[...]).astype(BF16)
        qf = q.astype(F32)
        q_two = (jnp.concatenate([qf, qf], axis=1) * lead[...]).astype(BF16)
        retained = dot(scores, vs[here]) + dot(q_two, st[here])
        centred = retained - jnp.mean(retained, axis=-1, keepdims=True)
        normal = centred * lax.rsqrt(jnp.mean(centred * centred, axis=-1, keepdims=True) + EPS)
        gated[...] = (normal * silu[here]).astype(BF16)
        return gated

    reduce_scatter(0, mixer_block, b_qo, DK, DV, between_mixer)
    w_ld.fast_end()
    w_ld.y_start(5, 6, 7)
    for n, p in enumerate((0, 2, 1, 3)):
        part = slice(p * PIECE, (p + 1) * PIECE)
        mixed = rs_final(0, p)
        summed = (tok[part].astype(F32) + rms(mixed, g_mo[...])).astype(BF16).astype(F32)
        after[part] = summed
        ch[rows(tp * OWN + p * PIECE, PIECE)] = rms(summed, g_ci[...]).astype(BF16)
        ag_start(1, ch, p)
        if n == 0:
            w_ld.y_relay(0, 1, 2)
        elif n == 1:
            w_u.fast_relay()
        elif n == 2:
            w_ld.y_relay(3, 4)

    w_ld.y_relay(5, 6, 7)
    drain(first_sends)
    before_last = len(sent)
    ag_first(1, ch, 0, 2)
    ag_first(1, ch, 1, 3)

    def expand(d, core=None):
        count = BLOCK if core is None else OWN
        first = lax.rem(x + d, X) * BLOCK + (0 if core is None else core * OWN)
        there = pl.ds(pl.multiple_of(first + 8, 8), count)
        left = ch[rows(first, count)]
        up[there, 0:256] = dot(left, b_u[:, 0:256])
        up[there, 256:512] = dot(left, jnp.concatenate([b_u[:, 256:384], b_ld[:, 0:128]], axis=1))
        up[there, 512:768] = dot(left, b_ld[:, 128:384])

    w_u.fast_one()
    w_u.fast_end()
    w_ld.y_end(*range(8))
    ag_sibling(1, ch, 0)
    expand(0)
    ag_second(1, ch, 0, 2)
    ag_sibling(1, ch, 1)
    expand(1)
    ag_second(1, ch, 1, 3)
    ag_sibling(1, ch, 3)
    expand(3)
    expand(2, c)
    ag_sibling(1, ch, 2)
    expand(2, 1 - c)

    def conv(first, column, at):
        near = up[pl.ds(pl.multiple_of(first, 8), 80), column : column + FFP]
        before = pltpu.roll(near, 1, 0)[8:72]
        behind = pltpu.roll(near, 79, 0)[8:72]
        return (
            taps[at : at + 1] * before
            + taps[at + 1 : at + 2] * near[8:72]
            + taps[at + 2 : at + 3] * behind
            + taps[at + 3 : at + 4]
        )

    def channel_block(d):
        i = lax.rem(x + d, X)

        def tile(n, carry):
            first = i * BLOCK + n * HALF
            g = conv(first, 0, 0)
            act = 0.5 * g * (1.0 + jnp.tanh(0.7978845608028654 * (g + 0.044715 * g * g * g)))
            hid[pl.ds(pl.multiple_of(n * HALF, HALF), HALF)] = (
                act * conv(first, FFP, 8)
            ).astype(BF16)
            return carry

        lax.fori_loop(0, BLOCK // HALF, tile, 0)
        return hid

    reduce_scatter(1, channel_block, b_ld, FFP, FFP, lambda n: None)
    drain(before_last)
    for p in (0, 2, 1, 3):
        part = slice(p * PIECE, (p + 1) * PIECE)
        out[part] = (after[part] + rms(rs_final(1, p), g_co[...])).astype(BF16)

    for copy in sent:
        copy.wait_send()


def layer(
    tokens, mixer_in_gain, query_weight, key_weight, value_weight, gate_weight, decay_logits,
    mixer_output, mixer_out_gain, channel_in_gain, gelu_weight, linear_weight, gelu_kernel,
    linear_kernel, gelu_bias, linear_bias, down_weight, channel_out_gain,
):
    inner, outer = rotation_tables()

    def row(v):
        return v.reshape(1, -1)

    operands = (
        tokens[0], row(mixer_in_gain), query_weight, key_weight, value_weight, gate_weight,
        decay_logits.T, mixer_output.T, row(mixer_out_gain), row(channel_in_gain), gelu_weight,
        linear_weight, gelu_kernel, linear_kernel, gelu_bias, linear_bias, down_weight.T,
        row(channel_out_gain), jnp.asarray(inner), jnp.asarray(outer),
    )
    operands = [pltpu.with_memory_space_constraint(v, pltpu.HBM) for v in operands]
    dma = pltpu.SemaphoreType.DMA
    result = pl.pallas_call(
        kernel,
        out_shape=pltpu.VMEM((OWN, D), BF16),
        in_specs=[pl.BlockSpec(memory_space=pltpu.HBM)] * len(operands),
        out_specs=pl.BlockSpec(memory_space=pltpu.VMEM),
        scratch_shapes=[
            pltpu.VMEM((OWN, D), BF16),
            pltpu.VMEM((1, D), F32),
            pltpu.VMEM((1, 2), F32),
            pltpu.VMEM((1, D), F32),
            pltpu.VMEM((1, D), F32),
            pltpu.VMEM((3, FFOWN), F32),
            pltpu.VMEM((3, FFOWN), F32),
            pltpu.VMEM((FFOWN,), F32),
            pltpu.VMEM((FFOWN,), F32),
            pltpu.VMEM((1, D), F32),
            pltpu.VMEM((BLOCK, 256), F32),
            pltpu.VMEM((8 * X, 256), F32),
            pltpu.VMEM((UNIT, FFOWN), BF16),
            pltpu.VMEM((UNIT, FFOWN), BF16),
            pltpu.VMEM((UNIT, FFOWN), BF16),
            pltpu.VMEM((SEQ, D), BF16),
            pltpu.VMEM((SEQ, D), BF16),
            pltpu.VMEM((D, DK), BF16),
            pltpu.VMEM((D, DV), BF16),
            pltpu.VMEM((D, FFP), BF16),
            pltpu.VMEM((D, DV), BF16),
            pltpu.VMEM((D, DK + DV), BF16),
            pltpu.VMEM((D, 2 * FFP), BF16),
            pltpu.VMEM((SEQ, DK), BF16),
            pltpu.VMEM((SEQ, DV), BF16),
            pltpu.VMEM((SEQ, DV), F32),
            pltpu.VMEM((SEQ, DV), F32),
            pltpu.VMEM((SEQ, DV), BF16),
            pltpu.VMEM((BLOCK, BLOCK), F32),
            pltpu.VMEM((BLOCK, BLOCK), F32),
            pltpu.VMEM((BLOCK, BLOCK), F32),
            pltpu.VMEM((4 * OWN, D), F32),
            pltpu.VMEM((2, 4 * OWN, D), BF16),
            pltpu.VMEM((2, 4, OWN, D), BF16),
            pltpu.VMEM((2, 4, PIECE, D), BF16),
            pltpu.VMEM((2, 4, PIECE, D), BF16),
            pltpu.VMEM((2, 8, PIECE, D), BF16),
            pltpu.VMEM((2, 8, PIECE, D), BF16),
            pltpu.VMEM((SEQ + 16, 2 * FFP), F32),
            pltpu.VMEM((BLOCK, FFP), BF16),
            pltpu.VMEM((BLOCK, DV), BF16),
            pltpu.VMEM((OWN, D), F32),
            pltpu.VMEM((16, FFP), F32),
            dma((20,)),
            dma((2, 28)), dma((2, 28)),
            dma((3, 3)), dma((3, 3)),
            dma((3, 8, 3)), dma((3, 8, 3)),
            dma((6, 8)), dma((6, 8)),
            dma((2, 4, 4)), dma((2, 4, 4)),
            dma((2, 4)), dma((2, 4)),
            dma((2, 8)), dma((2, 8)),
        ],
        compiler_params=pltpu.CompilerParams(
            collective_id=0, has_side_effects=True, vmem_limit_bytes=40 * 1024 * 1024
        ),
        name="layer",
    )(*operands)
    return result[None]


def solution(mesh):
    by_position = P(("rep", "fs"), "tp", None)
    up_rows, down_rows = P("fs", "tp"), P("tp", "fs")
    in_specs = (
        by_position, P(), up_rows, up_rows, up_rows, up_rows, P(None, "tp"), down_rows, P(), P(),
        up_rows, up_rows, P(None, "tp"), P(None, "tp"), P("tp"), P("tp"), down_rows, P(),
    )
    return jax.shard_map(
        layer, mesh=mesh, in_specs=in_specs, out_specs=by_position, check_vma=False
    )
```

```python
import jax
import jax.numpy as jnp
import numpy as np
from jax import lax
from jax.experimental import pallas as pl
from jax.experimental.pallas import tpu as pltpu
from jax.sharding import PartitionSpec as P

MESH = pl.DeviceIdType.MESH
F32 = jnp.float32
BF16 = jnp.bfloat16

X, Y, Z, ZALL = 4, 4, 8, 16
D = 1024
DK = 128
DV = 256
SEQ = 1024
OWN = 128
HALF = 64
PIECE = 32
BLOCK = 256
UNIT = 32
FFP = 384
FFOWN = 352
EPS = 1e-6
NT = (((1,), (1,)), ((), ()))
TN = (((0,), (0,)), ((), ()))


def rotation_tables():
    frequency = 10000.0 ** (-np.arange(64, dtype=np.float64) / 64)

    def pair(positions):
        angles = positions[:, None] * frequency[None, :]
        cosine, sine = np.cos(angles), np.sin(angles)
        return np.concatenate([cosine, cosine], 1), np.concatenate([-sine, sine], 1)

    inner = np.concatenate(pair(np.arange(BLOCK, dtype=np.float64)), 1)
    outer = np.concatenate(pair(BLOCK * np.repeat(np.arange(X, dtype=np.float64), 8)), 1)
    return inner.astype(np.float32), outer.astype(np.float32)


def dot(a, b, dims=None):
    if dims is None:
        return jnp.dot(a, b, preferred_element_type=F32)
    return lax.dot_general(a, b, dims, preferred_element_type=F32)


def rms(values, gain):
    return values * lax.rsqrt(jnp.mean(values * values, axis=-1, keepdims=True) + EPS) * gain


def kernel(
    h_tok, h_g_in, h_wq, h_wk, h_wv, h_wg, h_logits, h_wo, h_g_mo, h_g_ci, h_gelu, h_linear,
    h_k_gelu, h_k_linear, h_b_gelu, h_b_linear, h_wd, h_g_co, h_inner, h_outer,
    out,
    tok, g_in, logits, g_mo, g_ci, k_gelu, k_linear, bias_g, bias_l, g_co, inner, outer,
    s_u, s_l, s_d,
    xn, ch, b_k, b_g, b_u, b_v, b_qo, b_ld, ks, vs, silu, us, st, dmat, lead, tail, pf, ps, pr, rs_send, rs_recv,
    ms_send, ms_recv, up, hid, gated, after, taps,
    in_s, ag_s, ag_r, ay_s, ay_r, by_s, by_r, fz_s, fz_r, pp_s, pp_r, rr_s, rr_r, mm_s, mm_r,
):
    rep, fs, tp = lax.axis_index("rep"), lax.axis_index("fs"), lax.axis_index("tp")
    x, c = tp // 2, tp % 2
    z, y = fs // Y, fs % Y
    zz = rep * Z + z

    def x_dev(step):
        return (rep, fs, lax.rem(x + step, X) * 2 + c)

    def y_dev(step):
        return (rep, z * Y + lax.rem(y + step, Y), tp)

    def z_dev(step):
        there = lax.rem(zz + step, ZALL)
        return (there // Z, lax.rem(there, Z) * Y + y, tp)

    sibling = (rep, fs, x * 2 + (1 - c))
    x_next, x_prev = x_dev(1), x_dev(X - 1)
    y_next, y_prev, y_far = y_dev(1), y_dev(Y - 1), y_dev(2)
    z_next, z_prev = z_dev(1), z_dev(ZALL - 1)
    z_two = (z_dev(2), z_dev(ZALL - 2))

    barrier = pltpu.get_barrier_semaphore()
    for peer in (x_next, x_prev, sibling, y_next, y_prev, y_far, z_next, z_prev, *z_two):
        pl.semaphore_signal(barrier, inc=1, device_id=peer, device_id_type=MESH)

    def rows(first, count):
        return pl.ds(pl.multiple_of(first, count), count)

    own = rows(fs * UNIT, UNIT)
    loads = [
        pltpu.make_async_copy(src, dst, in_s.at[k])
        for k, (src, dst) in enumerate((
            (h_tok, tok), (h_g_in, g_in), (h_wq, b_qo.at[own, 0:128]), (h_wk, b_k.at[own]),
            (h_wv, b_v.at[own]), (h_wg, b_g.at[own]), (h_wo, b_qo.at[own, 128:384]), (h_logits, logits),
            (h_gelu, s_u), (h_linear, s_l), (h_wd, s_d), (h_k_gelu, k_gelu), (h_k_linear, k_linear),
            (h_b_gelu, bias_g), (h_b_linear, bias_l), (h_g_mo, g_mo), (h_g_ci, g_ci), (h_g_co, g_co),
            (h_inner, inner), (h_outer, outer),
        ))
    ]
    for load in loads:
        load.start()

    sent = []

    def drain(count):
        for copy in sent[:count]:
            copy.wait_send()
        del sent[:count]


    held = [None]

    def send(src, dst, send_sem, recv_sem, peer):
        copy = pltpu.make_async_remote_copy(
            src_ref=src, dst_ref=dst, send_sem=send_sem, recv_sem=recv_sem,
            device_id=peer, device_id_type=MESH,
        )
        sent.append(copy)
        if held[0] is None:
            copy.start()
        else:
            held[0].append(copy)

    def prepare(*sends):
        held[0] = []
        for one in sends:
            one()
        copies, held[0] = held[0], None
        return copies

    def start_on(core, copies):
        @pl.when(c == core)
        def _():
            for copy in copies:
                copy.start()

    def received(dst, send_sem, recv_sem):
        pltpu.make_async_remote_copy(
            src_ref=dst, dst_ref=dst, send_sem=send_sem, recv_sem=recv_sem,
            device_id=sibling, device_id_type=MESH,
        ).wait_recv()

    def ag_place(buf, d, core, p):
        chip = lax.rem(x + d, X)
        return buf.at[rows((chip * 2 + core) * OWN + p * PIECE, PIECE)]

    def ag_send(t, buf, k, d, p, peer):
        here = ag_place(buf, d, c, p)
        send(here, here, ag_s.at[t, k], ag_r.at[t, k], peer)

    def ag_wait(t, buf, k, d, core, p):
        received(ag_place(buf, d, core, p), ag_s.at[t, k], ag_r.at[t, k])

    def ag_start(t, buf, *pieces):
        for p in pieces:
            ag_send(t, buf, p, 0, p, x_next)
            ag_send(t, buf, 4 + p, 0, p, x_prev)
            ag_send(t, buf, 12 + p, 0, p, sibling)

    def ag_first(t, buf, *pieces):
        for p in pieces:
            ag_wait(t, buf, p, 3, c, p)
            if p < 2:
                ag_send(t, buf, 8 + p, 3, p, x_next)
            ag_send(t, buf, 24 + p, 3, p, sibling)
            ag_wait(t, buf, 4 + p, 1, c, p)
            if p >= 2:
                ag_send(t, buf, 8 + p, 1, p, x_prev)
            ag_send(t, buf, 16 + p, 1, p, sibling)

    def ag_second(t, buf, *pieces):
        for p in pieces:
            ag_wait(t, buf, 8 + p, 2, c, p)
            ag_send(t, buf, 20 + p, 2, p, sibling)

    def ag_sibling(t, buf, d):
        for p in range(4):
            ag_wait(t, buf, 12 + 4 * d + p, d, 1 - c, p)

    class FastZ:
        def hop(self, off, k, peer, piece=None):
            here = self.piece(off, piece)
            send(here, here, fz_s.at[self.f, k], fz_r.at[self.f, k], peer)

        def landed(self, off, k, piece=None):
            received(self.piece(off, piece), fz_s.at[self.f, k], fz_r.at[self.f, k])

        def start_two(self):
            self.hop(0, 1, z_two[0])
            self.hop(0, 5, z_two[1])

        def start_one(self):
            self.hop(0, 0, z_next)
            self.hop(0, 4, z_prev)

        def fast_start(self):
            self.start_two()
            self.start_one()

        def fast_one(self):
            self.landed(-1, 0)
            self.landed(1, 4)

        def fast_relay(self):
            self.landed(-2, 1)
            self.hop(-2, 3, z_two[0], 0)
            self.hop(-2, 2, z_next)
            self.landed(2, 5)
            self.hop(2, 7, z_two[1], 1)
            self.hop(2, 6, z_prev)

        def fast_end(self):
            self.landed(-3, 2)
            self.landed(3, 6)
            self.landed(4, 3, 0)
            self.landed(4, 7, 1)

    class OverYZ(FastZ):
        def __init__(self, n, buf, f=None):
            self.n, self.buf, self.f = n, buf, f

        def piece(self, off, half):
            first = lax.rem(z + off + Z, Z) * (Y * UNIT)
            if half is None:
                return self.buf.at[rows(first, Y * UNIT)]
            return self.buf.at[rows(first + half * HALF, HALF)]

        def y_start(self):
            here = self.buf.at[rows(fs * UNIT, UNIT)]
            for k, peer in ((0, y_next), (1, y_prev), (2, y_far)):
                send(here, here, ay_s.at[self.n, k], ay_r.at[self.n, k], peer)

        def y_wait(self):
            for k, step in ((0, Y - 1), (1, 1), (2, 2)):
                there = self.buf.at[rows((z * Y + lax.rem(y + step, Y)) * UNIT, UNIT)]
                received(there, ay_s.at[self.n, k], ay_r.at[self.n, k])

    offsets = (0, -1, 1, -2, 2, -3, 3, 4)

    class OverZY(FastZ):
        def __init__(self, n, buf, f=None):
            self.n, self.buf, self.f = n, buf, f

        def piece(self, off, half):
            first = self.unit(off, 0)
            if half is None:
                return self.buf.at[rows(first, UNIT)]
            return self.buf.at[rows(first + half * 16, 16)]

        def unit(self, off, y_step):
            return (lax.rem(z + off + Z, Z) * Y + lax.rem(y + y_step, Y)) * UNIT

        def y_send(self, j, k, y_step, peer):
            here = self.buf.at[rows(self.unit(offsets[j], y_step), UNIT)]
            send(here, here, by_s.at[self.n, j, k], by_r.at[self.n, j, k], peer)

        def y_wait(self, j, k, y_step):
            there = self.buf.at[rows(self.unit(offsets[j], y_step), UNIT)]
            received(there, by_s.at[self.n, j, k], by_r.at[self.n, j, k])

        def y_start(self, *slots):
            for j in slots:
                self.y_send(j, 0, 0, y_next)
                self.y_send(j, 1, 0, y_prev)

        def y_relay(self, *slots):
            for j in slots:
                if j % 2 == 0:
                    self.y_wait(j, 0, 3)
                    self.y_send(j, 2, 3, y_next)
                    self.y_wait(j, 1, 1)
                else:
                    self.y_wait(j, 1, 1)
                    self.y_send(j, 2, 1, y_prev)
                    self.y_wait(j, 0, 3)

        def y_end(self, *slots):
            for j in slots:
                self.y_wait(j, 2, 2)

    w_k, w_g, w_u = OverYZ(0, b_k, 0), OverYZ(1, b_g, 1), OverYZ(2, b_u, 2)
    w_v, w_qo, w_ld = OverZY(0, b_v, 3), OverZY(1, b_qo, 4), OverZY(2, b_ld, 5)

    for k in (0, 1, 2, 3, 4, 5, 6, 7):
        loads[k].wait()
    tokens = tok[...].astype(F32)
    xn[rows(tp * OWN, OWN)] = rms(tokens, g_in[...]).astype(BF16)
    for k in range(8, len(loads)):
        loads[k].wait()
    b_u[own] = jnp.zeros((UNIT, FFP), BF16)
    b_u[own, 0:FFOWN] = s_u[...]
    b_ld[own] = jnp.zeros((UNIT, 2 * FFP), BF16)
    b_ld[own, 0:FFOWN] = s_l[...]
    b_ld[own, FFP : FFP + FFOWN] = s_d[...]

    pl.semaphore_wait(barrier, 10)

    ag_start(0, xn, 0, 2)
    w_v.fast_start()
    w_k.y_start()
    w_v.y_start(0)
    ag_start(0, xn, 1, 3)
    w_qo.fast_start()
    w_g.y_start()
    w_qo.y_start(0)

    log_f = -jnp.log1p(jnp.exp(-logits[0:1, 0:1]))
    log_b = -jnp.log1p(jnp.exp(-logits[0:1, 1:2]))
    at = lax.broadcasted_iota(jnp.int32, (BLOCK, BLOCK), 0)
    lane = lax.broadcasted_iota(jnp.int32, (BLOCK, BLOCK), 1)
    apart = (at - lane).astype(F32)
    dmat[...] = jnp.exp(jnp.where(at >= lane, apart * log_f, -apart * log_b))
    ahead = at.astype(F32)
    lead[...] = jnp.exp(
        jnp.where(lane < DK, (ahead + 1.0) * log_f, (float(BLOCK) - ahead) * log_b)
    )
    tail[...] = jnp.exp(jnp.where(lane < DK, (BLOCK - 1.0 - ahead) * log_f, ahead * log_b))
    step_f, step_b = jnp.exp(BLOCK * log_f), jnp.exp(BLOCK * log_b)
    taps[...] = jnp.zeros((16, FFP), F32)
    taps[0:3, 0:FFOWN] = k_gelu[...]
    taps[3:4, 0:FFOWN] = bias_g[...].reshape(1, FFOWN)
    taps[8:11, 0:FFOWN] = k_linear[...]
    taps[11:12, 0:FFOWN] = bias_l[...].reshape(1, FFOWN)
    up[0:8] = jnp.zeros((8, 2 * FFP), F32)
    up[SEQ + 8 : SEQ + 16] = jnp.zeros((8, 2 * FFP), F32)

    w_v.fast_relay()
    w_v.fast_one()
    w_v.y_start(1, 2, 3, 4)
    w_k.y_wait()
    w_k.fast_start()
    ag_first(0, xn, 0, 2)
    w_qo.fast_relay()
    w_qo.fast_one()
    qo_y = prepare(lambda: w_qo.y_start(1, 2, 3, 4))
    start_on(0, qo_y)
    w_g.y_wait()
    w_g.start_two()
    w_v.y_relay(0)
    w_v.fast_end()
    w_v.y_start(5, 6, 7)
    ag_first(0, xn, 1, 3)
    w_v.y_relay(1, 2, 3, 4)
    start_on(1, qo_y)
    w_qo.y_relay(0)
    w_k.fast_relay()
    w_g.start_one()
    w_qo.fast_end()
    qo_late = prepare(lambda: w_qo.y_start(5, 6))
    start_on(0, qo_late)
    ag_second(0, xn, 0, 2)
    w_v.y_relay(5, 6, 7)
    start_on(1, qo_late)
    w_qo.y_start(7)
    ag_second(0, xn, 1, 3)
    w_qo.y_relay(1, 2, 3, 4)
    w_g.fast_relay()
    ag_sibling(0, xn, 0)
    ag_sibling(0, xn, 1)
    ag_sibling(0, xn, 3)
    ag_sibling(0, xn, 2)
    w_k.fast_one()
    w_k.fast_end()
    w_v.y_end(*range(8))
    w_qo.y_relay(5, 6, 7)

    def between_mixer(n):
        if n == 1:
            w_ld.fast_relay()
            w_u.y_wait()
            w_u.fast_start()
        elif n == 2:
            w_ld.fast_one()
            w_ld.y_start(1, 2, 3, 4)

    def turn(values, i):
        base = outer[rows(i * 8, 8)][0:1]
        base_cos, base_sin = base[:, 0:128], base[:, 128:256]
        cosine = base_cos * inner[:, 0:128] - base_sin * inner[:, 128:256]
        sine = base_sin * inner[:, 0:128] + base_cos * inner[:, 128:256]
        return values * cosine + pltpu.roll(values, 64, 1) * sine

    for pair in range(2):
        wide = slice(pair * 2 * BLOCK, (pair + 1) * 2 * BLOCK)
        k_wide = dot(xn[wide], b_k[...])
        v_wide = dot(xn[wide], b_v[...]).astype(BF16)
        vs[wide] = v_wide
        for n in range(2):
            i = 2 * pair + n
            here, inside = slice(i * BLOCK, (i + 1) * BLOCK), slice(n * BLOCK, (n + 1) * BLOCK)
            k = (turn(k_wide[inside], i) * DK**-0.5).astype(BF16)
            ks[here] = k
            kf = k.astype(F32)
            k_two = (jnp.concatenate([kf, kf], axis=1) * tail[...]).astype(BF16)
            us[here] = dot(k_two, v_wide[inside], TN)
        if pair == 0:
            w_u.y_start()
            w_ld.fast_start()
            w_ld.y_start(0)

    total = jnp.zeros((DK, DV), F32)
    for i in range(X):
        st[i * BLOCK : i * BLOCK + DK] = total.astype(BF16)
        total = step_f * total + us[i * BLOCK : i * BLOCK + DK]
    total = jnp.zeros((DK, DV), F32)
    for i in reversed(range(X)):
        st[i * BLOCK + DK : (i + 1) * BLOCK] = total.astype(BF16)
        total = step_b * total + us[i * BLOCK + DK : (i + 1) * BLOCK]


    w_g.fast_one()
    w_g.fast_end()
    for pair in range(2):
        wide = slice(pair * 2 * BLOCK, (pair + 1) * 2 * BLOCK)
        gates = dot(xn[wide], b_g[...])
        silu[wide] = gates / (1.0 + jnp.exp(-gates))
    w_qo.y_end(*range(8))

    first_sends = len(sent)

    def rs_block(t, d, left, weights, first, width):
        left = jnp.concatenate([left[rows((1 - c) * OWN, OWN)], left[rows(c * OWN, OWN)]], axis=0)
        there = slice(d * OWN, (d + 1) * OWN)
        for j in range(4):
            columns = slice(j * 256, (j + 1) * 256)
            part = dot(left, weights[columns, first : first + width], NT)
            ps[t, there, columns] = part[:OWN].astype(BF16)
            pf[there, columns] = part[OWN:]
        for p in (0, 2, 1, 3):
            send(
                ps.at[t, pl.ds(d * OWN + p * PIECE, PIECE)],
                pr.at[t, d, pl.ds(p * PIECE, PIECE)], pp_s.at[t, d, p], pp_r.at[t, d, p], sibling,
            )

    def rs_pair(t, d, p):
        received(pr.at[t, d, pl.ds(p * PIECE, PIECE)], pp_s.at[t, d, p], pp_r.at[t, d, p])
        mine = pf[d * OWN + p * PIECE : d * OWN + (p + 1) * PIECE]
        return mine + pr[t, d, p * PIECE : (p + 1) * PIECE].astype(F32)

    def rs_far(t):
        for p in (0, 2, 1, 3):
            rs_send[t, p] = rs_pair(t, 2, p).astype(BF16)
            peer = x_next if p < 2 else x_prev
            send(rs_send.at[t, p], rs_recv.at[t, p], rr_s.at[t, p], rr_r.at[t, p], peer)

    def rs_near(t, way, p, relay):
        total = rs_pair(t, 1 if way == 0 else 3, p)
        if relay:
            received(rs_recv.at[t, p], rr_s.at[t, p], rr_r.at[t, p])
            total = total + rs_recv[t, p].astype(F32)
        k = way * 4 + p
        ms_send[t, k] = total.astype(BF16)
        peer = x_next if way == 0 else x_prev
        send(ms_send.at[t, k], ms_recv.at[t, k], mm_s.at[t, k], mm_r.at[t, k], peer)

    def rs_final(t, p):
        total = rs_pair(t, 0, p)
        for k in (p, 4 + p):
            received(ms_recv.at[t, k], mm_s.at[t, k], mm_r.at[t, k])
            total = total + ms_recv[t, k].astype(F32)
        return total

    def reduce_scatter(t, block, weights, first, width, between):
        for n, d in enumerate((2, 1, 3, 0)):
            rs_block(t, d, block(d), weights, first, width)
            if n == 1:
                rs_far(t)
            if n == 2:
                rs_near(t, 0, 2, False)
            if n == 3:
                rs_near(t, 1, 0, False)
            between(n)
        rs_near(t, 0, 0, True)
        rs_near(t, 1, 2, True)
        rs_near(t, 0, 3, False)
        rs_near(t, 1, 1, False)
        rs_near(t, 0, 1, True)
        rs_near(t, 1, 3, True)

    def mixer_block(d):
        i = lax.rem(x + d, X)
        here = rows(i * BLOCK, BLOCK)
        q = turn(dot(xn[here], b_qo[:, 0:DK]), i).astype(BF16)
        scores = (dot(q, ks[here], NT) * dmat[...]).astype(BF16)
        qf = q.astype(F32)
        q_two = (jnp.concatenate([qf, qf], axis=1) * lead[...]).astype(BF16)
        retained = dot(scores, vs[here]) + dot(q_two, st[here])
        centred = retained - jnp.mean(retained, axis=-1, keepdims=True)
        normal = centred * lax.rsqrt(jnp.mean(centred * centred, axis=-1, keepdims=True) + EPS)
        gated[...] = (normal * silu[here]).astype(BF16)
        return gated

    reduce_scatter(0, mixer_block, b_qo, DK, DV, between_mixer)
    for n, p in enumerate((0, 2, 1, 3)):
        part = slice(p * PIECE, (p + 1) * PIECE)
        mixed = rs_final(0, p)
        summed = (tok[part].astype(F32) + rms(mixed, g_mo[...])).astype(BF16).astype(F32)
        after[part] = summed
        ch[rows(tp * OWN + p * PIECE, PIECE)] = rms(summed, g_ci[...]).astype(BF16)
        ag_start(1, ch, p)
        if n == 0:
            w_ld.fast_end()
            w_ld.y_start(5, 6, 7)
            w_ld.y_relay(0, 1, 2)
        elif n == 1:
            w_u.fast_relay()
        elif n == 2:
            w_ld.y_relay(3, 4)

    w_ld.y_relay(5, 6, 7)
    drain(first_sends)
    before_last = len(sent)
    ag_first(1, ch, 0, 2)
    ag_first(1, ch, 1, 3)

    def expand(d, core=None):
        count = BLOCK if core is None else OWN
        first = lax.rem(x + d, X) * BLOCK + (0 if core is None else core * OWN)
        there = pl.ds(pl.multiple_of(first + 8, 8), count)
        left = ch[rows(first, count)]
        up[there, 0:256] = dot(left, b_u[:, 0:256])
        up[there, 256:512] = dot(left, jnp.concatenate([b_u[:, 256:384], b_ld[:, 0:128]], axis=1))
        up[there, 512:768] = dot(left, b_ld[:, 128:384])

    w_u.fast_one()
    w_u.fast_end()
    w_ld.y_end(*range(8))
    ag_sibling(1, ch, 0)
    expand(0)
    ag_second(1, ch, 0, 2)
    ag_sibling(1, ch, 1)
    expand(1)
    ag_second(1, ch, 1, 3)
    ag_sibling(1, ch, 3)
    expand(3)
    expand(2, c)
    ag_sibling(1, ch, 2)
    expand(2, 1 - c)

    def conv(first, column, at):
        near = up[pl.ds(pl.multiple_of(first, 8), 80), column : column + FFP]
        before = pltpu.roll(near, 1, 0)[8:72]
        behind = pltpu.roll(near, 79, 0)[8:72]
        return (
            taps[at : at + 1] * before
            + taps[at + 1 : at + 2] * near[8:72]
            + taps[at + 2 : at + 3] * behind
            + taps[at + 3 : at + 4]
        )

    def channel_block(d):
        i = lax.rem(x + d, X)

        def tile(n, carry):
            first = i * BLOCK + n * HALF
            g = conv(first, 0, 0)
            act = 0.5 * g * (1.0 + jnp.tanh(0.7978845608028654 * (g + 0.044715 * g * g * g)))
            hid[pl.ds(pl.multiple_of(n * HALF, HALF), HALF)] = (
                act * conv(first, FFP, 8)
            ).astype(BF16)
            return carry

        lax.fori_loop(0, BLOCK // HALF, tile, 0)
        return hid

    reduce_scatter(1, channel_block, b_ld, FFP, FFP, lambda n: None)
    drain(before_last)
    for p in (0, 2, 1, 3):
        part = slice(p * PIECE, (p + 1) * PIECE)
        out[part] = (after[part] + rms(rs_final(1, p), g_co[...])).astype(BF16)

    for copy in sent:
        copy.wait_send()


def layer(
    tokens, mixer_in_gain, query_weight, key_weight, value_weight, gate_weight, decay_logits,
    mixer_output, mixer_out_gain, channel_in_gain, gelu_weight, linear_weight, gelu_kernel,
    linear_kernel, gelu_bias, linear_bias, down_weight, channel_out_gain,
):
    inner, outer = rotation_tables()

    def row(v):
        return v.reshape(1, -1)

    operands = (
        tokens[0], row(mixer_in_gain), query_weight, key_weight, value_weight, gate_weight,
        decay_logits.T, mixer_output.T, row(mixer_out_gain), row(channel_in_gain), gelu_weight,
        linear_weight, gelu_kernel, linear_kernel, gelu_bias, linear_bias, down_weight.T,
        row(channel_out_gain), jnp.asarray(inner), jnp.asarray(outer),
    )
    operands = [pltpu.with_memory_space_constraint(v, pltpu.HBM) for v in operands]
    dma = pltpu.SemaphoreType.DMA
    result = pl.pallas_call(
        kernel,
        out_shape=pltpu.VMEM((OWN, D), BF16),
        in_specs=[pl.BlockSpec(memory_space=pltpu.HBM)] * len(operands),
        out_specs=pl.BlockSpec(memory_space=pltpu.VMEM),
        scratch_shapes=[
            pltpu.VMEM((OWN, D), BF16),
            pltpu.VMEM((1, D), F32),
            pltpu.VMEM((1, 2), F32),
            pltpu.VMEM((1, D), F32),
            pltpu.VMEM((1, D), F32),
            pltpu.VMEM((3, FFOWN), F32),
            pltpu.VMEM((3, FFOWN), F32),
            pltpu.VMEM((FFOWN,), F32),
            pltpu.VMEM((FFOWN,), F32),
            pltpu.VMEM((1, D), F32),
            pltpu.VMEM((BLOCK, 256), F32),
            pltpu.VMEM((8 * X, 256), F32),
            pltpu.VMEM((UNIT, FFOWN), BF16),
            pltpu.VMEM((UNIT, FFOWN), BF16),
            pltpu.VMEM((UNIT, FFOWN), BF16),
            pltpu.VMEM((SEQ, D), BF16),
            pltpu.VMEM((SEQ, D), BF16),
            pltpu.VMEM((D, DK), BF16),
            pltpu.VMEM((D, DV), BF16),
            pltpu.VMEM((D, FFP), BF16),
            pltpu.VMEM((D, DV), BF16),
            pltpu.VMEM((D, DK + DV), BF16),
            pltpu.VMEM((D, 2 * FFP), BF16),
            pltpu.VMEM((SEQ, DK), BF16),
            pltpu.VMEM((SEQ, DV), BF16),
            pltpu.VMEM((SEQ, DV), F32),
            pltpu.VMEM((SEQ, DV), F32),
            pltpu.VMEM((SEQ, DV), BF16),
            pltpu.VMEM((BLOCK, BLOCK), F32),
            pltpu.VMEM((BLOCK, BLOCK), F32),
            pltpu.VMEM((BLOCK, BLOCK), F32),
            pltpu.VMEM((4 * OWN, D), F32),
            pltpu.VMEM((2, 4 * OWN, D), BF16),
            pltpu.VMEM((2, 4, OWN, D), BF16),
            pltpu.VMEM((2, 4, PIECE, D), BF16),
            pltpu.VMEM((2, 4, PIECE, D), BF16),
            pltpu.VMEM((2, 8, PIECE, D), BF16),
            pltpu.VMEM((2, 8, PIECE, D), BF16),
            pltpu.VMEM((SEQ + 16, 2 * FFP), F32),
            pltpu.VMEM((BLOCK, FFP), BF16),
            pltpu.VMEM((BLOCK, DV), BF16),
            pltpu.VMEM((OWN, D), F32),
            pltpu.VMEM((16, FFP), F32),
            dma((20,)),
            dma((2, 28)), dma((2, 28)),
            dma((3, 3)), dma((3, 3)),
            dma((3, 8, 3)), dma((3, 8, 3)),
            dma((6, 8)), dma((6, 8)),
            dma((2, 4, 4)), dma((2, 4, 4)),
            dma((2, 4)), dma((2, 4)),
            dma((2, 8)), dma((2, 8)),
        ],
        compiler_params=pltpu.CompilerParams(
            collective_id=0, has_side_effects=True, vmem_limit_bytes=40 * 1024 * 1024
        ),
        name="layer",
    )(*operands)
    return result[None]


def solution(mesh):
    by_position = P(("rep", "fs"), "tp", None)
    up_rows, down_rows = P("fs", "tp"), P("tp", "fs")
    in_specs = (
        by_position, P(), up_rows, up_rows, up_rows, up_rows, P(None, "tp"), down_rows, P(), P(),
        up_rows, up_rows, P(None, "tp"), P(None, "tp"), P("tp"), P("tp"), down_rows, P(),
    )
    return jax.shard_map(
        layer, mesh=mesh, in_specs=in_specs, out_specs=by_position, check_vma=False
    )
```
